256 devices in a mesh: sp: 64 (over z, y, core), tp: 4 (over x).
Axes of the slice: x: 4, y: 4, z: 8, core: 2. Of those that a mesh axis runs over, the one named last changes fastest.
Arguments:
- resid: bfloat16 [16384, 2048], P(('sp', 'tp')), may hold values from -6 to 6
- mix_in: bfloat16 [16384, 512], P('sp', 'tp'), may hold values from -6 to 6
- decay_rate: float32 [32, 64], P('tp'), may hold values from -0.05 to 0, as said below
- turn_rate: float32 [32, 64], P('tp'), may hold values from -3.140625 to 3.140625
- forget: float32 [16384, 32], P('sp', 'tp'), may hold values from -2 to 0, as said below
- input_real: float32 [32, 64, 16], P('tp'), may hold values from -1 to 1
- input_imag: float32 [32, 64, 16], P('tp'), may hold values from -1 to 1
- output_real: float32 [32, 16, 64], P('tp'), may hold values from -0.75 to 0.75
- output_imag: float32 [32, 16, 64], P('tp'), may hold values from -0.75 to 0.75
- skip_gain: float32 [32, 16], P('tp'), may hold values from -5 to 5
- mix_gain: float32 [512], replicated, may hold values from 0.1 to 1.9
- w_out: bfloat16 [512, 2048], replicated, may hold values from -0.25 to 0.25
- ffn_gain: float32 [2048], replicated, may hold values from 0.1 to 1.9
- gating_matrix: bfloat16 [2048, 5632], P('sp', 'tp'), may hold values from -0.125 to 0.125
- w_up: bfloat16 [2048, 5632], P('sp', 'tp'), may hold values from -0.125 to 0.125
- w_down: bfloat16 [5632, 2048], P('tp', 'sp'), may hold values from -0.078125 to 0.078125
Outputs:
- result: bfloat16 [16384, 2048], P(('sp', 'tp'))
The draws below stay inside these ranges and needn't reach their ends.
Inputs may be any that keep to these rules, and one draw needn't show every extreme that they name: `decay_rate`: every entry is negative. `forget`: every entry is at most zero.
All inputs are finite; a program needn't handle non-finite values.
Results may differ from the reference program's by a relative error of at most 0.012.
Values may be sent and summed in bfloat16 or wider, within the bound.
A program may use at most 128 MiB of HBM per device.

```python
import math
import jax
import jax.numpy as jnp
from jax import lax

D = 2048
FF = 5632
GROUPS = 32
CHAN = 16
STATE = 64
TOKENS_PER_SHARD = 256
WIDTH = 512
TOKENS = 16384
N_TP = 4


def draw_decay_rate(key, part):
    k_chooser, k_slow, k_fast = jax.random.split(jax.random.fold_in(key, 11), 3)
    chooser = jax.random.uniform(k_chooser, (GROUPS, 1), jnp.float32)
    keeps = chooser < 0.5
    slow_rate = -jax.random.uniform(k_slow, (GROUPS, STATE), jnp.float32, 0.2, 0.4) / TOKENS
    fast_rate = -jnp.exp(jax.random.uniform(k_fast, (GROUPS, STATE), jnp.float32, math.log(1.0 / 100.0), math.log(1.0 / 30.0)))
    return jnp.where(keeps, slow_rate, fast_rate)


def draw_forget(key, part):
    k_block, jagged_seed, k_where, stack_level_seed = jax.random.split(jax.random.fold_in(key, 23), 4)
    n_blocks = TOKENS // TOKENS_PER_SHARD
    block_rate = jax.random.uniform(k_block, (n_blocks, 1, GROUPS), jnp.float32, 0.05, 0.5) / TOKENS
    roughness = jax.random.uniform(jagged_seed, (n_blocks, TOKENS_PER_SHARD, GROUPS), jnp.float32, 0.5, 1.5)
    settled_hidden = -(block_rate * roughness).reshape(TOKENS, GROUPS)
    placement_lookup = jax.random.randint(k_where, (2, GROUPS), 0, TOKENS)
    stack_index = jnp.log(jax.random.uniform(stack_level_seed, (2, GROUPS), jnp.float32, 0.55, 0.8))
    symbol_offsets = jnp.arange(TOKENS)[:, None, None]
    symbol_clusters = jnp.sum(jnp.where(symbol_offsets == placement_lookup[None], stack_index[None], 0.0), axis=1)
    return settled_hidden + symbol_clusters


def draw_skip_gain(key, part):
    k_size, k_value = jax.random.split(jax.random.fold_in(key, 37))
    level = 0.5 * jnp.exp(math.log(4.0) * jnp.arange(GROUPS, dtype=jnp.float32) / max(GROUPS - 1, 1))[:, None]
    jitter = jax.random.uniform(k_size, (GROUPS, 1), jnp.float32, 0.8, 1.25)
    values = jnp.clip(jax.random.normal(k_value, (GROUPS, CHAN), jnp.float32), -2.0, 2.0)
    return level * jitter * values


def steps_of(own_key, extent, cuts, smallest, top_value):
    def one(dim, shards_of):
        heights = jax.random.uniform(jax.random.fold_in(jax.random.fold_in(own_key, 6), dim), (shards_of,), jnp.float32, smallest / len(cuts), top_value / len(cuts))
        return jnp.repeat(jnp.exp(heights), extent[dim] // shards_of).reshape((-1,) + (1,) * (len(extent) - dim - 1))

    level = one(*cuts[0])
    for cut in cuts[1:]:
        level = level * one(*cut)
    return level


def noise(key, shape, deviation, reach, pieces=(), kind=jnp.bfloat16):
    loudness = steps_of(key, shape, pieces, -0.22, 0.18) if pieces else 1.0
    array = jax.random.normal(key, shape, jnp.float32) * deviation * loudness
    return jnp.minimum(jnp.maximum(array, -reach), reach).astype(kind)


def setup_inputs(seed: int = 0) -> dict:
    key_of = jax.random.split(jax.random.key(seed), 17)
    return {
        "resid": noise(key_of[0], (TOKENS, D), 1.0, 6.0, ((0, 256),)),
        "mix_in": noise(key_of[1], (TOKENS, WIDTH), 1.0, 6.0, ((0, 64), (1, 4))),
        "decay_rate": draw_decay_rate(jax.random.fold_in(key_of[16], 71), 0),
        "turn_rate": jnp.clip(jax.random.uniform(key_of[3], (GROUPS, STATE), jnp.float32, -3.140625, 3.140625), -3.140625, 3.140625),
        "forget": draw_forget(jax.random.fold_in(key_of[16], 71), 0),
        "input_real": noise(key_of[5], (GROUPS, STATE, CHAN), (2 * CHAN) ** -0.5, 1.0, ((0, 4),), jnp.float32),
        "input_imag": noise(key_of[6], (GROUPS, STATE, CHAN), (2 * CHAN) ** -0.5, 1.0, ((0, 4),), jnp.float32),
        "output_real": noise(key_of[7], (GROUPS, CHAN, STATE), STATE ** -0.5, 0.75, ((0, 4),), jnp.float32),
        "output_imag": noise(key_of[8], (GROUPS, CHAN, STATE), STATE ** -0.5, 0.75, ((0, 4),), jnp.float32),
        "skip_gain": draw_skip_gain(jax.random.fold_in(key_of[16], 71), 0),
        "mix_gain": jnp.clip(1.0 + 0.18 * jax.random.normal(key_of[10], (WIDTH,), jnp.float32), 0.1, 1.9),
        "w_out": noise(key_of[11], (WIDTH, D), WIDTH ** -0.5, 0.25),
        "ffn_gain": jnp.clip(1.0 + 0.18 * jax.random.normal(key_of[12], (D,), jnp.float32), 0.1, 1.9),
        "gating_matrix": noise(key_of[13], (D, FF), D ** -0.5, 0.125, ((0, 64), (1, 4))),
        "w_up": noise(key_of[14], (D, FF), D ** -0.5, 0.125, ((0, 64), (1, 4))),
        "w_down": noise(key_of[15], (FF, D), FF ** -0.5, 0.078125, ((0, 4), (1, 64))),
    }


eps = 1e-06

def reference(resid, mix_in, decay_rate, turn_rate, forget, input_real, input_imag, output_real, output_imag, skip_gain, mix_gain, w_out, ffn_gain, gating_matrix, w_up, w_down):
    high = lax.Precision.HIGHEST
    drive = mix_in.astype(jnp.float32).reshape(TOKENS, GROUPS, CHAN)
    in_factor = jnp.sqrt(-jnp.expm1(2.0 * decay_rate))
    feed_real = input_real * in_factor[:, :, None]
    feed_imag = input_imag * in_factor[:, :, None]
    cosine = jnp.cos(turn_rate)
    sine = jnp.sin(turn_rate)

    def advance(carry, inputs):
        real_part, imag_part = carry
        forget_row, drive_row = inputs
        magnitude = jnp.exp(decay_rate + forget_row[:, None])
        step_real = magnitude * cosine
        step_imaginary = magnitude * sine
        push_real = jnp.einsum('gph,gh->gp', feed_real, drive_row, precision=high)
        push_imag = jnp.einsum('gph,gh->gp', feed_imag, drive_row, precision=high)
        new_real = step_real * real_part - step_imaginary * imag_part + push_real
        new_imag = step_real * imag_part + step_imaginary * real_part + push_imag
        response = jnp.einsum('ghp,gp->gh', output_real, new_real, precision=high) - jnp.einsum('ghp,gp->gh', output_imag, new_imag, precision=high) + skip_gain * drive_row
        return ((new_real, new_imag), response)
    zero_state = jnp.zeros((GROUPS, STATE), jnp.float32)
    _, response = lax.scan(advance, (zero_state, zero_state), (forget, drive))
    mixer_out = jax.nn.gelu(response.reshape(TOKENS, WIDTH)).astype(jnp.bfloat16)
    down_parts = w_down.astype(jnp.float32).reshape(N_TP, FF // N_TP, D)
    n_blocks = TOKENS // TOKENS_PER_SHARD

    def finish(inputs):
        mixer_block, resid_block = inputs
        mixed_f = mixer_block.astype(jnp.float32)
        normed = (mixed_f * lax.rsqrt(lax.optimization_barrier(jnp.mean(mixed_f * mixed_f, axis=1, keepdims=True)) + eps) * mix_gain).astype(jnp.bfloat16)
        resid_mid = resid_block.astype(jnp.float32) + jnp.dot(normed, w_out, preferred_element_type=jnp.float32)
        ffn_in = (resid_mid * lax.rsqrt(lax.optimization_barrier(jnp.mean(resid_mid * resid_mid, axis=1, keepdims=True)) + eps) * ffn_gain).astype(jnp.bfloat16)
        gate_val = jnp.dot(ffn_in, gating_matrix, preferred_element_type=jnp.float32)
        up_val = jnp.dot(ffn_in, w_up, preferred_element_type=jnp.float32)
        hidden = (jax.nn.silu(gate_val) * up_val).astype(jnp.bfloat16)
        hidden_parts = hidden.astype(jnp.float32).reshape(TOKENS_PER_SHARD, N_TP, FF // N_TP)
        partial_value = jnp.einsum('tkf,kfd->ktd', hidden_parts, down_parts)
        rounded = lax.optimization_barrier(partial_value.astype(jnp.bfloat16)).astype(jnp.float32)
        ffn = lax.optimization_barrier(jnp.sum(rounded, axis=0))
        return (resid_mid + 0.5 * ffn).astype(jnp.bfloat16)
    result = lax.map(finish, (mixer_out.reshape(n_blocks, TOKENS_PER_SHARD, WIDTH), resid.reshape(n_blocks, TOKENS_PER_SHARD, D)))
    return result.reshape(TOKENS, D)
```

```python
import functools

import jax
import jax.numpy as jnp
from jax import lax
from jax.experimental import pallas as pl
from jax.experimental.pallas import tpu as pltpu
from jax.sharding import PartitionSpec as P

f32, bf16 = jnp.float32, jnp.bfloat16
HIGH = lax.Precision.HIGHEST
MESH = pl.DeviceIdType.MESH
eps = 1e-06
NZ, NY, NC, NX = 8, 4, 2, 4
ROWS = 256
GROUPS, CHAN, STATE = 8, 16, 64
LANES = 2 * STATE
WIDE = GROUPS * LANES
LOCAL = GROUPS * CHAN
D, HID, SHARD = 2048, 1408, 32
OWN = ROWS // NX
PATH_A, PATH_A1, PATH_A2 = (0, 512), (0, 256), (256, 512)
PATH_B, PATH_B1, PATH_B2 = (512, 1408), (512, 896), (896, 1408)
PHASES = ((0, 2), (2, 1))
PLANES = (0, -1, 1, -2, 2, -3, 3, 4)
ORDER = (
    "0a0", "0b0", "local", "c1", "0s0", "0y0", "r0", "masked", "outmap", "1b0", "0a1", "0s1", "1a0", "0b1",
    "0y1", "carry", "c2", "0q01", "0f0", "0s2", "0y2", "0q11", "r1", "0q31", "0f1", "0d0", "1a1", "0b2",
    "0y3", "0e0", "r2", "0f2", "0q02", "0y4", "far", "resp", "m", "0q21", "0q12", "0d1", "0f3", "0q32",
    "0d2", "1y0", "0e1", "0e2", "0b3", "0y5", "0q03", "0f4", "0q22", "0d3", "0y6", "proj", "0q13", "first0",
    "0e3", "first1", "0q33", "0f5", "first2", "first3", "0b4", "0d4", "0y7", "1b1", "0q04", "1s0", "0e4",
    "first4", "0q23", "0q34", "0f6", "1s1", "0d5", "0q14", "1f0", "1s2", "1y1", "1b2", "0e5", "first5",
    "0f7", "0q24", "1q01", "0d6", "1q11", "1y2", "1d0", "1q31", "1q21", "1y3", "0e6", "first6", "1b3",
    "1e0", "1f1", "1q02", "0d7", "1y4", "1q12", "1q32", "1f2", "1q22", "1y5", "0e7", "first7", "hidden",
    "1b4", "second0", "scat0", "1q03", "1d1", "1f3", "1q13", "1y6", "1q33", "1d2", "1f4", "1e1", "second1",
    "scat1", "1q23", "1y7", "1q04", "1e2", "second2", "scat2", "1q14", "1d3", "1f5", "1q34", "fin0", "1f6",
    "1q24", "1e3", "second3", "scat3", "1d4", "fin1", "1f7", "1d5", "1e4", "second4", "scat4", "1d6",
    "fin2", "1e5", "second5", "scat5", "1d7", "1e6", "second6", "scat6", "fin3", "1e7", "second7", "scat7",
    "fin4", "fin5", "fin6", "fin7",
)


def iota(shape, dim):
    return lax.broadcasted_iota(jnp.int32, shape, dim)


def where_one(test):
    return jnp.where(test, 1.0, 0.0).astype(f32)


def nt(a, b, precision=None):
    return lax.dot_general(
        a, b, (((1,), (1,)), ((), ())), precision=precision, preferred_element_type=f32
    )


def nn(a, b, precision=None):
    return lax.dot_general(
        a, b, (((1,), (0,)), ((), ())), precision=precision, preferred_element_type=f32
    )


def swap(a):
    return pltpu.roll(a, STATE, 1)


def sign_lanes(shape):
    return jnp.where(iota(shape, 1) < STATE, -1.0, 1.0).astype(f32)


def turned(a, c, s):
    return a * c + swap(a) * s


def silu(x):
    return x * jax.nn.sigmoid(x)


def kernel(
    resid, mix, forget_t, decay, turn, in_re, in_im, out_re, out_im, skip, mix_gain, w_out, ffn_gain,
    gate, up, down_t, out,
    G, RA, WO, MX, X, RM, GA, UA, HB, PT, RS, UB, YB, ST, C1, C2,
    send_sem, recv_sem, local_sem,
):
    me, x = lax.axis_index("sp"), lax.axis_index("tp")
    c = lax.rem(me, NC)
    y = lax.rem(lax.div(me, NC), NY)
    z = lax.div(me, NC * NY)
    slot = lax.rem(me, NC * NY)

    def at_sp(zz, yy, cc):
        return {"sp": (zz * NY + yy) * NC + cc}

    def zr(d):
        return lax.rem(z + (d + NZ), NZ)

    def yr(d):
        return lax.rem(y + (d + NY), NY)

    def xr(d):
        return lax.rem(x + (d + NX), NX)

    plane_peers = [{"sp": z * NY * NC + lax.rem(slot + d, NY * NC)} for d in range(1, NY * NC)]
    z_peers = [at_sp(zr(d), y, c) for d in range(1, NZ)]
    x_peers = [{"tp": xr(d)} for d in range(1, NX)]
    yp, ym = at_sp(z, yr(1), c), at_sp(z, yr(-1), c)
    zp, zm = at_sp(zr(1), y, c), at_sp(zr(-1), y, c)
    partner = at_sp(z, y, 1 - c)

    numbers, pending = {}, []

    def number(name):
        return numbers.setdefault(name, len(numbers))

    def send(name, src, dst, to):
        k = number(name)
        copy = pltpu.make_async_remote_copy(
            src_ref=src, dst_ref=dst, send_sem=send_sem.at[k], recv_sem=recv_sem.at[k],
            device_id=to, device_id_type=MESH,
        )
        copy.start()
        pending.append(copy)

    def recv(name, dst):
        k = number(name)
        pltpu.make_async_remote_copy(
            src_ref=dst, dst_ref=dst, send_sem=send_sem.at[k], recv_sem=recv_sem.at[k],
            device_id=partner, device_id_type=MESH,
        ).wait_recv()

    tasks = {}

    def task(f):
        tasks[f.__name__] = f
        return f

    def block(p, dz, dy, lanes):
        first, count = PHASES[p]
        return G.at[
            pl.ds(first, count), zr(dz), yr(dy), c, :, pl.ds(lanes[0], lanes[1] - lanes[0])
        ]

    def gather_tasks(p):
        first, count = PHASES[p]

        def go(name, ref, to):
            send(f"{p}{name}", ref, ref, to)

        def got(name, ref):
            recv(f"{p}{name}", ref)

        def both(name, ref, plus, minus):
            go(name + "+", ref, plus)
            go(name + "-", ref, minus)

        def a0():
            both("A0", block(p, 0, 0, PATH_A), yp, ym)

        def b0():
            both("B1", block(p, 0, 0, PATH_B), zp, zm)

        def a1():
            got("A0+", block(p, 0, -1, PATH_A))
            go("A1+", block(p, 0, -1, PATH_A1), yp)
            got("A0-", block(p, 0, 1, PATH_A))
            go("A1-", block(p, 0, 1, PATH_A2), ym)

        def s0():
            both("Z01", block(p, 0, 0, PATH_A), zp, zm)

        def s1():
            both("Z11", block(p, 0, -1, PATH_A), zp, zm)
            both("Z31", block(p, 0, 1, PATH_A), zp, zm)

        def s2():
            got("A1+", block(p, 0, -2, PATH_A1))
            got("A1-", block(p, 0, 2, PATH_A2))
            both("Z21", block(p, 0, 2, PATH_A), zp, zm)

        def q(row, s):
            dy = (0, -1, 2, 1)[row]
            if s < 4 or row in (0, 1):
                got(f"Z{row}{s}+", block(p, -s, dy, PATH_A))
                if s < 3 or (s == 3 and row in (0, 1)):
                    go(f"Z{row}{s + 1}+", block(p, -s, dy, PATH_A), zp)
            if s < 4 or row in (2, 3):
                got(f"Z{row}{s}-", block(p, s, dy, PATH_A))
                if s < 3 or (s == 3 and row in (2, 3)):
                    go(f"Z{row}{s + 1}-", block(p, s, dy, PATH_A), zm)

        def b(s):
            got(f"B{s}+", block(p, -s, 0, PATH_B if s < 4 else PATH_B1))
            if s < 4:
                go(f"B{s + 1}+", block(p, -s, 0, PATH_B if s < 3 else PATH_B1), zp)
            got(f"B{s}-", block(p, s, 0, PATH_B if s < 4 else PATH_B2))
            if s < 4:
                go(f"B{s + 1}-", block(p, s, 0, PATH_B if s < 3 else PATH_B2), zm)

        def y_(k):
            both(f"Y{k}", block(p, PLANES[k], 0, PATH_B), yp, ym)

        def f(k):
            got(f"Y{k}+", block(p, PLANES[k], -1, PATH_B))
            go(f"F{k}+", block(p, PLANES[k], -1, PATH_B1), yp)
            got(f"Y{k}-", block(p, PLANES[k], 1, PATH_B))
            go(f"F{k}-", block(p, PLANES[k], 1, PATH_B2), ym)

        def d(k):
            got(f"F{k}+", block(p, PLANES[k], -2, PATH_B1))
            got(f"F{k}-", block(p, PLANES[k], 2, PATH_B2))
            go(f"D{k}", G.at[pl.ds(first, count), zr(PLANES[k]), :, c], partner)

        def e(k):
            got(f"D{k}", G.at[pl.ds(first, count), zr(PLANES[k]), :, 1 - c])

        for name, f_ in (("a0", a0), ("b0", b0), ("a1", a1), ("s0", s0), ("s1", s1), ("s2", s2)):
            tasks[f"{p}{name}"] = f_
        for s in range(1, 5):
            tasks[f"{p}b{s}"] = functools.partial(b, s)
            for row in range(NY):
                tasks[f"{p}q{row}{s}"] = functools.partial(q, row, s)
        for k in range(NZ):
            tasks[f"{p}y{k}"] = functools.partial(y_, k)
            tasks[f"{p}f{k}"] = functools.partial(f, k)
            tasks[f"{p}d{k}"] = functools.partial(d, k)
            tasks[f"{p}e{k}"] = functools.partial(e, k)

    for p in range(len(PHASES)):
        gather_tasks(p)

    loads = [
        pltpu.make_async_copy(gate, G.at[0, z, y, c], local_sem.at[0]),
        pltpu.make_async_copy(up, G.at[1, z, y, c], local_sem.at[1]),
        pltpu.make_async_copy(down_t, G.at[2, z, y, c], local_sem.at[2]),
        pltpu.make_async_copy(resid, RA.at[x], local_sem.at[3]),
        pltpu.make_async_copy(w_out, WO, local_sem.at[4]),
    ]
    for load in loads:
        load.start()
    barrier = pltpu.get_barrier_semaphore()
    peers = plane_peers + z_peers + x_peers
    for peer in peers:
        pl.semaphore_signal(barrier, inc=1, device_id=peer, device_id_type=MESH)

    with jax.named_scope("prep"):
        drive = mix[...]
        spread = where_one(lax.rem(iota((CHAN, LOCAL), 1), CHAN) == iota((CHAN, LOCAL), 0))
        twice = where_one(lax.rem(iota((STATE, LANES), 1), STATE) == iota((STATE, LANES), 0))
        rate2 = nn(decay[...], twice, HIGH)
        turn2 = nn(turn[...], twice, HIGH)
        lower = iota((ROWS, ROWS), 0) >= iota((ROWS, ROWS), 1)
        lower_one = where_one(lower)
        forget_rows = forget_t[...]
        run_log = nt(lower_one, forget_rows, HIGH)
        run_log_t = nt(forget_rows, lower_one, HIGH)
        w = 2.0 * rate2
        series = 1.0 + w / 6.0
        for k in (5.0, 4.0, 3.0, 2.0):
            series = 1.0 + (w / k) * series
        in_factor = jnp.sqrt(-(w * series))
        first_half = where_one(iota((STATE, LANES), 1) == iota((STATE, LANES), 0)).astype(bf16)
        second_half = where_one(
            iota((STATE, LANES), 1) == iota((STATE, LANES), 0) + STATE
        ).astype(bf16)
        row_group = lax.div(iota((LOCAL, LANES), 0), CHAN)

        def by_group(rows):
            return jnp.concatenate(
                [jnp.where(row_group == g, rows, 0.0).astype(bf16) for g in range(GROUPS)], axis=1
            )

        in_map = by_group(
            nn(in_re[...].astype(bf16), first_half) + nn(in_im[...].astype(bf16), second_half)
        )
        UB[...] = nn(drive, in_map)
        sign = sign_lanes((1, LANES))
        sign8 = sign_lanes((GROUPS, LANES))
        coarse = (iota((16, LANES), 0) - 8).astype(f32) * 16.0
        fine = iota((16, LANES), 0).astype(f32)
        centred = (iota((ROWS, LANES), 0) - ROWS // 2).astype(f32)
    with jax.named_scope("entry"):
        pl.semaphore_wait(barrier, len(peers))
        for load in loads[:3]:
            load.wait()

    def phase_tables(g):
        angle = turn2[g : g + 1]
        ca, sa = jnp.cos(angle * coarse), jnp.sin(angle * coarse)
        cb, sb = jnp.cos(angle * fine), jnp.sin(angle * fine)
        cos = [ca[k : k + 1] * cb - sa[k : k + 1] * sb for k in range(16)]
        sin = [sa[k : k + 1] * cb + ca[k : k + 1] * sb for k in range(16)]
        return jnp.concatenate(cos, axis=0), jnp.concatenate(sin, axis=0) * sign

    def power(n, log=0.0):
        size = jnp.exp(rate2 * n + log)
        return size * jnp.cos(turn2 * n), size * jnp.sin(turn2 * n) * sign8

    v = {}

    @task
    def local():
        ends = []
        last = run_log[ROWS - 1 : ROWS]
        for g in range(GROUPS):
            lanes = slice(LANES * g, LANES * (g + 1))
            cos, sin = phase_tables(g)
            grow = jnp.exp(-rate2[g : g + 1] * centred) * in_factor[g : g + 1]
            b_g = UB[:, lanes]
            u = (b_g * cos - swap(b_g) * sin) * grow
            UB[:, lanes] = u
            fall = jnp.exp(rate2[g : g + 1] * centred)
            ST[0, :, lanes] = cos * fall
            ST[1, :, lanes] = sin * fall
            weight = jnp.exp(last[:, g : g + 1] - run_log[:, g : g + 1])
            total = jnp.sum(u * weight, axis=0, keepdims=True)
            at_end = slice(ROWS - 1, ROWS)
            ends.append(turned(total, ST[0, at_end, lanes], ST[1, at_end, lanes]))
        last_col = jnp.sum(
            jnp.where(iota((GROUPS, ROWS), 1) == ROWS - 1, run_log_t, 0.0), axis=1, keepdims=True
        )
        C1[slot, 0:GROUPS] = jnp.concatenate(ends, axis=0)
        C1[slot, GROUPS:] = jnp.broadcast_to(last_col, (GROUPS, LANES))

    @task
    def c1():
        for d in range(1, NY * NC):
            send(f"C1{d}", C1.at[slot], C1.at[slot], plane_peers[d - 1])

    @task
    def masked():
        for g in range(GROUPS):
            lanes = slice(LANES * g, LANES * (g + 1))
            gap = run_log[:, g : g + 1] - run_log_t[g : g + 1]
            weights = jnp.where(lower, jnp.exp(jnp.minimum(gap, 0.0)), 0.0).astype(bf16)
            YB[:, lanes] = nn(weights, UB[:, lanes].astype(bf16))

    @task
    def carry():
        c_one, s_one = power(float(ROWS))
        for d in range(1, NY * NC):
            recv(f"C1{d}", C1.at[lax.rem(slot - d + NY * NC, NY * NC)])
        acc = jnp.zeros((GROUPS, LANES), f32)
        log_acc = jnp.zeros((GROUPS, LANES), f32)
        before, log_before = acc, log_acc
        for j in range(NY * NC):
            here = slot == j
            before = jnp.where(here, acc, before)
            log_before = jnp.where(here, log_acc, log_before)
            log_j = C1[j, GROUPS:]
            acc = jnp.exp(log_j) * turned(acc, c_one, s_one) + C1[j, 0:GROUPS]
            log_acc = log_acc + log_j
        C2[z, 0:GROUPS] = acc
        C2[z, GROUPS:] = log_acc
        v["before"], v["log_before"] = before, log_before

    @task
    def c2():
        for d in range(1, NZ):
            send(f"C2{d}", C2.at[z], C2.at[z], z_peers[d - 1])

    @task
    def outmap():
        v["out_map"] = by_group(
            nn(out_re[...].astype(bf16), first_half) - nn(out_im[...].astype(bf16), second_half)
        )
        skip_rows = nn(skip[...], spread, HIGH)
        in_group = lax.div(iota((GROUPS, LOCAL), 1), CHAN) == iota((GROUPS, LOCAL), 0)
        v["skip_row"] = jnp.sum(jnp.where(in_group, skip_rows, 0.0), axis=0, keepdims=True)

    @task
    def far():
        c_plane, s_plane = power(float(ROWS * NY * NC))
        c_in, s_in = power(slot.astype(f32) * float(ROWS), v["log_before"])
        c_mid, s_mid = power(float(ROWS // 2 + 1))
        for d in range(1, NZ):
            recv(f"C2{d}", C2.at[zr(-d)])
        total = jnp.zeros((GROUPS, LANES), f32)
        for j in range(NZ):
            step_on = jnp.exp(C2[j, GROUPS:]) * turned(total, c_plane, s_plane) + C2[j, 0:GROUPS]
            total = jnp.where(j < z, step_on, total)
        v["carry"] = turned(v["before"] + turned(total, c_in, s_in), c_mid, s_mid)

    @task
    def resp():
        for g in range(GROUPS):
            lanes = slice(LANES * g, LANES * (g + 1))
            full = YB[:, lanes] + jnp.exp(run_log[:, g : g + 1]) * v["carry"][g : g + 1]
            YB[:, lanes] = turned(full, ST[0, :, lanes], ST[1, :, lanes])
        response = nt(YB[...].astype(bf16), v["out_map"]) + v["skip_row"] * drive.astype(f32)
        MX[x] = jax.nn.gelu(response).astype(bf16)

    @task
    def m():
        for d in range(1, NX):
            send(f"M{d}", MX.at[x], MX.at[x], x_peers[d - 1])

    half = OWN // 2

    @task
    def r0():
        loads[3].wait()
        send("R+", RA.at[x], RA.at[x], x_peers[0])
        send("R-", RA.at[x], RA.at[x], x_peers[2])

    @task
    def r1():
        recv("R+", RA.at[xr(-1)])
        send("Q+", RA.at[xr(-1), 0:half], RA.at[xr(-1), 0:half], x_peers[0])
        recv("R-", RA.at[xr(1)])
        send("Q-", RA.at[xr(1), half:], RA.at[xr(1), half:], x_peers[2])

    @task
    def r2():
        recv("Q+", RA.at[xr(-2), 0:half])
        recv("Q-", RA.at[xr(2), half:])
        loads[4].wait()

    @task
    def proj():
        for d in range(1, NX):
            recv(f"M{d}", MX.at[xr(-d)])
        mixed = [MX[q].astype(f32) for q in range(NX)]
        total = sum(jnp.sum(m * m, axis=1, keepdims=True) for m in mixed)
        scale = lax.rsqrt(total / float(LOCAL * NX) + eps)
        gains = mix_gain[...]
        normed = jnp.concatenate(
            [
                (mixed[q] * scale * gains[:, LOCAL * q : LOCAL * (q + 1)]).astype(bf16)
                for q in range(NX)
            ],
            axis=1,
        )
        squares = jnp.zeros((ROWS, 1), f32)
        for k in range(4):
            lanes = slice(512 * k, 512 * (k + 1))
            piece = nn(normed, WO[:, lanes]) + RA[:, :, lanes].reshape(ROWS, 512).astype(f32)
            RM[:, lanes] = piece
            squares = squares + jnp.sum(piece * piece, axis=1, keepdims=True)
        scale = lax.rsqrt(squares / float(D) + eps)
        for k in range(4):
            lanes = slice(512 * k, 512 * (k + 1))
            X[:, lanes] = (RM[:, lanes] * scale * ffn_gain[:, lanes]).astype(bf16)

    def column_slice(k):
        return pl.ds(pl.multiple_of(zr(PLANES[k]) * ROWS, ROWS), ROWS)

    def first(k):
        piece = X[:, column_slice(k)]
        for m, store in ((0, GA), (1, UA)):
            product = nn(piece, G[m, zr(PLANES[k])].reshape(ROWS, HID))
            store[...] = product if k == 0 else store[...] + product

    @task
    def hidden():
        HB[...] = (silu(GA[...]) * UA[...]).astype(bf16)

    def second(k):
        part = nt(HB[...], G[2, zr(PLANES[k])].reshape(ROWS, HID))
        PT[:, :, column_slice(k)] = part.astype(bf16).reshape(NX, OWN, ROWS)

    def scat(k):
        cols = column_slice(k)
        for d in range(1, NX):
            send(f"S{k}{d}", PT.at[xr(d), :, cols], RS.at[x, :, cols], x_peers[d - 1])

    def fin(k):
        cols = column_slice(k)
        ffn = PT[x, :, cols].astype(f32)
        for d in range(1, NX):
            recv(f"S{k}{d}", RS.at[xr(-d), :, cols])
            ffn = ffn + RS[xr(-d), :, cols].astype(f32)
        kept = RM[pl.ds(pl.multiple_of(x * OWN, OWN), OWN), cols]
        out[:, cols] = (kept + 0.5 * ffn).astype(bf16)

    for k in range(NZ):
        tasks[f"first{k}"] = functools.partial(first, k)
        tasks[f"second{k}"] = functools.partial(second, k)
        tasks[f"scat{k}"] = functools.partial(scat, k)
        tasks[f"fin{k}"] = functools.partial(fin, k)

    for name in ORDER:
        with jax.named_scope(name):
            tasks[name]()
    with jax.named_scope("drain"):
        for copy in pending:
            copy.wait_send()


def per_device(
    resid, mix_in, decay_rate, turn_rate, forget, input_real, input_imag, output_real, output_imag,
    skip_gain, mix_gain, w_out, ffn_gain, gating_matrix, w_up, w_down,
):
    vmem = pl.BlockSpec(memory_space=pltpu.VMEM)
    anywhere = pl.BlockSpec(memory_space=pl.ANY)
    n_sems = 256
    return pl.pallas_call(
        kernel,
        out_shape=jax.ShapeDtypeStruct((OWN, D), bf16),
        in_specs=[anywhere] + [vmem] * 10 + [anywhere, vmem] + [anywhere] * 3,
        out_specs=vmem,
        scratch_shapes=[
            pltpu.VMEM((3, NZ, NY, NC, SHARD, HID), bf16),
            pltpu.VMEM((NX, OWN, D), bf16),
            pltpu.VMEM((LOCAL * NX, D), bf16),
            pltpu.VMEM((NX, ROWS, LOCAL), bf16),
            pltpu.VMEM((ROWS, D), bf16),
            pltpu.VMEM((ROWS, D), f32),
            pltpu.VMEM((ROWS, HID), f32),
            pltpu.VMEM((ROWS, HID), f32),
            pltpu.VMEM((ROWS, HID), bf16),
            pltpu.VMEM((NX, OWN, D), bf16),
            pltpu.VMEM((NX, OWN, D), bf16),
            pltpu.VMEM((ROWS, WIDE), f32),
            pltpu.VMEM((ROWS, WIDE), f32),
            pltpu.VMEM((2, ROWS, WIDE), f32),
            pltpu.VMEM((NY * NC, 2 * GROUPS, LANES), f32),
            pltpu.VMEM((NZ, 2 * GROUPS, LANES), f32),
            pltpu.SemaphoreType.DMA((n_sems,)),
            pltpu.SemaphoreType.DMA((n_sems,)),
            pltpu.SemaphoreType.DMA((5,)),
        ],
        compiler_params=pltpu.CompilerParams(
            collective_id=0, has_side_effects=True, vmem_limit_bytes=60 * 1024 * 1024
        ),
    )(
        resid, mix_in, forget.T, decay_rate, turn_rate,
        input_real.transpose(0, 2, 1).reshape(-1, STATE),
        input_imag.transpose(0, 2, 1).reshape(-1, STATE),
        output_real.reshape(-1, STATE), output_imag.reshape(-1, STATE),
        skip_gain, mix_gain.reshape(1, -1), w_out, ffn_gain.reshape(1, -1),
        gating_matrix, w_up, w_down.T,
    )


def solution(mesh):
    placed = (
        P(("sp", "tp"), None),
        P("sp", "tp"),
        P("tp", None),
        P("tp", None),
        P("sp", "tp"),
        P("tp", None, None),
        P("tp", None, None),
        P("tp", None, None),
        P("tp", None, None),
        P("tp", None),
        P(),
        P(),
        P(),
        P("sp", "tp"),
        P("sp", "tp"),
        P("tp", "sp"),
    )
    return jax.shard_map(
        per_device, mesh=mesh, in_specs=placed, out_specs=P(("sp", "tp"), None), check_vma=False
    )
```

```python
import functools

import jax
import jax.numpy as jnp
from jax import lax
from jax.experimental import pallas as pl
from jax.experimental.pallas import tpu as pltpu
from jax.sharding import PartitionSpec as P

f32, bf16 = jnp.float32, jnp.bfloat16
HIGH = lax.Precision.HIGHEST
MESH = pl.DeviceIdType.MESH
eps = 1e-06
NZ, NY, NC, NX = 8, 4, 2, 4
ROWS = 256
GROUPS, CHAN, STATE = 8, 16, 64
LANES = 2 * STATE
WIDE = GROUPS * LANES
LOCAL = GROUPS * CHAN
D, HID, SHARD = 2048, 1408, 32
OWN = ROWS // NX
PATH_A = ((512, 256), (640, 384))
PHASES = ((0, 2), (2, 1))
PLANES = (0, -1, 1, -2, 2, -3, 3, 4)
OPENING = ("0a0", "0b0",)
N_GROUPS, N_ARRIVALS = 19, 113
ORDER = (
    "local", "c1", "0s0", "0y0", "r0", "masked", "outmap", "1b0", "1s0", "0a1", "0s1", "0b1", "0y1", "0q01",
    "0y2", "carry", "c2", "0s2", "0f0", "0q11", "r1", "1a0", "0q31", "0f1", "1y0", "0b2", "0y3", "0d0",
    "0q02", "r2", "0f2", "0e0", "0y4", "0q21", "0d1", "far", "resp", "m", "0q12", "0q32", "0f3", "0e1",
    "0d2", "1a1", "1f0", "0b3", "0y5", "0e2", "0f4", "0q03", "0y6", "0q22", "0d3", "0q13", "proj", "0q33",
    "0f5", "0e3", "first0", "first1", "0b4", "0d4", "0y7", "first2", "first3", "0q04", "1b1", "1q01", "1s1",
    "0f6", "0q23", "0e4", "first4", "0q34", "1y1", "0d5", "0q14", "1y2", "1s2", "1d0", "1b2", "1y3", "0e5",
    "first5", "0f7", "1e0", "1q02", "0d6", "1q11", "1y4", "1q31", "0q24", "1f1", "0e6", "first6", "1q21",
    "1f2", "1f3", "1b3", "1y5", "1q03", "1y6", "0d7", "1q12", "1f4", "1q32", "1d1", "1d2", "0e7", "first7",
    "hidden", "1b4", "1q22", "1q04", "1d3", "1y7", "second0", "scat0", "1f5", "1e1", "second1", "scat1",
    "1q13", "1e2", "second2", "scat2", "1q33", "1f6", "1e3", "second3", "scat3", "1d4", "1q23", "pass0",
    "1f7", "pass1", "1d5", "1e4", "second4", "pass2", "scat4", "1q14", "1d6", "pass3", "1q34", "1e5",
    "second5", "scat5", "1q24", "1d7", "fin0", "1e6", "second6", "scat6", "fin1", "fin2", "1e7", "second7",
    "pass4", "scat7", "fin3", "pass5", "pass6", "fin4", "pass7", "fin5", "fin6", "fin7",
)


def iota(shape, dim):
    return lax.broadcasted_iota(jnp.int32, shape, dim)


def where_one(test):
    return jnp.where(test, 1.0, 0.0).astype(f32)


def nt(a, b, precision=None):
    return lax.dot_general(
        a, b, (((1,), (1,)), ((), ())), precision=precision, preferred_element_type=f32
    )


def nn(a, b, precision=None):
    return lax.dot_general(
        a, b, (((1,), (0,)), ((), ())), precision=precision, preferred_element_type=f32
    )


def swap(a):
    return pltpu.roll(a, STATE, 1)


def sign_lanes(shape):
    return jnp.where(iota(shape, 1) < STATE, -1.0, 1.0).astype(f32)


def turned(a, c, s):
    return a * c + swap(a) * s


def silu(x):
    return x * jax.nn.sigmoid(x)


def kernel(
    resid, mix_h, forget_h, decay_h, turn_h, in_re_h, in_im_h, out_re_h, out_im_h, skip_h, mix_gain_h,
    w_out, ffn_gain_h, gate, up, down_t, out,
    mix, forget_t, decay, turn, in_re, in_im, out_re, out_im, skip, mix_gain, ffn_gain,
    G, RA, WO, MX, X, RM, GA, UA, HB, PT, RS, RB, UB, YB, ST, C1, C2,
    send_sem, recv_sem, local_sem, entry_sem,
):
    me, x = lax.axis_index("sp"), lax.axis_index("tp")
    c = lax.rem(me, NC)
    y = lax.rem(lax.div(me, NC), NY)
    z = lax.div(me, NC * NY)
    slot = lax.rem(me, NC * NY)

    def at_sp(zz, yy, cc):
        return {"sp": (zz * NY + yy) * NC + cc}

    def zr(d):
        return lax.rem(z + (d + NZ), NZ)

    def yr(d):
        return lax.rem(y + (d + NY), NY)

    def xr(d):
        return lax.rem(x + (d + NX), NX)

    plane_peers = [{"sp": z * NY * NC + lax.rem(slot + d, NY * NC)} for d in range(1, NY * NC)]
    z_peers = [at_sp(zr(d), y, c) for d in range(1, NZ)]
    x_peers = [{"tp": xr(d)} for d in range(1, NX)]
    yp, ym = at_sp(z, yr(1), c), at_sp(z, yr(-1), c)
    zp, zm = at_sp(zr(1), y, c), at_sp(zr(-1), y, c)
    partner = at_sp(z, y, 1 - c)

    groups, arrivals = {}, {}

    def send(group, name, src, dst, to):
        k = groups.setdefault(group, len(groups))
        n = arrivals.setdefault(name, len(arrivals))
        pltpu.make_async_remote_copy(
            src_ref=src, dst_ref=dst, send_sem=send_sem.at[k], recv_sem=recv_sem.at[n],
            device_id=to, device_id_type=MESH,
        ).start()

    def waiter(k, n, bytes_of):
        return pltpu.make_async_remote_copy(
            src_ref=bytes_of, dst_ref=bytes_of, send_sem=send_sem.at[k], recv_sem=recv_sem.at[n],
            device_id=partner, device_id_type=MESH,
        )

    def recv(name, bytes_of):
        waiter(0, arrivals[name], bytes_of).wait_recv()

    def sent(group, bytes_of):
        waiter(groups[group], 0, bytes_of).wait_send()

    tasks, drains = {}, []

    def task(f):
        tasks[f.__name__] = f
        return f

    def gather_tasks(p):
        first, count = PHASES[p]
        cut, cut_plus = PATH_A[p]
        tiles = (HID - cut) // 128
        few, many = cut + tiles // 2 * 128, cut + (tiles - tiles // 2) * 128
        path_a, path_a1, path_a2 = (0, cut), (0, cut_plus), (cut_plus, cut)
        path_b = (cut, HID)

        def halves(odd):
            middle = many if odd else few
            return (cut, middle), (middle, HID)

        def block(dz, dy, lanes):
            return G.at[
                pl.ds(first, count), zr(dz), yr(dy), c, :, pl.ds(lanes[0], lanes[1] - lanes[0])
            ]

        def sized(planes, rows, lanes):
            return G.at[
                pl.ds(first, count), pl.ds(0, planes), pl.ds(0, rows), c, :,
                pl.ds(lanes[0], lanes[1] - lanes[0]),
            ]

        def go(name, ref, to):
            send(f"{p}{name[0]}", f"{p}{name}", ref, ref, to)

        def both(name, ref, plus, minus):
            go(name, ref, plus)
            go(name, ref, minus)

        def got(name, lanes, count_of=1):
            recv(f"{p}{name}", sized(1, count_of, lanes))

        def a0():
            both("A0", block(0, 0, path_a), yp, ym)

        def b0():
            both("B1", block(0, 0, path_b), zp, zm)

        def a1():
            got("A0", path_a, 2)
            go("A1", block(0, -1, path_a1), yp)
            go("A1", block(0, 1, path_a2), ym)

        def s0():
            both("Z01", block(0, 0, path_a), zp, zm)

        def s1():
            both("Z11", block(0, -1, path_a), zp, zm)
            both("Z31", block(0, 1, path_a), zp, zm)

        def s2():
            got("A1", path_a)
            both("Z21", block(0, 2, path_a), zp, zm)

        def q(row, s):
            dy = (0, -1, 2, 1)[row]
            got(f"Z{row}{s}", path_a, 2 if s < 4 else 1)
            if s < 3 or (s == 3 and row in (0, 1)):
                go(f"Z{row}{s + 1}", block(-s, dy, path_a), zp)
            if s < 3 or (s == 3 and row in (2, 3)):
                go(f"Z{row}{s + 1}", block(s, dy, path_a), zm)

        def b(s):
            got(f"B{s}", path_b, 2 if s < 4 else 1)
            plus, minus = (path_b, path_b) if s < 3 else halves(p)
            if s < 4:
                go(f"B{s + 1}", block(-s, 0, plus), zp)
                go(f"B{s + 1}", block(s, 0, minus), zm)

        def y_(k):
            both(f"Y{k}", block(PLANES[k], 0, path_b), yp, ym)

        def f(k):
            got(f"Y{k}", path_b, 2)
            plus, minus = halves(k % 2)
            go(f"F{k}", block(PLANES[k], -1, plus), yp)
            go(f"F{k}", block(PLANES[k], 1, minus), ym)

        def d(k):
            got(f"F{k}", path_b)
            go(f"D{k}", G.at[pl.ds(first, count), zr(PLANES[k]), :, c], partner)

        def e(k):
            recv(f"{p}D{k}", sized(1, NY, (0, HID)))

        def all_sent():
            for kind, planes, rows, lanes in (
                ("A", 1, 3, path_a), ("Z", 7, 4, path_a), ("Y", 8, 2, path_b), ("F", 8, 1, path_b),
                ("B", 7, 1, path_b), ("D", 8, 4, (0, HID)),
            ):
                sent(f"{p}{kind}", sized(planes, rows, lanes))

        drains.append(all_sent)
        for name, f_ in (("a0", a0), ("b0", b0), ("a1", a1), ("s0", s0), ("s1", s1), ("s2", s2)):
            tasks[f"{p}{name}"] = f_
        for s in range(1, 5):
            tasks[f"{p}b{s}"] = functools.partial(b, s)
            for row in range(NY):
                tasks[f"{p}q{row}{s}"] = functools.partial(q, row, s)
        for k in range(NZ):
            tasks[f"{p}y{k}"] = functools.partial(y_, k)
            tasks[f"{p}f{k}"] = functools.partial(f, k)
            tasks[f"{p}d{k}"] = functools.partial(d, k)
            tasks[f"{p}e{k}"] = functools.partial(e, k)

    for p in range(len(PHASES)):
        gather_tasks(p)

    barrier = pltpu.get_barrier_semaphore()
    peers = plane_peers + z_peers + x_peers
    for peer in peers:
        pl.semaphore_signal(barrier, inc=1, device_id=peer, device_id_type=MESH)
    small = [
        (mix_h, mix), (forget_h, forget_t), (decay_h, decay), (turn_h, turn), (in_re_h, in_re),
        (in_im_h, in_im), (out_re_h, out_re), (out_im_h, out_im), (skip_h, skip),
        (mix_gain_h, mix_gain), (ffn_gain_h, ffn_gain),
    ]
    early = [pltpu.make_async_copy(a, b, entry_sem.at[k]) for k, (a, b) in enumerate(small)]
    loads = [
        pltpu.make_async_copy(gate, G.at[0, z, y, c], local_sem.at[0]),
        pltpu.make_async_copy(up, G.at[1, z, y, c], local_sem.at[1]),
        pltpu.make_async_copy(down_t, G.at[2, z, y, c], local_sem.at[2]),
        pltpu.make_async_copy(resid, RA.at[x], local_sem.at[3]),
        pltpu.make_async_copy(w_out, WO, local_sem.at[4]),
    ]
    for load in loads[:3] + early + loads[3:]:
        load.start()

    with jax.named_scope("entry"):
        pl.semaphore_wait(barrier, len(peers))
        for load in loads[:3]:
            load.wait()
    with jax.named_scope("opening"):
        for name in OPENING:
            tasks[name]()
        for load in early:
            load.wait()
    with jax.named_scope("prep"):
        drive = mix[...]
        spread = where_one(lax.rem(iota((CHAN, LOCAL), 1), CHAN) == iota((CHAN, LOCAL), 0))
        twice = where_one(lax.rem(iota((STATE, LANES), 1), STATE) == iota((STATE, LANES), 0))
        rate2 = nn(decay[...], twice, HIGH)
        turn2 = nn(turn[...], twice, HIGH)
        lower = iota((ROWS, ROWS), 0) >= iota((ROWS, ROWS), 1)
        lower_one = where_one(lower)
        forget_rows = forget_t[...]
        run_log = nt(lower_one, forget_rows, HIGH)
        run_log_t = nt(forget_rows, lower_one, HIGH)
        w = 2.0 * rate2
        series = 1.0 + w / 6.0
        for k in (5.0, 4.0, 3.0, 2.0):
            series = 1.0 + (w / k) * series
        in_factor = jnp.sqrt(-(w * series))
        first_half = where_one(iota((STATE, LANES), 1) == iota((STATE, LANES), 0)).astype(bf16)
        second_half = where_one(
            iota((STATE, LANES), 1) == iota((STATE, LANES), 0) + STATE
        ).astype(bf16)
        row_group = lax.div(iota((LOCAL, LANES), 0), CHAN)

        def by_group(rows):
            return jnp.concatenate(
                [jnp.where(row_group == g, rows, 0.0).astype(bf16) for g in range(GROUPS)], axis=1
            )

        in_map = by_group(
            nn(in_re[...].astype(bf16), first_half) + nn(in_im[...].astype(bf16), second_half)
        )
        UB[...] = nn(drive, in_map)
        sign = sign_lanes((1, LANES))
        sign8 = sign_lanes((GROUPS, LANES))
        coarse = (iota((16, LANES), 0) - 8).astype(f32) * 16.0
        fine = iota((16, LANES), 0).astype(f32)
        centred = (iota((ROWS, LANES), 0) - ROWS // 2).astype(f32)

    def phase_tables(g):
        angle = turn2[g : g + 1]
        ca, sa = jnp.cos(angle * coarse), jnp.sin(angle * coarse)
        cb, sb = jnp.cos(angle * fine), jnp.sin(angle * fine)
        cos = [ca[k : k + 1] * cb - sa[k : k + 1] * sb for k in range(16)]
        sin = [sa[k : k + 1] * cb + ca[k : k + 1] * sb for k in range(16)]
        return jnp.concatenate(cos, axis=0), jnp.concatenate(sin, axis=0) * sign

    def power(n, log=0.0):
        size = jnp.exp(rate2 * n + log)
        return size * jnp.cos(turn2 * n), size * jnp.sin(turn2 * n) * sign8

    v = {}

    @task
    def local():
        ends = []
        last = run_log[ROWS - 1 : ROWS]
        for g in range(GROUPS):
            lanes = slice(LANES * g, LANES * (g + 1))
            cos, sin = phase_tables(g)
            grow = jnp.exp(-rate2[g : g + 1] * centred) * in_factor[g : g + 1]
            b_g = UB[:, lanes]
            u = (b_g * cos - swap(b_g) * sin) * grow
            UB[:, lanes] = u
            fall = jnp.exp(rate2[g : g + 1] * centred)
            ST[0, :, lanes] = cos * fall
            ST[1, :, lanes] = sin * fall
            weight = jnp.exp(last[:, g : g + 1] - run_log[:, g : g + 1])
            total = jnp.sum(u * weight, axis=0, keepdims=True)
            at_end = slice(ROWS - 1, ROWS)
            ends.append(turned(total, ST[0, at_end, lanes], ST[1, at_end, lanes]))
        last_col = jnp.sum(
            jnp.where(iota((GROUPS, ROWS), 1) == ROWS - 1, run_log_t, 0.0), axis=1, keepdims=True
        )
        C1[slot, 0:GROUPS] = jnp.concatenate(ends, axis=0)
        C1[slot, GROUPS:] = jnp.broadcast_to(last_col, (GROUPS, LANES))

    @task
    def c1():
        for d in range(1, NY * NC):
            send("C1", "C1", C1.at[slot], C1.at[slot], plane_peers[d - 1])

    @task
    def masked():
        for g in range(GROUPS):
            lanes = slice(LANES * g, LANES * (g + 1))
            gap = run_log[:, g : g + 1] - run_log_t[g : g + 1]
            weights = jnp.where(lower, jnp.exp(jnp.minimum(gap, 0.0)), 0.0).astype(bf16)
            YB[:, lanes] = nn(weights, UB[:, lanes].astype(bf16))

    @task
    def carry():
        c_one, s_one = power(float(ROWS))
        recv("C1", C1.at[1:])
        acc = jnp.zeros((GROUPS, LANES), f32)
        log_acc = jnp.zeros((GROUPS, LANES), f32)
        before, log_before = acc, log_acc
        for j in range(NY * NC):
            here = slot == j
            before = jnp.where(here, acc, before)
            log_before = jnp.where(here, log_acc, log_before)
            log_j = C1[j, GROUPS:]
            acc = jnp.exp(log_j) * turned(acc, c_one, s_one) + C1[j, 0:GROUPS]
            log_acc = log_acc + log_j
        C2[z, 0:GROUPS] = acc
        C2[z, GROUPS:] = log_acc
        v["before"], v["log_before"] = before, log_before

    @task
    def c2():
        for d in range(1, NZ):
            send("C2", "C2", C2.at[z], C2.at[z], z_peers[d - 1])

    @task
    def outmap():
        v["out_map"] = by_group(
            nn(out_re[...].astype(bf16), first_half) - nn(out_im[...].astype(bf16), second_half)
        )
        skip_rows = nn(skip[...], spread, HIGH)
        in_group = lax.div(iota((GROUPS, LOCAL), 1), CHAN) == iota((GROUPS, LOCAL), 0)
        v["skip_row"] = jnp.sum(jnp.where(in_group, skip_rows, 0.0), axis=0, keepdims=True)

    @task
    def far():
        c_plane, s_plane = power(float(ROWS * NY * NC))
        c_in, s_in = power(slot.astype(f32) * float(ROWS), v["log_before"])
        c_mid, s_mid = power(float(ROWS // 2 + 1))
        recv("C2", C2.at[1:])
        total = jnp.zeros((GROUPS, LANES), f32)
        for j in range(NZ):
            step_on = jnp.exp(C2[j, GROUPS:]) * turned(total, c_plane, s_plane) + C2[j, 0:GROUPS]
            total = jnp.where(j < z, step_on, total)
        v["carry"] = turned(v["before"] + turned(total, c_in, s_in), c_mid, s_mid)

    @task
    def resp():
        for g in range(GROUPS):
            lanes = slice(LANES * g, LANES * (g + 1))
            full = YB[:, lanes] + jnp.exp(run_log[:, g : g + 1]) * v["carry"][g : g + 1]
            YB[:, lanes] = turned(full, ST[0, :, lanes], ST[1, :, lanes])
        response = nt(YB[...].astype(bf16), v["out_map"]) + v["skip_row"] * drive.astype(f32)
        MX[x] = jax.nn.gelu(response).astype(bf16)

    @task
    def m():
        for d in range(1, NX):
            send("M", "M", MX.at[x], MX.at[x], x_peers[d - 1])

    half = OWN // 2

    @task
    def r0():
        loads[3].wait()
        send("R", "R", RA.at[x], RA.at[x], x_peers[0])
        send("R", "R", RA.at[x], RA.at[x], x_peers[2])

    @task
    def r1():
        recv("R", RA.at[2:])
        send("Q", "Q", RA.at[xr(-1), 0:half], RA.at[xr(-1), 0:half], x_peers[0])
        send("Q", "Q", RA.at[xr(1), half:], RA.at[xr(1), half:], x_peers[2])

    @task
    def r2():
        recv("Q", RA.at[0])
        loads[4].wait()

    @task
    def proj():
        recv("M", MX.at[1:])
        mixed = [MX[q].astype(f32) for q in range(NX)]
        total = sum(jnp.sum(m * m, axis=1, keepdims=True) for m in mixed)
        scale = lax.rsqrt(total / float(LOCAL * NX) + eps)
        gains = mix_gain[...]
        normed = jnp.concatenate(
            [
                (mixed[q] * scale * gains[:, LOCAL * q : LOCAL * (q + 1)]).astype(bf16)
                for q in range(NX)
            ],
            axis=1,
        )
        squares = jnp.zeros((ROWS, 1), f32)
        for k in range(4):
            lanes = slice(512 * k, 512 * (k + 1))
            piece = nn(normed, WO[:, lanes]) + RA[:, :, lanes].reshape(ROWS, 512).astype(f32)
            RM[:, lanes] = piece
            squares = squares + jnp.sum(piece * piece, axis=1, keepdims=True)
        scale = lax.rsqrt(squares / float(D) + eps)
        for k in range(4):
            lanes = slice(512 * k, 512 * (k + 1))
            X[:, lanes] = (RM[:, lanes] * scale * ffn_gain[:, lanes]).astype(bf16)

    def column_slice(k):
        return pl.ds(pl.multiple_of(zr(PLANES[k]) * ROWS, ROWS), ROWS)

    def first(k):
        piece = X[:, column_slice(k)]
        for m, store in ((0, GA), (1, UA)):
            product = nn(piece, G[m, zr(PLANES[k])].reshape(ROWS, HID))
            store[...] = product if k == 0 else store[...] + product

    @task
    def hidden():
        HB[...] = (silu(GA[...]) * UA[...]).astype(bf16)

    def second(k):
        part = nt(HB[...], G[2, zr(PLANES[k])].reshape(ROWS, HID))
        PT[:, :, column_slice(k)] = part.astype(bf16).reshape(NX, OWN, ROWS)

    def part_slice(k, side):
        return pl.ds(pl.multiple_of(zr(PLANES[k]) * ROWS + 128 * side, 128), 128)

    def scat(k):
        for side, to in ((0, x_peers[0]), (1, x_peers[2])):
            send("S", f"S{k}", PT.at[xr(2), :, part_slice(k, side)], RB.at[k, side], to)

    def pass_(k):
        recv(f"S{k}", RB.at[k])
        cols = column_slice(k)
        for side, dx in ((0, 1), (1, -1)):
            lanes = part_slice(k, side)
            sum_ = PT[xr(dx), :, lanes].astype(f32) + RB[k, side].astype(f32)
            PT[xr(dx), :, lanes] = sum_.astype(bf16)
        send("V", f"V{k}", PT.at[xr(1), :, cols], RS.at[0, :, cols], x_peers[0])
        send("V", f"V{k}", PT.at[xr(-1), :, cols], RS.at[1, :, cols], x_peers[2])

    def fin(k):
        cols = column_slice(k)
        recv(f"V{k}", RS.at[:, :, 0:ROWS])
        ffn = PT[x, :, cols].astype(f32) + RS[0, :, cols].astype(f32) + RS[1, :, cols].astype(f32)
        kept = RM[pl.ds(pl.multiple_of(x * OWN, OWN), OWN), cols]
        out[:, cols] = (kept + 0.5 * ffn).astype(bf16)

    for k in range(NZ):
        tasks[f"first{k}"] = functools.partial(first, k)
        tasks[f"second{k}"] = functools.partial(second, k)
        tasks[f"scat{k}"] = functools.partial(scat, k)
        tasks[f"pass{k}"] = functools.partial(pass_, k)
        tasks[f"fin{k}"] = functools.partial(fin, k)

    for name in ORDER:
        with jax.named_scope(name):
            tasks[name]()
    with jax.named_scope("drain"):
        assert (len(groups), len(arrivals)) == (N_GROUPS, N_ARRIVALS)
        for drain in drains:
            drain()
        sent("C1", C1.at[1:])
        sent("C2", C2.at[1:])
        sent("M", MX.at[1:])
        sent("R", RA.at[2:])
        sent("Q", RA.at[0])
        sent("S", RB)
        sent("V", RS)


def per_device(
    resid, mix_in, decay_rate, turn_rate, forget, input_real, input_imag, output_real, output_imag,
    skip_gain, mix_gain, w_out, ffn_gain, gating_matrix, w_up, w_down,
):
    operands = (
        resid, mix_in, forget.T, decay_rate, turn_rate,
        input_real.transpose(0, 2, 1).reshape(-1, STATE),
        input_imag.transpose(0, 2, 1).reshape(-1, STATE),
        output_real.reshape(-1, STATE), output_imag.reshape(-1, STATE),
        skip_gain, mix_gain.reshape(1, -1), w_out, ffn_gain.reshape(1, -1),
        gating_matrix, w_up, w_down.T,
    )
    own = [pltpu.VMEM(operands[k].shape, operands[k].dtype) for k in (*range(1, 11), 12)]
    return pl.pallas_call(
        kernel,
        out_shape=jax.ShapeDtypeStruct((OWN, D), bf16),
        in_specs=[pl.BlockSpec(memory_space=pl.ANY)] * len(operands),
        out_specs=pl.BlockSpec(memory_space=pltpu.VMEM),
        scratch_shapes=own + [
            pltpu.VMEM((3, NZ, NY, NC, SHARD, HID), bf16),
            pltpu.VMEM((NX, OWN, D), bf16),
            pltpu.VMEM((LOCAL * NX, D), bf16),
            pltpu.VMEM((NX, ROWS, LOCAL), bf16),
            pltpu.VMEM((ROWS, D), bf16),
            pltpu.VMEM((ROWS, D), f32),
            pltpu.VMEM((ROWS, HID), f32),
            pltpu.VMEM((ROWS, HID), f32),
            pltpu.VMEM((ROWS, HID), bf16),
            pltpu.VMEM((NX, OWN, D), bf16),
            pltpu.VMEM((2, OWN, D), bf16),
            pltpu.VMEM((NZ, 2, OWN, 128), bf16),
            pltpu.VMEM((ROWS, WIDE), f32),
            pltpu.VMEM((ROWS, WIDE), f32),
            pltpu.VMEM((2, ROWS, WIDE), f32),
            pltpu.VMEM((NY * NC, 2 * GROUPS, LANES), f32),
            pltpu.VMEM((NZ, 2 * GROUPS, LANES), f32),
            pltpu.SemaphoreType.DMA((N_GROUPS,)),
            pltpu.SemaphoreType.DMA((N_ARRIVALS,)),
            pltpu.SemaphoreType.DMA((5,)),
            pltpu.SemaphoreType.DMA((len(own),)),
        ],
        compiler_params=pltpu.CompilerParams(
            collective_id=0, has_side_effects=True, vmem_limit_bytes=60 * 1024 * 1024
        ),
    )(*operands)


def solution(mesh):
    placed = (
        P(("sp", "tp"), None),
        P("sp", "tp"),
        P("tp", None),
        P("tp", None),
        P("sp", "tp"),
        P("tp", None, None),
        P("tp", None, None),
        P("tp", None, None),
        P("tp", None, None),
        P("tp", None),
        P(),
        P(),
        P(),
        P("sp", "tp"),
        P("sp", "tp"),
        P("tp", "sp"),
    )
    return jax.shard_map(
        per_device, mesh=mesh, in_specs=placed, out_specs=P(("sp", "tp"), None), check_vma=False
    )
```

```python
import functools

import jax
import jax.numpy as jnp
from jax import lax
from jax.experimental import pallas as pl
from jax.experimental.pallas import tpu as pltpu
from jax.sharding import PartitionSpec as P

f32, bf16 = jnp.float32, jnp.bfloat16
HIGH = lax.Precision.HIGHEST
MESH = pl.DeviceIdType.MESH
eps = 1e-06
NZ, NY, NC, NX = 8, 4, 2, 4
ROWS = 256
GROUPS, CHAN, STATE = 8, 16, 64
LANES = 2 * STATE
WIDE = GROUPS * LANES
LOCAL = GROUPS * CHAN
D, HID, SHARD = 2048, 1408, 32
OWN = ROWS // NX
PATH_A = ((512, 256), (640, 384))
PHASES = ((0, 2), (2, 1))
PLANES = (0, -1, 1, -2, 2, -3, 3, 4)
OPENING = ("0a0", "1a0", "0b0", "1s0", "1y0",)
DIRECT = ()
N_GROUPS, N_ARRIVALS = 19, 113
ORDER = (
    "r0", "local", "c1", "1b0", "outmap", "0s0", "masked", "0y0", "0a1", "0s1", "0b1", "0y2", "0y1",
    "carry", "c2", "r1", "0f0", "0s2", "0q11", "0q31", "0f2", "0b2", "0y4", "r2", "0y3", "0f1", "0d0",
    "0q21", "far", "0e0", "0q12", "resp", "m", "0q01", "0d2", "0f4", "0q32", "1f0", "0b3", "0y5", "0y6",
    "0e2", "0q22", "0f3", "0d1", "0q13", "0e1", "0q02", "0d4", "0q33", "proj", "0e4", "1a1", "0f5", "0b4",
    "1q01", "first0", "first1", "first4", "0y7", "first2", "0q23", "1b1", "1y1", "0q14", "0d3", "1s2",
    "1d0", "0q34", "0q03", "1y2", "0d5", "0e3", "first3", "1e0", "1s1", "0q24", "0f6", "0e5", "first5",
    "0f7", "1b2", "1y3", "1f1", "1q21", "0q04", "1q11", "1f2", "1q31", "0d6", "1y4", "1b3", "1y5", "0d7",
    "1q02", "1y6", "0e6", "first6", "1q12", "1f3", "1d1", "1q22", "1d2", "1q32", "0e7", "first7", "1b4",
    "1y7", "hidden", "second0", "1e1", "1q03", "scat0", "second1", "scat1", "1f5", "1e2", "second2",
    "scat2", "1q13", "1f4", "1q23", "1f6", "1d3", "1q33", "pass0", "1f7", "1q04", "pass1", "1d5", "1e3",
    "second3", "scat3", "1d4", "1q14", "pass2", "1q24", "1d6", "1e5", "second5", "scat5", "1q34", "1d7",
    "1e4", "second4", "fin0", "scat4", "1e6", "second6", "scat6", "fin1", "pass3", "1e7", "second7", "fin2",
    "scat7", "pass5", "pass4", "pass6", "fin3", "pass7", "fin5", "fin4", "fin6", "fin7",
)


def iota(shape, dim):
    return lax.broadcasted_iota(jnp.int32, shape, dim)


def where_one(test):
    return jnp.where(test, 1.0, 0.0).astype(f32)


def nt(a, b, precision=None):
    return lax.dot_general(
        a, b, (((1,), (1,)), ((), ())), precision=precision, preferred_element_type=f32
    )


def nn(a, b, precision=None):
    return lax.dot_general(
        a, b, (((1,), (0,)), ((), ())), precision=precision, preferred_element_type=f32
    )


def swap(a):
    return pltpu.roll(a, STATE, 1)


def sign_lanes(shape):
    return jnp.where(iota(shape, 1) < STATE, -1.0, 1.0).astype(f32)


def turned(a, c, s):
    return a * c + swap(a) * s


def silu(x):
    return x * jax.nn.sigmoid(x)


def kernel(
    resid, mix_h, forget_h, decay_h, turn_h, in_re_h, in_im_h, out_re_h, out_im_h, skip_h, mix_gain_h,
    w_out, ffn_gain_h, gate, up, down_t, out,
    mix, forget_t, decay, turn, in_re, in_im, out_re, out_im, skip, mix_gain, ffn_gain,
    G, RA, WO, MX, X, RM, GA, UA, HB, PT, RS, RB, RT, OB, UB, YB, ST, C1, C2,
    send_sem, recv_sem, local_sem, entry_sem, out_sem,
):
    me, x = lax.axis_index("sp"), lax.axis_index("tp")
    c = lax.rem(me, NC)
    y = lax.rem(lax.div(me, NC), NY)
    z = lax.div(me, NC * NY)
    slot = lax.rem(me, NC * NY)

    def at_sp(zz, yy, cc):
        return {"sp": (zz * NY + yy) * NC + cc}

    def zr(d):
        return lax.rem(z + (d + NZ), NZ)

    def yr(d):
        return lax.rem(y + (d + NY), NY)

    def xr(d):
        return lax.rem(x + (d + NX), NX)

    plane_peers = [{"sp": z * NY * NC + lax.rem(slot + d, NY * NC)} for d in range(1, NY * NC)]
    z_peers = [at_sp(zr(d), y, c) for d in range(1, NZ)]
    x_peers = [{"tp": xr(d)} for d in range(1, NX)]
    yp, ym = at_sp(z, yr(1), c), at_sp(z, yr(-1), c)
    zp, zm = at_sp(zr(1), y, c), at_sp(zr(-1), y, c)
    partner = at_sp(z, y, 1 - c)

    groups, arrivals = {}, {}

    def send(group, name, src, dst, to):
        k = groups.setdefault(group, len(groups))
        n = arrivals.setdefault(name, len(arrivals))
        pltpu.make_async_remote_copy(
            src_ref=src, dst_ref=dst, send_sem=send_sem.at[k], recv_sem=recv_sem.at[n],
            device_id=to, device_id_type=MESH,
        ).start()

    def waiter(k, n, bytes_of):
        return pltpu.make_async_remote_copy(
            src_ref=bytes_of, dst_ref=bytes_of, send_sem=send_sem.at[k], recv_sem=recv_sem.at[n],
            device_id=partner, device_id_type=MESH,
        )

    def recv(name, bytes_of):
        waiter(0, arrivals[name], bytes_of).wait_recv()

    def sent(group, bytes_of):
        waiter(groups[group], 0, bytes_of).wait_send()

    tasks, drains, stores = {}, [], []

    def task(f):
        tasks[f.__name__] = f
        return f

    def gather_tasks(p):
        first, count = PHASES[p]
        cut, cut_plus = PATH_A[p]
        tiles = (HID - cut) // 128
        few, many = cut + tiles // 2 * 128, cut + (tiles - tiles // 2) * 128
        path_a, path_a1, path_a2 = (0, cut), (0, cut_plus), (cut_plus, cut)
        path_b = (cut, HID)

        def halves(odd):
            middle = many if odd else few
            return (cut, middle), (middle, HID)

        def block(dz, dy, lanes):
            return G.at[
                pl.ds(first, count), zr(dz), yr(dy), c, :, pl.ds(lanes[0], lanes[1] - lanes[0])
            ]

        def sized(planes, rows, lanes):
            return G.at[
                pl.ds(first, count), pl.ds(0, planes), pl.ds(0, rows), c, :,
                pl.ds(lanes[0], lanes[1] - lanes[0]),
            ]

        def go(name, ref, to):
            send(f"{p}{name[0]}", f"{p}{name}", ref, ref, to)

        def both(name, ref, plus, minus):
            go(name, ref, plus)
            go(name, ref, minus)

        def got(name, lanes, count_of=1):
            recv(f"{p}{name}", sized(1, count_of, lanes))

        def a0():
            both("A0", block(0, 0, path_a), yp, ym)

        def b0():
            both("B1", block(0, 0, path_b), zp, zm)

        def a1():
            got("A0", path_a, 2)
            go("A1", block(0, -1, path_a1), yp)
            go("A1", block(0, 1, path_a2), ym)

        def s0():
            both("Z01", block(0, 0, path_a), zp, zm)

        def s1():
            both("Z11", block(0, -1, path_a), zp, zm)
            both("Z31", block(0, 1, path_a), zp, zm)

        def s2():
            got("A1", path_a)
            both("Z21", block(0, 2, path_a), zp, zm)

        def q(row, s):
            dy = (0, -1, 2, 1)[row]
            got(f"Z{row}{s}", path_a, 2 if s < 4 else 1)
            if s < 3 or (s == 3 and row in (0, 1)):
                go(f"Z{row}{s + 1}", block(-s, dy, path_a), zp)
            if s < 3 or (s == 3 and row in (2, 3)):
                go(f"Z{row}{s + 1}", block(s, dy, path_a), zm)

        def b(s):
            got(f"B{s}", path_b, 2 if s < 4 else 1)
            plus, minus = (path_b, path_b) if s < 3 else halves(p)
            if s < 4:
                go(f"B{s + 1}", block(-s, 0, plus), zp)
                go(f"B{s + 1}", block(s, 0, minus), zm)

        def y_(k):
            both(f"Y{k}", block(PLANES[k], 0, path_b), yp, ym)

        def f(k):
            got(f"Y{k}", path_b, 2)
            plus, minus = halves(k % 2)
            go(f"F{k}", block(PLANES[k], -1, plus), yp)
            go(f"F{k}", block(PLANES[k], 1, minus), ym)

        def d(k):
            got(f"F{k}", path_b)
            go(f"D{k}", G.at[pl.ds(first, count), zr(PLANES[k]), :, c], partner)

        def e(k):
            recv(f"{p}D{k}", sized(1, NY, (0, HID)))

        def all_sent():
            for kind, planes, rows, lanes in (
                ("A", 1, 3, path_a), ("Z", 7, 4, path_a), ("Y", 8, 2, path_b), ("F", 8, 1, path_b),
                ("B", 7, 1, path_b), ("D", 8, 4, (0, HID)),
            ):
                sent(f"{p}{kind}", sized(planes, rows, lanes))

        drains.append(all_sent)
        for name, f_ in (("a0", a0), ("b0", b0), ("a1", a1), ("s0", s0), ("s1", s1), ("s2", s2)):
            tasks[f"{p}{name}"] = f_
        for s in range(1, 5):
            tasks[f"{p}b{s}"] = functools.partial(b, s)
            for row in range(NY):
                tasks[f"{p}q{row}{s}"] = functools.partial(q, row, s)
        for k in range(NZ):
            tasks[f"{p}y{k}"] = functools.partial(y_, k)
            tasks[f"{p}f{k}"] = functools.partial(f, k)
            tasks[f"{p}d{k}"] = functools.partial(d, k)
            tasks[f"{p}e{k}"] = functools.partial(e, k)

    for p in range(len(PHASES)):
        gather_tasks(p)

    barrier = pltpu.get_barrier_semaphore()
    peers = plane_peers + z_peers + x_peers
    for peer in peers:
        pl.semaphore_signal(barrier, inc=1, device_id=peer, device_id_type=MESH)
    small = [
        (mix_h, mix), (forget_h, forget_t), (decay_h, decay), (turn_h, turn), (in_re_h, in_re),
        (in_im_h, in_im), (out_re_h, out_re), (out_im_h, out_im), (skip_h, skip),
        (mix_gain_h, mix_gain), (ffn_gain_h, ffn_gain),
    ]
    early = [pltpu.make_async_copy(a, b, entry_sem.at[k]) for k, (a, b) in enumerate(small)]
    loads = [
        pltpu.make_async_copy(gate, G.at[0, z, y, c], local_sem.at[0]),
        pltpu.make_async_copy(up, G.at[1, z, y, c], local_sem.at[1]),
        pltpu.make_async_copy(down_t, G.at[2, z, y, c], local_sem.at[2]),
        pltpu.make_async_copy(resid, RA.at[x], local_sem.at[3]),
        pltpu.make_async_copy(w_out, WO, local_sem.at[4]),
    ]
    for load in loads[:3] + early + loads[3:]:
        load.start()

    with jax.named_scope("entry"):
        pl.semaphore_wait(barrier, len(peers))
        for load in loads[:3]:
            load.wait()
    with jax.named_scope("opening"):
        for name in OPENING:
            tasks[name]()
        for load in early:
            load.wait()
    with jax.named_scope("prep"):
        drive = mix[...]
        spread = where_one(lax.rem(iota((CHAN, LOCAL), 1), CHAN) == iota((CHAN, LOCAL), 0))
        twice = where_one(lax.rem(iota((STATE, LANES), 1), STATE) == iota((STATE, LANES), 0))
        rate2 = nn(decay[...], twice, HIGH)
        turn2 = nn(turn[...], twice, HIGH)
        lower = iota((ROWS, ROWS), 0) >= iota((ROWS, ROWS), 1)
        lower_one = where_one(lower)
        forget_rows = forget_t[...]
        run_log = nt(lower_one, forget_rows, HIGH)
        run_log_t = nt(forget_rows, lower_one, HIGH)
        w = 2.0 * rate2
        series = 1.0 + w / 6.0
        for k in (5.0, 4.0, 3.0, 2.0):
            series = 1.0 + (w / k) * series
        in_factor = jnp.sqrt(-(w * series))
        first_half = where_one(iota((STATE, LANES), 1) == iota((STATE, LANES), 0)).astype(bf16)
        second_half = where_one(
            iota((STATE, LANES), 1) == iota((STATE, LANES), 0) + STATE
        ).astype(bf16)
        row_group = lax.div(iota((LOCAL, LANES), 0), CHAN)

        def by_group(rows):
            return jnp.concatenate(
                [jnp.where(row_group == g, rows, 0.0).astype(bf16) for g in range(GROUPS)], axis=1
            )

        in_map = by_group(
            nn(in_re[...].astype(bf16), first_half) + nn(in_im[...].astype(bf16), second_half)
        )
        UB[...] = nn(drive, in_map)
        sign = sign_lanes((1, LANES))
        sign8 = sign_lanes((GROUPS, LANES))
        coarse = (iota((16, LANES), 0) - 8).astype(f32) * 16.0
        fine = iota((16, LANES), 0).astype(f32)
        centred = (iota((ROWS, LANES), 0) - ROWS // 2).astype(f32)

    def phase_tables(g):
        angle = turn2[g : g + 1]
        ca, sa = jnp.cos(angle * coarse), jnp.sin(angle * coarse)
        cb, sb = jnp.cos(angle * fine), jnp.sin(angle * fine)
        cos = [ca[k : k + 1] * cb - sa[k : k + 1] * sb for k in range(16)]
        sin = [sa[k : k + 1] * cb + ca[k : k + 1] * sb for k in range(16)]
        return jnp.concatenate(cos, axis=0), jnp.concatenate(sin, axis=0) * sign

    def power(n, log=0.0):
        size = jnp.exp(rate2 * n + log)
        return size * jnp.cos(turn2 * n), size * jnp.sin(turn2 * n) * sign8

    v = {}
    on_diagonal = iota((GROUPS, LANES), 0) == iota((GROUPS, LANES), 1)

    def as_row(column):
        return jnp.sum(jnp.where(on_diagonal, column, 0.0), axis=0, keepdims=True)

    def as_column(row):
        return jnp.sum(jnp.where(on_diagonal, row, 0.0), axis=1, keepdims=True)

    @task
    def local():
        ends = []
        last = run_log[ROWS - 1 : ROWS]
        for g in range(GROUPS):
            lanes = slice(LANES * g, LANES * (g + 1))
            cos, sin = phase_tables(g)
            grow = jnp.exp(-rate2[g : g + 1] * centred) * in_factor[g : g + 1]
            b_g = UB[:, lanes]
            u = (b_g * cos - swap(b_g) * sin) * grow
            UB[:, lanes] = u
            fall = jnp.exp(rate2[g : g + 1] * centred)
            ST[0, :, lanes] = cos * fall
            ST[1, :, lanes] = sin * fall
            weight = jnp.exp(last[:, g : g + 1] - run_log[:, g : g + 1])
            total = jnp.sum(u * weight, axis=0, keepdims=True)
            at_end = slice(ROWS - 1, ROWS)
            ends.append(turned(total, ST[0, at_end, lanes], ST[1, at_end, lanes]))
        last_col = jnp.sum(
            jnp.where(iota((GROUPS, ROWS), 1) == ROWS - 1, run_log_t, 0.0), axis=1, keepdims=True
        )
        C1[slot, 0:GROUPS] = jnp.concatenate(ends, axis=0)
        C1[slot, GROUPS:] = as_row(last_col)

    @task
    def c1():
        for d in range(1, NY * NC):
            send("C1", "C1", C1.at[slot], C1.at[slot], plane_peers[d - 1])

    @task
    def masked():
        for g in range(GROUPS):
            lanes = slice(LANES * g, LANES * (g + 1))
            gap = run_log[:, g : g + 1] - run_log_t[g : g + 1]
            weights = jnp.where(lower, jnp.exp(jnp.minimum(gap, 0.0)), 0.0).astype(bf16)
            YB[:, lanes] = nn(weights, UB[:, lanes].astype(bf16))

    @task
    def carry():
        c_one, s_one = power(float(ROWS))
        recv("C1", C1.at[1:])
        acc = jnp.zeros((GROUPS, LANES), f32)
        log_acc = jnp.zeros((GROUPS, 1), f32)
        before, log_before = acc, log_acc
        for j in range(NY * NC):
            here = slot == j
            before = jnp.where(here, acc, before)
            log_before = jnp.where(here, log_acc, log_before)
            log_j = as_column(C1[j, GROUPS:])
            acc = jnp.exp(log_j) * turned(acc, c_one, s_one) + C1[j, 0:GROUPS]
            log_acc = log_acc + log_j
        C2[z, 0:GROUPS] = acc
        C2[z, GROUPS:] = as_row(log_acc)
        v["before"], v["log_before"] = before, log_before

    @task
    def c2():
        for d in range(1, NZ):
            send("C2", "C2", C2.at[z], C2.at[z], z_peers[d - 1])

    @task
    def outmap():
        v["out_map"] = by_group(
            nn(out_re[...].astype(bf16), first_half) - nn(out_im[...].astype(bf16), second_half)
        )
        skip_rows = nn(skip[...], spread, HIGH)
        in_group = lax.div(iota((GROUPS, LOCAL), 1), CHAN) == iota((GROUPS, LOCAL), 0)
        v["skip_row"] = jnp.sum(jnp.where(in_group, skip_rows, 0.0), axis=0, keepdims=True)

    @task
    def far():
        c_plane, s_plane = power(float(ROWS * NY * NC))
        c_in, s_in = power(slot.astype(f32) * float(ROWS), v["log_before"])
        c_mid, s_mid = power(float(ROWS // 2 + 1))
        recv("C2", C2.at[1:])
        total = jnp.zeros((GROUPS, LANES), f32)
        for j in range(NZ):
            fade = jnp.exp(as_column(C2[j, GROUPS:]))
            step_on = fade * turned(total, c_plane, s_plane) + C2[j, 0:GROUPS]
            total = jnp.where(j < z, step_on, total)
        v["carry"] = turned(v["before"] + turned(total, c_in, s_in), c_mid, s_mid)

    @task
    def resp():
        for g in range(GROUPS):
            lanes = slice(LANES * g, LANES * (g + 1))
            full = YB[:, lanes] + jnp.exp(run_log[:, g : g + 1]) * v["carry"][g : g + 1]
            YB[:, lanes] = turned(full, ST[0, :, lanes], ST[1, :, lanes])
        response = nt(YB[...].astype(bf16), v["out_map"]) + v["skip_row"] * drive.astype(f32)
        MX[x] = jax.nn.gelu(response).astype(bf16)

    @task
    def m():
        for d in range(1, NX):
            send("M", "M", MX.at[x], MX.at[x], x_peers[d - 1])

    half = OWN // 2

    @task
    def r0():
        loads[3].wait()
        send("R", "R", RA.at[x], RA.at[x], x_peers[0])
        send("R", "R", RA.at[x], RA.at[x], x_peers[2])

    @task
    def r1():
        recv("R", RA.at[2:])
        send("Q", "Q", RA.at[xr(-1), 0:half], RA.at[xr(-1), 0:half], x_peers[0])
        send("Q", "Q", RA.at[xr(1), half:], RA.at[xr(1), half:], x_peers[2])

    @task
    def r2():
        recv("Q", RA.at[0])
        loads[4].wait()

    @task
    def proj():
        recv("M", MX.at[1:])
        mixed = [MX[q].astype(f32) for q in range(NX)]
        total = sum(jnp.sum(m * m, axis=1, keepdims=True) for m in mixed)
        scale = lax.rsqrt(total / float(LOCAL * NX) + eps)
        gains = mix_gain[...]
        normed = jnp.concatenate(
            [
                (mixed[q] * scale * gains[:, LOCAL * q : LOCAL * (q + 1)]).astype(bf16)
                for q in range(NX)
            ],
            axis=1,
        )
        squares = jnp.zeros((ROWS, 1), f32)
        for k in range(4):
            lanes = slice(512 * k, 512 * (k + 1))
            piece = nn(normed, WO[:, lanes]) + RA[:, :, lanes].reshape(ROWS, 512).astype(f32)
            RM[:, lanes] = piece
            squares = squares + jnp.sum(piece * piece, axis=1, keepdims=True)
        scale = lax.rsqrt(squares / float(D) + eps)
        for k in range(4):
            lanes = slice(512 * k, 512 * (k + 1))
            X[:, lanes] = (RM[:, lanes] * scale * ffn_gain[:, lanes]).astype(bf16)

    def column_slice(k):
        return pl.ds(pl.multiple_of(zr(PLANES[k]) * ROWS, ROWS), ROWS)

    def first(k):
        piece = X[:, column_slice(k)]
        for m, store in ((0, GA), (1, UA)):
            product = nn(piece, G[m, zr(PLANES[k])].reshape(ROWS, HID))
            store[...] = product if k == 0 else store[...] + product

    @task
    def hidden():
        HB[...] = (silu(GA[...]) * UA[...]).astype(bf16)

    def second(k):
        part = nt(HB[...], G[2, zr(PLANES[k])].reshape(ROWS, HID))
        PT[:, :, column_slice(k)] = part.astype(bf16).reshape(NX, OWN, ROWS)

    def part_slice(k, side):
        return pl.ds(pl.multiple_of(zr(PLANES[k]) * ROWS + 128 * side, 128), 128)

    def scat(k):
        if k in DIRECT:
            cols = column_slice(k)
            for d in (2, 1, 3):
                send("T", f"S{k}", PT.at[xr(d), :, cols], RT.at[DIRECT.index(k), x], x_peers[d - 1])
            return
        for side, to in ((0, x_peers[0]), (1, x_peers[2])):
            send("S", f"S{k}", PT.at[xr(2), :, part_slice(k, side)], RB.at[k, side], to)

    def pass_(k):
        recv(f"S{k}", RB.at[k])
        cols = column_slice(k)
        for side, dx in ((0, 1), (1, -1)):
            lanes = part_slice(k, side)
            sum_ = PT[xr(dx), :, lanes].astype(f32) + RB[k, side].astype(f32)
            PT[xr(dx), :, lanes] = sum_.astype(bf16)
        send("V", f"V{k}", PT.at[xr(1), :, cols], RS.at[0, :, cols], x_peers[0])
        send("V", f"V{k}", PT.at[xr(-1), :, cols], RS.at[1, :, cols], x_peers[2])

    def fin(k):
        cols = column_slice(k)
        ffn = PT[x, :, cols].astype(f32)
        if k in DIRECT:
            n = DIRECT.index(k)
            recv(f"S{k}", RT.at[n, 1:])
            for d in range(1, NX):
                ffn = ffn + RT[n, xr(d)].astype(f32)
        else:
            recv(f"V{k}", RS.at[:, :, 0:ROWS])
            ffn = ffn + RS[0, :, cols].astype(f32) + RS[1, :, cols].astype(f32)
        kept = RM[pl.ds(pl.multiple_of(x * OWN, OWN), OWN), cols]
        OB[:, cols] = (kept + 0.5 * ffn).astype(bf16)
        copy = pltpu.make_async_copy(OB.at[:, cols], out.at[:, cols], out_sem.at[k])
        copy.start()
        stores.append(copy)

    for k in range(NZ):
        tasks[f"first{k}"] = functools.partial(first, k)
        tasks[f"second{k}"] = functools.partial(second, k)
        tasks[f"scat{k}"] = functools.partial(scat, k)
        tasks[f"pass{k}"] = functools.partial(pass_, k)
        tasks[f"fin{k}"] = functools.partial(fin, k)

    for name in ORDER:
        with jax.named_scope(name):
            tasks[name]()
    with jax.named_scope("drain"):
        assert (len(groups), len(arrivals)) == (N_GROUPS, N_ARRIVALS)
        for drain in drains:
            drain()
        sent("C1", C1.at[1:])
        sent("C2", C2.at[1:])
        sent("M", MX.at[1:])
        sent("R", RA.at[2:])
        sent("Q", RA.at[0])
        stages = NZ - len(DIRECT)
        sent("S", RB.at[0:stages])
        sent("V", RS.at[:, :, 0 : stages * ROWS])
        if DIRECT:
            sent("T", RT.at[:, 1:])
        for store in stores:
            store.wait()


def per_device(
    resid, mix_in, decay_rate, turn_rate, forget, input_real, input_imag, output_real, output_imag,
    skip_gain, mix_gain, w_out, ffn_gain, gating_matrix, w_up, w_down,
):
    operands = (
        resid, mix_in, forget.T, decay_rate, turn_rate,
        input_real.transpose(0, 2, 1).reshape(-1, STATE),
        input_imag.transpose(0, 2, 1).reshape(-1, STATE),
        output_real.reshape(-1, STATE), output_imag.reshape(-1, STATE),
        skip_gain, mix_gain.reshape(1, -1), w_out, ffn_gain.reshape(1, -1),
        gating_matrix, w_up, w_down.T,
    )
    own = [pltpu.VMEM(operands[k].shape, operands[k].dtype) for k in (*range(1, 11), 12)]
    return pl.pallas_call(
        kernel,
        out_shape=jax.ShapeDtypeStruct((OWN, D), bf16),
        in_specs=[pl.BlockSpec(memory_space=pl.ANY)] * len(operands),
        out_specs=pl.BlockSpec(memory_space=pl.ANY),
        scratch_shapes=own + [
            pltpu.VMEM((3, NZ, NY, NC, SHARD, HID), bf16),
            pltpu.VMEM((NX, OWN, D), bf16),
            pltpu.VMEM((LOCAL * NX, D), bf16),
            pltpu.VMEM((NX, ROWS, LOCAL), bf16),
            pltpu.VMEM((ROWS, D), bf16),
            pltpu.VMEM((ROWS, D), f32),
            pltpu.VMEM((ROWS, HID), f32),
            pltpu.VMEM((ROWS, HID), f32),
            pltpu.VMEM((ROWS, HID), bf16),
            pltpu.VMEM((NX, OWN, D), bf16),
            pltpu.VMEM((2, OWN, D), bf16),
            pltpu.VMEM((NZ, 2, OWN, 128), bf16),
            pltpu.VMEM((max(len(DIRECT), 1), NX, OWN, ROWS), bf16),
            pltpu.VMEM((OWN, D), bf16),
            pltpu.VMEM((ROWS, WIDE), f32),
            pltpu.VMEM((ROWS, WIDE), f32),
            pltpu.VMEM((2, ROWS, WIDE), f32),
            pltpu.VMEM((NY * NC, GROUPS + 1, LANES), f32),
            pltpu.VMEM((NZ, GROUPS + 1, LANES), f32),
            pltpu.SemaphoreType.DMA((N_GROUPS,)),
            pltpu.SemaphoreType.DMA((N_ARRIVALS,)),
            pltpu.SemaphoreType.DMA((5,)),
            pltpu.SemaphoreType.DMA((len(own),)),
            pltpu.SemaphoreType.DMA((NZ,)),
        ],
        compiler_params=pltpu.CompilerParams(
            collective_id=0, has_side_effects=True, vmem_limit_bytes=60 * 1024 * 1024
        ),
    )(*operands)


def solution(mesh):
    placed = (
        P(("sp", "tp"), None),
        P("sp", "tp"),
        P("tp", None),
        P("tp", None),
        P("sp", "tp"),
        P("tp", None, None),
        P("tp", None, None),
        P("tp", None, None),
        P("tp", None, None),
        P("tp", None),
        P(),
        P(),
        P(),
        P("sp", "tp"),
        P("sp", "tp"),
        P("tp", "sp"),
    )
    return jax.shard_map(
        per_device, mesh=mesh, in_specs=placed, out_specs=P(("sp", "tp"), None), check_vma=False
    )
```

```python
import functools

import jax
import jax.numpy as jnp
from jax import lax
from jax.experimental import pallas as pl
from jax.experimental.pallas import tpu as pltpu
from jax.sharding import PartitionSpec as P

f32, bf16 = jnp.float32, jnp.bfloat16
HIGH = lax.Precision.HIGHEST
MESH = pl.DeviceIdType.MESH
eps = 1e-06
NZ, NY, NC, NX = 8, 4, 2, 4
ROWS = 256
GROUPS, CHAN, STATE = 8, 16, 64
LANES = 2 * STATE
WIDE = GROUPS * LANES
LOCAL = GROUPS * CHAN
D, HID, SHARD = 2048, 1408, 32
OWN = ROWS // NX
PATH_A = ((512, 256), (640, 384))
PHASES = ((0, 2), (2, 1))
PLANES = (0, -1, 1, -2, 2, -3, 3, 4)
OPENING = ("1a0", "0a0", "0b0", "1y0",)
RELAY = (7,)
DIRECT = ()
N_GROUPS, N_ARRIVALS = 21, 114
ORDER = (
    "r0", "local", "1b0", "c1", "masked", "outmap", "1s0", "0y0", "0s0", "0a1", "0s1", "0b1", "0y1", "1f0",
    "h0", "carry", "r1", "h1", "0f0", "h2", "0s2", "c2", "0q11", "0y2", "0q31", "0f1", "0d0", "0b2", "0y4",
    "0y3", "r2", "0e0", "0q21", "far", "resp", "m", "1q01", "0q32", "0f2", "0q01", "0d1", "0f4", "0b3",
    "0y5", "0y6", "0e1", "0q22", "0d2", "0q12", "0e2", "0f3", "0q02", "0d4", "proj", "1a1", "1s1", "0b4",
    "0y7", "first0", "first1", "0e4", "0q23", "first4", "first2", "0q13", "0f6", "0d3", "1b1", "1y1", "1s2",
    "1d0", "0q03", "1y2", "1q11", "0e3", "first3", "1e0", "0f7", "0q33", "0q24", "0q14", "0d6", "0f5",
    "1b2", "1y3", "1f1", "1q21", "1f2", "0e6", "first6", "0q04", "1q31", "1y4", "0q34", "0d7", "1q12",
    "0d5", "1b3", "1y6", "1f3", "1q02", "1q22", "0e7", "first7", "1d1", "1y5", "1q32", "1d2", "0e5",
    "first5", "hidden", "1b4", "1y7", "second0", "scat0", "1e1", "second1", "scat1", "1q03", "1d3", "1f6",
    "1e2", "second2", "1q23", "scat2", "1q13", "1f4", "1f5", "1q33", "1e3", "second3", "1f7", "scat3",
    "pass0", "1d6", "pass1", "1q04", "1d4", "pass2", "1q24", "1d5", "1q14", "1e6", "second6", "1q34", "1d7",
    "scat6", "1e4", "second4", "scat4", "pass3", "1e5", "second5", "scat5", "fin0", "1e7", "second7",
    "scat7", "fin1", "fin2", "pass6", "pass4", "fin3", "pass5", "pass7", "fin6", "fin4", "fin5", "fin7",
)


def iota(shape, dim):
    return lax.broadcasted_iota(jnp.int32, shape, dim)


def where_one(test):
    return jnp.where(test, 1.0, 0.0).astype(f32)


def nt(a, b, precision=None):
    return lax.dot_general(
        a, b, (((1,), (1,)), ((), ())), precision=precision, preferred_element_type=f32
    )


def nn(a, b, precision=None):
    return lax.dot_general(
        a, b, (((1,), (0,)), ((), ())), precision=precision, preferred_element_type=f32
    )


def swap(a):
    return pltpu.roll(a, STATE, 1)


def sign_lanes(shape):
    return jnp.where(iota(shape, 1) < STATE, -1.0, 1.0).astype(f32)


def turned(a, c, s):
    return a * c + swap(a) * s


def silu(x):
    return x * jax.nn.sigmoid(x)


def kernel(
    resid, mix_h, forget_h, decay_h, turn_h, in_re_h, in_im_h, out_re_h, out_im_h, skip_h, mix_gain_h,
    w_out, ffn_gain_h, gate, up, down_t, out,
    mix, forget_t, decay, turn, in_re, in_im, out_re, out_im, skip, mix_gain, ffn_gain,
    G, RA, WO, MX, X, RM, GA, UA, HB, PT, RS, RB, RQ, RT, UB, YB, ST, C1, C2,
    send_sem, recv_sem, local_sem, entry_sem, hello_sem,
):
    me, x = lax.axis_index("sp"), lax.axis_index("tp")
    c = lax.rem(me, NC)
    y = lax.rem(lax.div(me, NC), NY)
    z = lax.div(me, NC * NY)
    slot = lax.rem(me, NC * NY)

    def at_sp(zz, yy, cc):
        return {"sp": (zz * NY + yy) * NC + cc}

    def zr(d):
        return lax.rem(z + (d + NZ), NZ)

    def yr(d):
        return lax.rem(y + (d + NY), NY)

    def xr(d):
        return lax.rem(x + (d + NX), NX)

    plane_peers = [{"sp": z * NY * NC + lax.rem(slot + d, NY * NC)} for d in range(1, NY * NC)]
    z_peers = [at_sp(zr(d), y, c) for d in range(1, NZ)]
    x_peers = [{"tp": xr(d)} for d in range(1, NX)]
    yp, ym = at_sp(z, yr(1), c), at_sp(z, yr(-1), c)
    zp, zm = at_sp(zr(1), y, c), at_sp(zr(-1), y, c)
    partner = at_sp(z, y, 1 - c)

    groups, arrivals = {}, {}

    def send(group, name, src, dst, to):
        k = groups.setdefault(group, len(groups))
        n = arrivals.setdefault(name, len(arrivals))
        pltpu.make_async_remote_copy(
            src_ref=src, dst_ref=dst, send_sem=send_sem.at[k], recv_sem=recv_sem.at[n],
            device_id=to, device_id_type=MESH,
        ).start()

    def waiter(k, n, bytes_of):
        return pltpu.make_async_remote_copy(
            src_ref=bytes_of, dst_ref=bytes_of, send_sem=send_sem.at[k], recv_sem=recv_sem.at[n],
            device_id=partner, device_id_type=MESH,
        )

    def recv(name, bytes_of):
        waiter(0, arrivals[name], bytes_of).wait_recv()

    def sent(group, bytes_of):
        waiter(groups[group], 0, bytes_of).wait_send()

    tasks, drains = {}, []

    def task(f):
        tasks[f.__name__] = f
        return f

    def gather_tasks(p):
        first, count = PHASES[p]
        cut, cut_plus = PATH_A[p]
        tiles = (HID - cut) // 128
        few, many = cut + tiles // 2 * 128, cut + (tiles - tiles // 2) * 128
        path_a, path_a1, path_a2 = (0, cut), (0, cut_plus), (cut_plus, cut)
        path_b = (cut, HID)

        def halves(odd):
            middle = many if odd else few
            return (cut, middle), (middle, HID)

        def block(dz, dy, lanes):
            return G.at[
                pl.ds(first, count), zr(dz), yr(dy), c, :, pl.ds(lanes[0], lanes[1] - lanes[0])
            ]

        def sized(planes, rows, lanes):
            return G.at[
                pl.ds(first, count), pl.ds(0, planes), pl.ds(0, rows), c, :,
                pl.ds(lanes[0], lanes[1] - lanes[0]),
            ]

        def go(name, ref, to):
            send(f"{p}{name[0]}", f"{p}{name}", ref, ref, to)

        def both(name, ref, plus, minus):
            go(name, ref, plus)
            go(name, ref, minus)

        def got(name, lanes, count_of=1):
            recv(f"{p}{name}", sized(1, count_of, lanes))

        def a0():
            both("A0", block(0, 0, path_a), yp, ym)

        def b0():
            both("B1", block(0, 0, path_b), zp, zm)

        def a1():
            got("A0", path_a, 2)
            go("A1", block(0, -1, path_a1), yp)
            go("A1", block(0, 1, path_a2), ym)

        def s0():
            both("Z01", block(0, 0, path_a), zp, zm)

        def s1():
            both("Z11", block(0, -1, path_a), zp, zm)
            both("Z31", block(0, 1, path_a), zp, zm)

        def s2():
            got("A1", path_a)
            both("Z21", block(0, 2, path_a), zp, zm)

        def q(row, s):
            dy = (0, -1, 2, 1)[row]
            got(f"Z{row}{s}", path_a, 2 if s < 4 else 1)
            if s < 3 or (s == 3 and row in (0, 1)):
                go(f"Z{row}{s + 1}", block(-s, dy, path_a), zp)
            if s < 3 or (s == 3 and row in (2, 3)):
                go(f"Z{row}{s + 1}", block(s, dy, path_a), zm)

        def b(s):
            got(f"B{s}", path_b, 2 if s < 4 else 1)
            plus, minus = (path_b, path_b) if s < 3 else halves(p)
            if s < 4:
                go(f"B{s + 1}", block(-s, 0, plus), zp)
                go(f"B{s + 1}", block(s, 0, minus), zm)

        def y_(k):
            both(f"Y{k}", block(PLANES[k], 0, path_b), yp, ym)

        def f(k):
            got(f"Y{k}", path_b, 2)
            plus, minus = halves(k % 2)
            go(f"F{k}", block(PLANES[k], -1, plus), yp)
            go(f"F{k}", block(PLANES[k], 1, minus), ym)

        def d(k):
            got(f"F{k}", path_b)
            go(f"D{k}", G.at[pl.ds(first, count), zr(PLANES[k]), :, c], partner)

        def e(k):
            recv(f"{p}D{k}", sized(1, NY, (0, HID)))

        def all_sent():
            for kind, planes, rows, lanes in (
                ("A", 1, 3, path_a), ("Z", 7, 4, path_a), ("Y", 8, 2, path_b), ("F", 8, 1, path_b),
                ("B", 7, 1, path_b), ("D", 8, 4, (0, HID)),
            ):
                sent(f"{p}{kind}", sized(planes, rows, lanes))

        drains.append(all_sent)
        for name, f_ in (("a0", a0), ("b0", b0), ("a1", a1), ("s0", s0), ("s1", s1), ("s2", s2)):
            tasks[f"{p}{name}"] = f_
        for s in range(1, 5):
            tasks[f"{p}b{s}"] = functools.partial(b, s)
            for row in range(NY):
                tasks[f"{p}q{row}{s}"] = functools.partial(q, row, s)
        for k in range(NZ):
            tasks[f"{p}y{k}"] = functools.partial(y_, k)
            tasks[f"{p}f{k}"] = functools.partial(f, k)
            tasks[f"{p}d{k}"] = functools.partial(d, k)
            tasks[f"{p}e{k}"] = functools.partial(e, k)

    for p in range(len(PHASES)):
        gather_tasks(p)

    barrier = pltpu.get_barrier_semaphore()
    peers = plane_peers + [zp, zm] + x_peers
    for peer in peers:
        pl.semaphore_signal(barrier, inc=1, device_id=peer, device_id_type=MESH)
    small = [
        (mix_h, mix), (forget_h, forget_t), (decay_h, decay), (turn_h, turn), (in_re_h, in_re),
        (in_im_h, in_im), (out_re_h, out_re), (out_im_h, out_im), (skip_h, skip),
        (mix_gain_h, mix_gain), (ffn_gain_h, ffn_gain),
    ]
    early = [pltpu.make_async_copy(a, b, entry_sem.at[k]) for k, (a, b) in enumerate(small)]
    loads = [
        pltpu.make_async_copy(gate, G.at[0, z, y, c], local_sem.at[0]),
        pltpu.make_async_copy(up, G.at[1, z, y, c], local_sem.at[0]),
        pltpu.make_async_copy(down_t, G.at[2, z, y, c], local_sem.at[0]),
        pltpu.make_async_copy(resid, RA.at[x], local_sem.at[1]),
        pltpu.make_async_copy(w_out, WO, local_sem.at[2]),
    ]
    for load in loads[:3] + early + loads[3:]:
        load.start()

    def hello(n):
        for peer in (zp, zm):
            pl.semaphore_signal(hello_sem.at[n], inc=1, device_id=peer, device_id_type=MESH)

    def met(n):
        pl.semaphore_wait(hello_sem.at[n], 2)
        if n < 2:
            hello(n + 1)

    for n in range(3):
        tasks[f"h{n}"] = functools.partial(met, n)

    with jax.named_scope("entry"):
        pl.semaphore_wait(barrier, len(peers))
        own_weights = G.at[:, z, y, c]
        pltpu.make_async_copy(own_weights, own_weights, local_sem.at[0]).wait()
        hello(0)
    with jax.named_scope("opening"):
        for name in OPENING:
            tasks[name]()
        for load in early:
            load.wait()
    with jax.named_scope("prep"):
        drive = mix[...]
        spread = where_one(lax.rem(iota((CHAN, LOCAL), 1), CHAN) == iota((CHAN, LOCAL), 0))
        twice = where_one(lax.rem(iota((STATE, LANES), 1), STATE) == iota((STATE, LANES), 0))
        rate2 = nn(decay[...], twice, HIGH)
        turn2 = nn(turn[...], twice, HIGH)
        lower = iota((ROWS, ROWS), 0) >= iota((ROWS, ROWS), 1)
        lower_one = where_one(lower)
        forget_rows = forget_t[...]
        run_log = nt(lower_one, forget_rows, HIGH)
        run_log_t = nt(forget_rows, lower_one, HIGH)
        w = 2.0 * rate2
        series = 1.0 + w / 6.0
        for k in (5.0, 4.0, 3.0, 2.0):
            series = 1.0 + (w / k) * series
        in_factor = jnp.sqrt(-(w * series))
        first_half = where_one(iota((STATE, LANES), 1) == iota((STATE, LANES), 0)).astype(bf16)
        second_half = where_one(
            iota((STATE, LANES), 1) == iota((STATE, LANES), 0) + STATE
        ).astype(bf16)
        row_group = lax.div(iota((LOCAL, LANES), 0), CHAN)

        def by_group(rows):
            return jnp.concatenate(
                [jnp.where(row_group == g, rows, 0.0).astype(bf16) for g in range(GROUPS)], axis=1
            )

        in_map = by_group(
            nn(in_re[...].astype(bf16), first_half) + nn(in_im[...].astype(bf16), second_half)
        )
        UB[...] = nn(drive, in_map)
        sign = sign_lanes((1, LANES))
        sign8 = sign_lanes((GROUPS, LANES))
        coarse = (iota((16, LANES), 0) - 8).astype(f32) * 16.0
        fine = iota((16, LANES), 0).astype(f32)
        centred = (iota((ROWS, LANES), 0) - ROWS // 2).astype(f32)

    def phase_tables(g):
        angle = turn2[g : g + 1]
        ca, sa = jnp.cos(angle * coarse), jnp.sin(angle * coarse)
        cb, sb = jnp.cos(angle * fine), jnp.sin(angle * fine)
        cos = [ca[k : k + 1] * cb - sa[k : k + 1] * sb for k in range(16)]
        sin = [sa[k : k + 1] * cb + ca[k : k + 1] * sb for k in range(16)]
        return jnp.concatenate(cos, axis=0), jnp.concatenate(sin, axis=0) * sign

    def power(n, log=0.0):
        size = jnp.exp(rate2 * n + log)
        return size * jnp.cos(turn2 * n), size * jnp.sin(turn2 * n) * sign8

    v = {}
    on_diagonal = iota((GROUPS, LANES), 0) == iota((GROUPS, LANES), 1)

    def as_row(column):
        return jnp.sum(jnp.where(on_diagonal, column, 0.0), axis=0, keepdims=True)

    def as_column(row):
        return jnp.sum(jnp.where(on_diagonal, row, 0.0), axis=1, keepdims=True)

    @task
    def local():
        ends = []
        last = run_log[ROWS - 1 : ROWS]
        for g in range(GROUPS):
            lanes = slice(LANES * g, LANES * (g + 1))
            cos, sin = phase_tables(g)
            grow = jnp.exp(-rate2[g : g + 1] * centred) * in_factor[g : g + 1]
            b_g = UB[:, lanes]
            u = (b_g * cos - swap(b_g) * sin) * grow
            UB[:, lanes] = u
            fall = jnp.exp(rate2[g : g + 1] * centred)
            ST[0, :, lanes] = cos * fall
            ST[1, :, lanes] = sin * fall
            weight = jnp.exp(last[:, g : g + 1] - run_log[:, g : g + 1])
            total = jnp.sum(u * weight, axis=0, keepdims=True)
            at_end = slice(ROWS - 1, ROWS)
            ends.append(turned(total, ST[0, at_end, lanes], ST[1, at_end, lanes]))
        last_col = jnp.sum(
            jnp.where(iota((GROUPS, ROWS), 1) == ROWS - 1, run_log_t, 0.0), axis=1, keepdims=True
        )
        C1[slot, 0:GROUPS] = jnp.concatenate(ends, axis=0)
        C1[slot, GROUPS:] = as_row(last_col)

    @task
    def c1():
        for d in range(1, NY * NC):
            send("C1", "C1", C1.at[slot], C1.at[slot], plane_peers[d - 1])

    @task
    def masked():
        for g in range(GROUPS):
            lanes = slice(LANES * g, LANES * (g + 1))
            gap = run_log[:, g : g + 1] - run_log_t[g : g + 1]
            weights = jnp.where(lower, jnp.exp(jnp.minimum(gap, 0.0)), 0.0).astype(bf16)
            YB[:, lanes] = nn(weights, UB[:, lanes].astype(bf16))

    @task
    def carry():
        c_one, s_one = power(float(ROWS))
        recv("C1", C1.at[1:])
        acc = jnp.zeros((GROUPS, LANES), f32)
        log_acc = jnp.zeros((GROUPS, 1), f32)
        before, log_before = acc, log_acc
        for j in range(NY * NC):
            here = slot == j
            before = jnp.where(here, acc, before)
            log_before = jnp.where(here, log_acc, log_before)
            log_j = as_column(C1[j, GROUPS:])
            acc = jnp.exp(log_j) * turned(acc, c_one, s_one) + C1[j, 0:GROUPS]
            log_acc = log_acc + log_j
        C2[z, 0:GROUPS] = acc
        C2[z, GROUPS:] = as_row(log_acc)
        v["before"], v["log_before"] = before, log_before

    @task
    def c2():
        for d in range(1, NZ):
            send("C2", "C2", C2.at[z], C2.at[z], z_peers[d - 1])

    @task
    def outmap():
        v["out_map"] = by_group(
            nn(out_re[...].astype(bf16), first_half) - nn(out_im[...].astype(bf16), second_half)
        )
        skip_rows = nn(skip[...], spread, HIGH)
        in_group = lax.div(iota((GROUPS, LOCAL), 1), CHAN) == iota((GROUPS, LOCAL), 0)
        v["skip_row"] = jnp.sum(jnp.where(in_group, skip_rows, 0.0), axis=0, keepdims=True)

    @task
    def far():
        c_plane, s_plane = power(float(ROWS * NY * NC))
        c_in, s_in = power(slot.astype(f32) * float(ROWS), v["log_before"])
        c_mid, s_mid = power(float(ROWS // 2 + 1))
        recv("C2", C2.at[1:])
        total = jnp.zeros((GROUPS, LANES), f32)
        for j in range(NZ):
            fade = jnp.exp(as_column(C2[j, GROUPS:]))
            step_on = fade * turned(total, c_plane, s_plane) + C2[j, 0:GROUPS]
            total = jnp.where(j < z, step_on, total)
        v["carry"] = turned(v["before"] + turned(total, c_in, s_in), c_mid, s_mid)

    @task
    def resp():
        for g in range(GROUPS):
            lanes = slice(LANES * g, LANES * (g + 1))
            full = YB[:, lanes] + jnp.exp(run_log[:, g : g + 1]) * v["carry"][g : g + 1]
            YB[:, lanes] = turned(full, ST[0, :, lanes], ST[1, :, lanes])
        response = nt(YB[...].astype(bf16), v["out_map"]) + v["skip_row"] * drive.astype(f32)
        MX[x] = jax.nn.gelu(response).astype(bf16)

    @task
    def m():
        for d in range(1, NX):
            send("M", "M", MX.at[x], MX.at[x], x_peers[d - 1])

    half = OWN // 2

    @task
    def r0():
        loads[3].wait()
        send("R", "R", RA.at[x], RA.at[x], x_peers[0])
        send("R", "R", RA.at[x], RA.at[x], x_peers[2])

    @task
    def r1():
        recv("R", RA.at[2:])
        send("Q", "Q", RA.at[xr(-1), 0:half], RA.at[xr(-1), 0:half], x_peers[0])
        send("Q", "Q", RA.at[xr(1), half:], RA.at[xr(1), half:], x_peers[2])

    @task
    def r2():
        recv("Q", RA.at[0])
        loads[4].wait()

    @task
    def proj():
        recv("M", MX.at[1:])
        mixed = [MX[q].astype(f32) for q in range(NX)]
        total = sum(jnp.sum(m * m, axis=1, keepdims=True) for m in mixed)
        scale = lax.rsqrt(total / float(LOCAL * NX) + eps)
        gains = mix_gain[...]
        normed = jnp.concatenate(
            [
                (mixed[q] * scale * gains[:, LOCAL * q : LOCAL * (q + 1)]).astype(bf16)
                for q in range(NX)
            ],
            axis=1,
        )
        squares = jnp.zeros((ROWS, 1), f32)
        for k in range(4):
            lanes = slice(512 * k, 512 * (k + 1))
            piece = nn(normed, WO[:, lanes]) + RA[:, :, lanes].reshape(ROWS, 512).astype(f32)
            RM[:, lanes] = piece
            squares = squares + jnp.sum(piece * piece, axis=1, keepdims=True)
        scale = lax.rsqrt(squares / float(D) + eps)
        for k in range(4):
            lanes = slice(512 * k, 512 * (k + 1))
            X[:, lanes] = (RM[:, lanes] * scale * ffn_gain[:, lanes]).astype(bf16)

    def column_slice(k):
        return pl.ds(pl.multiple_of(zr(PLANES[k]) * ROWS, ROWS), ROWS)

    def first(k):
        piece = X[:, column_slice(k)]
        for m, store in ((0, GA), (1, UA)):
            product = nn(piece, G[m, zr(PLANES[k])].reshape(ROWS, HID))
            store[...] = product if k == 0 else store[...] + product

    @task
    def hidden():
        HB[...] = (silu(GA[...]) * UA[...]).astype(bf16)

    def second(k):
        part = nt(HB[...], G[2, zr(PLANES[k])].reshape(ROWS, HID))
        PT[:, :, column_slice(k)] = part.astype(bf16).reshape(NX, OWN, ROWS)

    def part_slice(k, side):
        return pl.ds(pl.multiple_of(zr(PLANES[k]) * ROWS + 128 * side, 128), 128)

    def scat(k):
        if k in DIRECT:
            cols = column_slice(k)
            for d in (2, 1, 3):
                send("T", f"S{k}", PT.at[xr(d), :, cols], RT.at[DIRECT.index(k), x], x_peers[d - 1])
            return
        for side, to in ((0, x_peers[0]), (1, x_peers[2])):
            send("S", f"S{k}", PT.at[xr(2), :, part_slice(k, side)], RB.at[k, side], to)
        if k in RELAY:
            near(k, "W")

    def near(k, kind):
        cols = column_slice(k)
        send(kind, f"{kind}{k}", PT.at[xr(1), :, cols], RS.at[0, :, cols], x_peers[0])
        send(kind, f"{kind}{k}", PT.at[xr(-1), :, cols], RS.at[1, :, cols], x_peers[2])

    def pass_(k):
        recv(f"S{k}", RB.at[k])
        if k in RELAY:
            n = RELAY.index(k)
            for side, to in ((0, x_peers[0]), (1, x_peers[2])):
                send("U", f"V{k}", RB.at[k, side], RQ.at[n, side], to)
            return
        for side, dx in ((0, 1), (1, -1)):
            lanes = part_slice(k, side)
            sum_ = PT[xr(dx), :, lanes].astype(f32) + RB[k, side].astype(f32)
            PT[xr(dx), :, lanes] = sum_.astype(bf16)
        near(k, "V")

    def fin(k):
        cols = column_slice(k)
        ffn = PT[x, :, cols].astype(f32)
        if k in DIRECT:
            n = DIRECT.index(k)
            recv(f"S{k}", RT.at[n, 1:])
            for d in range(1, NX):
                ffn = ffn + RT[n, xr(d)].astype(f32)
        else:
            recv(f"W{k}" if k in RELAY else f"V{k}", RS.at[:, :, 0:ROWS])
            ffn = ffn + RS[0, :, cols].astype(f32) + RS[1, :, cols].astype(f32)
        if k in RELAY:
            n = RELAY.index(k)
            recv(f"V{k}", RQ.at[n])
            ffn = ffn + jnp.concatenate([RQ[n, 0], RQ[n, 1]], axis=1).astype(f32)
        kept = RM[pl.ds(pl.multiple_of(x * OWN, OWN), OWN), cols]
        out[:, cols] = (kept + 0.5 * ffn).astype(bf16)

    for k in range(NZ):
        tasks[f"first{k}"] = functools.partial(first, k)
        tasks[f"second{k}"] = functools.partial(second, k)
        tasks[f"scat{k}"] = functools.partial(scat, k)
        tasks[f"pass{k}"] = functools.partial(pass_, k)
        tasks[f"fin{k}"] = functools.partial(fin, k)

    for name in ORDER:
        with jax.named_scope(name):
            tasks[name]()
    with jax.named_scope("drain"):
        assert (len(groups), len(arrivals)) == (N_GROUPS, N_ARRIVALS)
        for drain in drains:
            drain()
        sent("C1", C1.at[1:])
        sent("C2", C2.at[1:])
        sent("M", MX.at[1:])
        sent("R", RA.at[2:])
        sent("Q", RA.at[0])
        passed = NZ - len(DIRECT)
        summed = passed - len(RELAY)
        sent("S", RB.at[0:passed])
        sent("V", RS.at[:, :, 0 : summed * ROWS])
        if DIRECT:
            sent("T", RT.at[:, 1:])
        if RELAY:
            sent("W", RS.at[:, :, 0 : len(RELAY) * ROWS])
            sent("U", RQ)


def per_device(
    resid, mix_in, decay_rate, turn_rate, forget, input_real, input_imag, output_real, output_imag,
    skip_gain, mix_gain, w_out, ffn_gain, gating_matrix, w_up, w_down,
):
    operands = (
        resid, mix_in, forget.T, decay_rate, turn_rate,
        input_real.transpose(0, 2, 1).reshape(-1, STATE),
        input_imag.transpose(0, 2, 1).reshape(-1, STATE),
        output_real.reshape(-1, STATE), output_imag.reshape(-1, STATE),
        skip_gain, mix_gain.reshape(1, -1), w_out, ffn_gain.reshape(1, -1),
        gating_matrix, w_up, w_down.T,
    )
    own = [pltpu.VMEM(operands[k].shape, operands[k].dtype) for k in (*range(1, 11), 12)]
    return pl.pallas_call(
        kernel,
        out_shape=jax.ShapeDtypeStruct((OWN, D), bf16),
        in_specs=[pl.BlockSpec(memory_space=pl.ANY)] * len(operands),
        out_specs=pl.BlockSpec(memory_space=pltpu.VMEM),
        scratch_shapes=own + [
            pltpu.VMEM((3, NZ, NY, NC, SHARD, HID), bf16),
            pltpu.VMEM((NX, OWN, D), bf16),
            pltpu.VMEM((LOCAL * NX, D), bf16),
            pltpu.VMEM((NX, ROWS, LOCAL), bf16),
            pltpu.VMEM((ROWS, D), bf16),
            pltpu.VMEM((ROWS, D), f32),
            pltpu.VMEM((ROWS, HID), f32),
            pltpu.VMEM((ROWS, HID), f32),
            pltpu.VMEM((ROWS, HID), bf16),
            pltpu.VMEM((NX, OWN, D), bf16),
            pltpu.VMEM((2, OWN, D), bf16),
            pltpu.VMEM((NZ, 2, OWN, 128), bf16),
            pltpu.VMEM((max(len(RELAY), 1), 2, OWN, 128), bf16),
            pltpu.VMEM((max(len(DIRECT), 1), NX, OWN, ROWS), bf16),
            pltpu.VMEM((ROWS, WIDE), f32),
            pltpu.VMEM((ROWS, WIDE), f32),
            pltpu.VMEM((2, ROWS, WIDE), f32),
            pltpu.VMEM((NY * NC, GROUPS + 1, LANES), f32),
            pltpu.VMEM((NZ, GROUPS + 1, LANES), f32),
            pltpu.SemaphoreType.DMA((N_GROUPS,)),
            pltpu.SemaphoreType.DMA((N_ARRIVALS,)),
            pltpu.SemaphoreType.DMA((3,)),
            pltpu.SemaphoreType.DMA((len(own),)),
            pltpu.SemaphoreType.REGULAR((3,)),
        ],
        compiler_params=pltpu.CompilerParams(
            collective_id=0, has_side_effects=True, vmem_limit_bytes=52 * 1024 * 1024
        ),
    )(*[pltpu.with_memory_space_constraint(operand, pltpu.HBM) for operand in operands])


def solution(mesh):
    placed = (
        P(("sp", "tp"), None),
        P("sp", "tp"),
        P("tp", None),
        P("tp", None),
        P("sp", "tp"),
        P("tp", None, None),
        P("tp", None, None),
        P("tp", None, None),
        P("tp", None, None),
        P("tp", None),
        P(),
        P(),
        P(),
        P("sp", "tp"),
        P("sp", "tp"),
        P("tp", "sp"),
    )
    return jax.shard_map(
        per_device, mesh=mesh, in_specs=placed, out_specs=P(("sp", "tp"), None), check_vma=False
    )
```

```python
import functools

import jax
import jax.numpy as jnp
from jax import lax
from jax.experimental import pallas as pl
from jax.experimental.pallas import tpu as pltpu
from jax.sharding import PartitionSpec as P

f32, bf16 = jnp.float32, jnp.bfloat16
HIGH = lax.Precision.HIGHEST
MESH = pl.DeviceIdType.MESH
eps = 1e-06
NZ, NY, NC, NX = 8, 4, 2, 4
ROWS = 256
GROUPS, CHAN, STATE = 8, 16, 64
LANES = 2 * STATE
WIDE = GROUPS * LANES
LOCAL = GROUPS * CHAN
D, HID, SHARD = 2048, 1408, 32
OWN = ROWS // NX
PATH_A = ((512, 256), (640, 384))
PHASES = ((0, 2), (2, 1))
PLANES = (0, -1, 1, -2, 2, -3, 3, 4)
OPENING = ("1a0", "0a0", "0b0", "1y0",)
RELAY = (7,)
DIRECT = ()
N_GROUPS = 21
ORDER = (
    "r0", "local", "1b0", "c1", "masked", "outmap", "1s0", "0y0", "0s0", "0a1", "0s1", "0b1", "0y1", "1f0",
    "h0", "carry", "r1", "h1", "0f0", "h2", "0s2", "c2", "0q11", "0y2", "0q31", "0f1", "0d0", "0b2", "0y4",
    "0y3", "r2", "0e0", "0q21", "far", "resp", "m", "1q01", "0q32", "0f2", "0q01", "0d1", "0f4", "0b3",
    "0y5", "0y6", "0e1", "0q22", "0d2", "0q12", "0e2", "0f3", "0q02", "0d4", "proj", "1a1", "1s1", "0b4",
    "0y7", "first0", "first1", "0e4", "0q23", "first4", "first2", "0q13", "0f6", "0d3", "1b1", "1y1", "1s2",
    "1d0", "0q03", "1y2", "1q11", "0e3", "first3", "1e0", "0f7", "0q33", "0q24", "0q14", "0d6", "0f5",
    "1b2", "1y3", "1f1", "1q21", "1f2", "0e6", "first6", "0q04", "1q31", "1y4", "0q34", "0d7", "1q12",
    "0d5", "1b3", "1y6", "1f3", "1q02", "1q22", "0e7", "first7", "1d1", "1y5", "1q32", "1d2", "0e5",
    "first5", "hidden", "1b4", "1y7", "second0", "scat0", "1e1", "second1", "scat1", "1q03", "1d3", "1f6",
    "1e2", "second2", "1q23", "scat2", "1q13", "1f4", "1f5", "1q33", "1e3", "second3", "1f7", "scat3",
    "pass0", "1d6", "pass1", "1q04", "1d4", "pass2", "1q24", "1d5", "1q14", "1e6", "second6", "1q34", "1d7",
    "scat6", "1e4", "second4", "scat4", "pass3", "1e5", "second5", "scat5", "fin0", "1e7", "second7",
    "scat7", "fin1", "fin2", "pass6", "pass4", "fin3", "pass5", "pass7", "fin6", "fin4", "fin5", "fin7",
)
ARRIVALS = (
    ("1A0", "1Y2", "1Y7"),
    ("0A0", "0Y2", "0F3", "1F1", "1F5"),
    ("0B1", "0B3", "1B2", "1B4"),
    ("1Y0", "0Y3", "1Y1", "1Y5"),
    ("R", "S0", "S7"),
    ("1B1", "1B3", "1Z14"),
    ("C1",),
    ("1Z01", "1Z31", "1Z33"),
    ("0Y0", "0Y4", "1A1", "1Y4"),
    ("0Z01", "0Z03"),
    ("0A1", "0F2", "1Y3", "1F6"),
    ("0Z11", "0Z02", "0Z04"),
    ("0Z31", "0Z33"),
    ("0B2", "0B4"),
    ("0Y1", "0Y5", "1Y6"),
    ("1F0", "1F2", "1F7"),
    ("Q", "V0", "V7"),
    ("0F0", "0F4", "0F7"),
    ("0Z21", "0Z23", "1Z32", "1Z34"),
    ("C2",),
    ("0Z12", "0Z14", "1Z03"),
    ("0Z32", "1Z11", "1Z13"),
    ("0F1", "0Y7"),
    ("0D0", "0D2", "0D3", "0D5", "1D4"),
    ("0Z22", "0Z24"),
    ("M",),
    ("1Z02", "1Z04"),
    ("0D1", "0D4", "0D6", "1D1", "1D6"),
    ("0Y6", "0F5", "1F4"),
    ("0Z13", "1Z22", "1Z24"),
    ("0F6", "1F3"),
    ("1Z21", "1Z23"),
    ("1D0", "0D7", "1D3", "1D7"),
    ("1Z12",),
    ("0Z34",),
    ("1D2",),
    ("S1", "V4"),
    ("S2", "V6"),
    ("S3", "V5"),
    ("V1",),
    ("V2",),
    ("1D5",),
    ("S6",),
    ("S4",),
    ("V3",),
    ("S5",),
    ("W7",),
)
ARRIVAL_OF = {name: k for k, names in enumerate(ARRIVALS) for name in names}


def iota(shape, dim):
    return lax.broadcasted_iota(jnp.int32, shape, dim)


def where_one(test):
    return jnp.where(test, 1.0, 0.0).astype(f32)


def nt(a, b, precision=None):
    return lax.dot_general(
        a, b, (((1,), (1,)), ((), ())), precision=precision, preferred_element_type=f32
    )


def nn(a, b, precision=None):
    return lax.dot_general(
        a, b, (((1,), (0,)), ((), ())), precision=precision, preferred_element_type=f32
    )


def swap(a):
    return pltpu.roll(a, STATE, 1)


def sign_lanes(shape):
    return jnp.where(iota(shape, 1) < STATE, -1.0, 1.0).astype(f32)


def turned(a, c, s):
    return a * c + swap(a) * s


def silu(x):
    return x * jax.nn.sigmoid(x)


def kernel(
    resid, mix_h, forget_h, decay_h, turn_h, in_re_h, in_im_h, out_re_h, out_im_h, skip_h, mix_gain_h,
    w_out, ffn_gain_h, gate, up, down_t, out,
    mix, forget_t, decay, turn, in_re, in_im, out_re, out_im, skip, mix_gain, ffn_gain,
    G, RA, WO, MX, X, RM, GA, UA, HB, PT, RS, RB, RQ, RT, UB, YB, ST, C1, C2,
    send_sem, recv_sem, local_sem, entry_sem, hello_sem,
):
    me, x = lax.axis_index("sp"), lax.axis_index("tp")
    c = lax.rem(me, NC)
    y = lax.rem(lax.div(me, NC), NY)
    z = lax.div(me, NC * NY)
    slot = lax.rem(me, NC * NY)

    def at_sp(zz, yy, cc):
        return {"sp": (zz * NY + yy) * NC + cc}

    def zr(d):
        return lax.rem(z + (d + NZ), NZ)

    def yr(d):
        return lax.rem(y + (d + NY), NY)

    def xr(d):
        return lax.rem(x + (d + NX), NX)

    plane_peers = [{"sp": z * NY * NC + lax.rem(slot + d, NY * NC)} for d in range(1, NY * NC)]
    z_peers = [at_sp(zr(d), y, c) for d in range(1, NZ)]
    x_peers = [{"tp": xr(d)} for d in range(1, NX)]
    yp, ym = at_sp(z, yr(1), c), at_sp(z, yr(-1), c)
    zp, zm = at_sp(zr(1), y, c), at_sp(zr(-1), y, c)
    partner = at_sp(z, y, 1 - c)

    groups = {}

    def send(group, name, src, dst, to):
        k = groups.setdefault(group, len(groups))
        n = ARRIVAL_OF[name]
        pltpu.make_async_remote_copy(
            src_ref=src, dst_ref=dst, send_sem=send_sem.at[k], recv_sem=recv_sem.at[n],
            device_id=to, device_id_type=MESH,
        ).start()

    def waiter(k, n, bytes_of):
        return pltpu.make_async_remote_copy(
            src_ref=bytes_of, dst_ref=bytes_of, send_sem=send_sem.at[k], recv_sem=recv_sem.at[n],
            device_id=partner, device_id_type=MESH,
        )

    def recv(name, bytes_of):
        waiter(0, ARRIVAL_OF[name], bytes_of).wait_recv()

    def sent(group, bytes_of):
        waiter(groups[group], 0, bytes_of).wait_send()

    tasks, drains = {}, []

    def task(f):
        tasks[f.__name__] = f
        return f

    def gather_tasks(p):
        first, count = PHASES[p]
        cut, cut_plus = PATH_A[p]
        tiles = (HID - cut) // 128
        few, many = cut + tiles // 2 * 128, cut + (tiles - tiles // 2) * 128
        path_a, path_a1, path_a2 = (0, cut), (0, cut_plus), (cut_plus, cut)
        path_b = (cut, HID)

        def halves(odd):
            middle = many if odd else few
            return (cut, middle), (middle, HID)

        def block(dz, dy, lanes):
            return G.at[
                pl.ds(first, count), zr(dz), yr(dy), c, :, pl.ds(lanes[0], lanes[1] - lanes[0])
            ]

        def sized(planes, rows, lanes):
            return G.at[
                pl.ds(first, count), pl.ds(0, planes), pl.ds(0, rows), c, :,
                pl.ds(lanes[0], lanes[1] - lanes[0]),
            ]

        def go(name, ref, to):
            send(f"{p}{name[0]}", f"{p}{name}", ref, ref, to)

        def both(name, ref, plus, minus):
            go(name, ref, plus)
            go(name, ref, minus)

        def got(name, lanes, count_of=1):
            recv(f"{p}{name}", sized(1, count_of, lanes))

        def a0():
            both("A0", block(0, 0, path_a), yp, ym)

        def b0():
            both("B1", block(0, 0, path_b), zp, zm)

        def a1():
            got("A0", path_a, 2)
            go("A1", block(0, -1, path_a1), yp)
            go("A1", block(0, 1, path_a2), ym)

        def s0():
            both("Z01", block(0, 0, path_a), zp, zm)

        def s1():
            both("Z11", block(0, -1, path_a), zp, zm)
            both("Z31", block(0, 1, path_a), zp, zm)

        def s2():
            got("A1", path_a)
            both("Z21", block(0, 2, path_a), zp, zm)

        def q(row, s):
            dy = (0, -1, 2, 1)[row]
            got(f"Z{row}{s}", path_a, 2 if s < 4 else 1)
            if s < 3 or (s == 3 and row in (0, 1)):
                go(f"Z{row}{s + 1}", block(-s, dy, path_a), zp)
            if s < 3 or (s == 3 and row in (2, 3)):
                go(f"Z{row}{s + 1}", block(s, dy, path_a), zm)

        def b(s):
            got(f"B{s}", path_b, 2 if s < 4 else 1)
            plus, minus = (path_b, path_b) if s < 3 else halves(p)
            if s < 4:
                go(f"B{s + 1}", block(-s, 0, plus), zp)
                go(f"B{s + 1}", block(s, 0, minus), zm)

        def y_(k):
            both(f"Y{k}", block(PLANES[k], 0, path_b), yp, ym)

        def f(k):
            got(f"Y{k}", path_b, 2)
            plus, minus = halves(k % 2)
            go(f"F{k}", block(PLANES[k], -1, plus), yp)
            go(f"F{k}", block(PLANES[k], 1, minus), ym)

        def d(k):
            got(f"F{k}", path_b)
            go(f"D{k}", G.at[pl.ds(first, count), zr(PLANES[k]), :, c], partner)

        def e(k):
            recv(f"{p}D{k}", sized(1, NY, (0, HID)))

        def all_sent():
            for kind, planes, rows, lanes in (
                ("A", 1, 3, path_a), ("Z", 7, 4, path_a), ("Y", 8, 2, path_b), ("F", 8, 1, path_b),
                ("B", 7, 1, path_b), ("D", 8, 4, (0, HID)),
            ):
                sent(f"{p}{kind}", sized(planes, rows, lanes))

        drains.append(all_sent)
        for name, f_ in (("a0", a0), ("b0", b0), ("a1", a1), ("s0", s0), ("s1", s1), ("s2", s2)):
            tasks[f"{p}{name}"] = f_
        for s in range(1, 5):
            tasks[f"{p}b{s}"] = functools.partial(b, s)
            for row in range(NY):
                tasks[f"{p}q{row}{s}"] = functools.partial(q, row, s)
        for k in range(NZ):
            tasks[f"{p}y{k}"] = functools.partial(y_, k)
            tasks[f"{p}f{k}"] = functools.partial(f, k)
            tasks[f"{p}d{k}"] = functools.partial(d, k)
            tasks[f"{p}e{k}"] = functools.partial(e, k)

    for p in range(len(PHASES)):
        gather_tasks(p)

    barrier = pltpu.get_barrier_semaphore()
    peers = plane_peers + [zp, zm] + x_peers
    for peer in peers:
        pl.semaphore_signal(barrier, inc=1, device_id=peer, device_id_type=MESH)
    small = [
        (mix_h, mix), (forget_h, forget_t), (decay_h, decay), (turn_h, turn), (in_re_h, in_re),
        (in_im_h, in_im), (out_re_h, out_re), (out_im_h, out_im), (skip_h, skip),
        (mix_gain_h, mix_gain), (ffn_gain_h, ffn_gain),
    ]
    early = [pltpu.make_async_copy(a, b, entry_sem.at[k]) for k, (a, b) in enumerate(small)]
    loads = [
        pltpu.make_async_copy(gate, G.at[0, z, y, c], local_sem.at[0]),
        pltpu.make_async_copy(up, G.at[1, z, y, c], local_sem.at[0]),
        pltpu.make_async_copy(down_t, G.at[2, z, y, c], local_sem.at[0]),
        pltpu.make_async_copy(resid, RA.at[x], local_sem.at[1]),
        pltpu.make_async_copy(w_out, WO, local_sem.at[2]),
    ]
    for load in loads[:3] + early + loads[3:]:
        load.start()

    def hello(n):
        for peer in (zp, zm):
            pl.semaphore_signal(hello_sem.at[n], inc=1, device_id=peer, device_id_type=MESH)

    def met(n):
        pl.semaphore_wait(hello_sem.at[n], 2)
        if n < 2:
            hello(n + 1)

    for n in range(3):
        tasks[f"h{n}"] = functools.partial(met, n)

    with jax.named_scope("entry"):
        pl.semaphore_wait(barrier, len(peers))
        own_weights = G.at[:, z, y, c]
        pltpu.make_async_copy(own_weights, own_weights, local_sem.at[0]).wait()
        hello(0)
    with jax.named_scope("opening"):
        for name in OPENING:
            tasks[name]()
        for load in early:
            load.wait()
    with jax.named_scope("prep"):
        drive = mix[...]
        spread = where_one(lax.rem(iota((CHAN, LOCAL), 1), CHAN) == iota((CHAN, LOCAL), 0))
        twice = where_one(lax.rem(iota((STATE, LANES), 1), STATE) == iota((STATE, LANES), 0))
        rate2 = nn(decay[...], twice, HIGH)
        turn2 = nn(turn[...], twice, HIGH)
        lower = iota((ROWS, ROWS), 0) >= iota((ROWS, ROWS), 1)
        lower_one = where_one(lower)
        forget_rows = forget_t[...]
        run_log = nt(lower_one, forget_rows, HIGH)
        run_log_t = nt(forget_rows, lower_one, HIGH)
        w = 2.0 * rate2
        series = 1.0 + w / 6.0
        for k in (5.0, 4.0, 3.0, 2.0):
            series = 1.0 + (w / k) * series
        in_factor = jnp.sqrt(-(w * series))
        first_half = where_one(iota((STATE, LANES), 1) == iota((STATE, LANES), 0)).astype(bf16)
        second_half = where_one(
            iota((STATE, LANES), 1) == iota((STATE, LANES), 0) + STATE
        ).astype(bf16)
        row_group = lax.div(iota((LOCAL, LANES), 0), CHAN)

        def by_group(rows):
            return jnp.concatenate(
                [jnp.where(row_group == g, rows, 0.0).astype(bf16) for g in range(GROUPS)], axis=1
            )

        in_map = by_group(
            nn(in_re[...].astype(bf16), first_half) + nn(in_im[...].astype(bf16), second_half)
        )
        UB[...] = nn(drive, in_map)
        sign = sign_lanes((1, LANES))
        sign8 = sign_lanes((GROUPS, LANES))
        coarse = (iota((16, LANES), 0) - 8).astype(f32) * 16.0
        fine = iota((16, LANES), 0).astype(f32)
        centred = (iota((ROWS, LANES), 0) - ROWS // 2).astype(f32)

    def phase_tables(g):
        angle = turn2[g : g + 1]
        ca, sa = jnp.cos(angle * coarse), jnp.sin(angle * coarse)
        cb, sb = jnp.cos(angle * fine), jnp.sin(angle * fine)
        cos = [ca[k : k + 1] * cb - sa[k : k + 1] * sb for k in range(16)]
        sin = [sa[k : k + 1] * cb + ca[k : k + 1] * sb for k in range(16)]
        return jnp.concatenate(cos, axis=0), jnp.concatenate(sin, axis=0) * sign

    def power(n, log=0.0):
        size = jnp.exp(rate2 * n + log)
        return size * jnp.cos(turn2 * n), size * jnp.sin(turn2 * n) * sign8

    v = {}
    on_diagonal = iota((GROUPS, LANES), 0) == iota((GROUPS, LANES), 1)

    def as_row(column):
        return jnp.sum(jnp.where(on_diagonal, column, 0.0), axis=0, keepdims=True)

    def as_column(row):
        return jnp.sum(jnp.where(on_diagonal, row, 0.0), axis=1, keepdims=True)

    @task
    def local():
        ends = []
        last = run_log[ROWS - 1 : ROWS]
        for g in range(GROUPS):
            lanes = slice(LANES * g, LANES * (g + 1))
            cos, sin = phase_tables(g)
            grow = jnp.exp(-rate2[g : g + 1] * centred) * in_factor[g : g + 1]
            b_g = UB[:, lanes]
            u = (b_g * cos - swap(b_g) * sin) * grow
            UB[:, lanes] = u
            fall = jnp.exp(rate2[g : g + 1] * centred)
            ST[0, :, lanes] = cos * fall
            ST[1, :, lanes] = sin * fall
            weight = jnp.exp(last[:, g : g + 1] - run_log[:, g : g + 1])
            total = jnp.sum(u * weight, axis=0, keepdims=True)
            at_end = slice(ROWS - 1, ROWS)
            ends.append(turned(total, ST[0, at_end, lanes], ST[1, at_end, lanes]))
        last_col = jnp.sum(
            jnp.where(iota((GROUPS, ROWS), 1) == ROWS - 1, run_log_t, 0.0), axis=1, keepdims=True
        )
        C1[slot, 0:GROUPS] = jnp.concatenate(ends, axis=0)
        C1[slot, GROUPS:] = as_row(last_col)

    @task
    def c1():
        for d in range(1, NY * NC):
            send("C1", "C1", C1.at[slot], C1.at[slot], plane_peers[d - 1])

    @task
    def masked():
        for g in range(GROUPS):
            lanes = slice(LANES * g, LANES * (g + 1))
            gap = run_log[:, g : g + 1] - run_log_t[g : g + 1]
            weights = jnp.where(lower, jnp.exp(jnp.minimum(gap, 0.0)), 0.0).astype(bf16)
            YB[:, lanes] = nn(weights, UB[:, lanes].astype(bf16))

    @task
    def carry():
        c_one, s_one = power(float(ROWS))
        recv("C1", C1.at[1:])
        acc = jnp.zeros((GROUPS, LANES), f32)
        log_acc = jnp.zeros((GROUPS, 1), f32)
        before, log_before = acc, log_acc
        for j in range(NY * NC):
            here = slot == j
            before = jnp.where(here, acc, before)
            log_before = jnp.where(here, log_acc, log_before)
            log_j = as_column(C1[j, GROUPS:])
            acc = jnp.exp(log_j) * turned(acc, c_one, s_one) + C1[j, 0:GROUPS]
            log_acc = log_acc + log_j
        C2[z, 0:GROUPS] = acc
        C2[z, GROUPS:] = as_row(log_acc)
        v["before"], v["log_before"] = before, log_before

    @task
    def c2():
        for d in range(1, NZ):
            send("C2", "C2", C2.at[z], C2.at[z], z_peers[d - 1])

    @task
    def outmap():
        v["out_map"] = by_group(
            nn(out_re[...].astype(bf16), first_half) - nn(out_im[...].astype(bf16), second_half)
        )
        skip_rows = nn(skip[...], spread, HIGH)
        in_group = lax.div(iota((GROUPS, LOCAL), 1), CHAN) == iota((GROUPS, LOCAL), 0)
        v["skip_row"] = jnp.sum(jnp.where(in_group, skip_rows, 0.0), axis=0, keepdims=True)

    @task
    def far():
        c_plane, s_plane = power(float(ROWS * NY * NC))
        c_in, s_in = power(slot.astype(f32) * float(ROWS), v["log_before"])
        c_mid, s_mid = power(float(ROWS // 2 + 1))
        recv("C2", C2.at[1:])
        total = jnp.zeros((GROUPS, LANES), f32)
        for j in range(NZ):
            fade = jnp.exp(as_column(C2[j, GROUPS:]))
            step_on = fade * turned(total, c_plane, s_plane) + C2[j, 0:GROUPS]
            total = jnp.where(j < z, step_on, total)
        v["carry"] = turned(v["before"] + turned(total, c_in, s_in), c_mid, s_mid)

    @task
    def resp():
        for g in range(GROUPS):
            lanes = slice(LANES * g, LANES * (g + 1))
            full = YB[:, lanes] + jnp.exp(run_log[:, g : g + 1]) * v["carry"][g : g + 1]
            YB[:, lanes] = turned(full, ST[0, :, lanes], ST[1, :, lanes])
        response = nt(YB[...].astype(bf16), v["out_map"]) + v["skip_row"] * drive.astype(f32)
        MX[x] = jax.nn.gelu(response).astype(bf16)

    @task
    def m():
        for d in range(1, NX):
            send("M", "M", MX.at[x], MX.at[x], x_peers[d - 1])

    half = OWN // 2

    @task
    def r0():
        loads[3].wait()
        send("R", "R", RA.at[x], RA.at[x], x_peers[0])
        send("R", "R", RA.at[x], RA.at[x], x_peers[2])

    @task
    def r1():
        recv("R", RA.at[2:])
        send("Q", "Q", RA.at[xr(-1), 0:half], RA.at[xr(-1), 0:half], x_peers[0])
        send("Q", "Q", RA.at[xr(1), half:], RA.at[xr(1), half:], x_peers[2])

    @task
    def r2():
        recv("Q", RA.at[0])
        loads[4].wait()

    @task
    def proj():
        recv("M", MX.at[1:])
        mixed = [MX[q].astype(f32) for q in range(NX)]
        total = sum(jnp.sum(m * m, axis=1, keepdims=True) for m in mixed)
        scale = lax.rsqrt(total / float(LOCAL * NX) + eps)
        gains = mix_gain[...]
        normed = jnp.concatenate(
            [
                (mixed[q] * scale * gains[:, LOCAL * q : LOCAL * (q + 1)]).astype(bf16)
                for q in range(NX)
            ],
            axis=1,
        )
        squares = jnp.zeros((ROWS, 1), f32)
        for k in range(4):
            lanes = slice(512 * k, 512 * (k + 1))
            piece = nn(normed, WO[:, lanes]) + RA[:, :, lanes].reshape(ROWS, 512).astype(f32)
            RM[:, lanes] = piece
            squares = squares + jnp.sum(piece * piece, axis=1, keepdims=True)
        scale = lax.rsqrt(squares / float(D) + eps)
        for k in range(4):
            lanes = slice(512 * k, 512 * (k + 1))
            X[:, lanes] = (RM[:, lanes] * scale * ffn_gain[:, lanes]).astype(bf16)

    def column_slice(k):
        return pl.ds(pl.multiple_of(zr(PLANES[k]) * ROWS, ROWS), ROWS)

    def first(k):
        piece = X[:, column_slice(k)]
        for m, store in ((0, GA), (1, UA)):
            product = nn(piece, G[m, zr(PLANES[k])].reshape(ROWS, HID))
            store[...] = product if k == 0 else store[...] + product

    @task
    def hidden():
        HB[...] = (silu(GA[...]) * UA[...]).astype(bf16)

    def second(k):
        part = nt(HB[...], G[2, zr(PLANES[k])].reshape(ROWS, HID))
        PT[:, :, column_slice(k)] = part.astype(bf16).reshape(NX, OWN, ROWS)

    def part_slice(k, side):
        return pl.ds(pl.multiple_of(zr(PLANES[k]) * ROWS + 128 * side, 128), 128)

    def scat(k):
        if k in DIRECT:
            cols = column_slice(k)
            for d in (2, 1, 3):
                send("T", f"S{k}", PT.at[xr(d), :, cols], RT.at[DIRECT.index(k), x], x_peers[d - 1])
            return
        for side, to in ((0, x_peers[0]), (1, x_peers[2])):
            send("S", f"S{k}", PT.at[xr(2), :, part_slice(k, side)], RB.at[k, side], to)
        if k in RELAY:
            near(k, "W")

    def near(k, kind):
        cols = column_slice(k)
        send(kind, f"{kind}{k}", PT.at[xr(1), :, cols], RS.at[0, :, cols], x_peers[0])
        send(kind, f"{kind}{k}", PT.at[xr(-1), :, cols], RS.at[1, :, cols], x_peers[2])

    def pass_(k):
        recv(f"S{k}", RB.at[k])
        if k in RELAY:
            n = RELAY.index(k)
            for side, to in ((0, x_peers[0]), (1, x_peers[2])):
                send("U", f"V{k}", RB.at[k, side], RQ.at[n, side], to)
            return
        for side, dx in ((0, 1), (1, -1)):
            lanes = part_slice(k, side)
            sum_ = PT[xr(dx), :, lanes].astype(f32) + RB[k, side].astype(f32)
            PT[xr(dx), :, lanes] = sum_.astype(bf16)
        near(k, "V")

    def fin(k):
        cols = column_slice(k)
        ffn = PT[x, :, cols].astype(f32)
        if k in DIRECT:
            n = DIRECT.index(k)
            recv(f"S{k}", RT.at[n, 1:])
            for d in range(1, NX):
                ffn = ffn + RT[n, xr(d)].astype(f32)
        else:
            recv(f"W{k}" if k in RELAY else f"V{k}", RS.at[:, :, 0:ROWS])
            ffn = ffn + RS[0, :, cols].astype(f32) + RS[1, :, cols].astype(f32)
        if k in RELAY:
            n = RELAY.index(k)
            recv(f"V{k}", RQ.at[n])
            ffn = ffn + jnp.concatenate([RQ[n, 0], RQ[n, 1]], axis=1).astype(f32)
        kept = RM[pl.ds(pl.multiple_of(x * OWN, OWN), OWN), cols]
        out[:, cols] = (kept + 0.5 * ffn).astype(bf16)

    for k in range(NZ):
        tasks[f"first{k}"] = functools.partial(first, k)
        tasks[f"second{k}"] = functools.partial(second, k)
        tasks[f"scat{k}"] = functools.partial(scat, k)
        tasks[f"pass{k}"] = functools.partial(pass_, k)
        tasks[f"fin{k}"] = functools.partial(fin, k)

    for name in ORDER:
        with jax.named_scope(name):
            tasks[name]()
    with jax.named_scope("drain"):
        assert len(groups) == N_GROUPS
        for drain in drains:
            drain()
        sent("C1", C1.at[1:])
        sent("C2", C2.at[1:])
        sent("M", MX.at[1:])
        sent("R", RA.at[2:])
        sent("Q", RA.at[0])
        passed = NZ - len(DIRECT)
        summed = passed - len(RELAY)
        sent("S", RB.at[0:passed])
        sent("V", RS.at[:, :, 0 : summed * ROWS])
        if DIRECT:
            sent("T", RT.at[:, 1:])
        if RELAY:
            sent("W", RS.at[:, :, 0 : len(RELAY) * ROWS])
            sent("U", RQ)


def per_device(
    resid, mix_in, decay_rate, turn_rate, forget, input_real, input_imag, output_real, output_imag,
    skip_gain, mix_gain, w_out, ffn_gain, gating_matrix, w_up, w_down,
):
    operands = (
        resid, mix_in, forget.T, decay_rate, turn_rate,
        input_real.transpose(0, 2, 1).reshape(-1, STATE),
        input_imag.transpose(0, 2, 1).reshape(-1, STATE),
        output_real.reshape(-1, STATE), output_imag.reshape(-1, STATE),
        skip_gain, mix_gain.reshape(1, -1), w_out, ffn_gain.reshape(1, -1),
        gating_matrix, w_up, w_down.T,
    )
    own = [pltpu.VMEM(operands[k].shape, operands[k].dtype) for k in (*range(1, 11), 12)]
    return pl.pallas_call(
        kernel,
        out_shape=jax.ShapeDtypeStruct((OWN, D), bf16),
        in_specs=[pl.BlockSpec(memory_space=pl.ANY)] * len(operands),
        out_specs=pl.BlockSpec(memory_space=pltpu.VMEM),
        scratch_shapes=own + [
            pltpu.VMEM((3, NZ, NY, NC, SHARD, HID), bf16),
            pltpu.VMEM((NX, OWN, D), bf16),
            pltpu.VMEM((LOCAL * NX, D), bf16),
            pltpu.VMEM((NX, ROWS, LOCAL), bf16),
            pltpu.VMEM((ROWS, D), bf16),
            pltpu.VMEM((ROWS, D), f32),
            pltpu.VMEM((ROWS, HID), f32),
            pltpu.VMEM((ROWS, HID), f32),
            pltpu.VMEM((ROWS, HID), bf16),
            pltpu.VMEM((NX, OWN, D), bf16),
            pltpu.VMEM((2, OWN, D), bf16),
            pltpu.VMEM((NZ, 2, OWN, 128), bf16),
            pltpu.VMEM((max(len(RELAY), 1), 2, OWN, 128), bf16),
            pltpu.VMEM((max(len(DIRECT), 1), NX, OWN, ROWS), bf16),
            pltpu.VMEM((ROWS, WIDE), f32),
            pltpu.VMEM((ROWS, WIDE), f32),
            pltpu.VMEM((2, ROWS, WIDE), f32),
            pltpu.VMEM((NY * NC, GROUPS + 1, LANES), f32),
            pltpu.VMEM((NZ, GROUPS + 1, LANES), f32),
            pltpu.SemaphoreType.DMA((N_GROUPS,)),
            pltpu.SemaphoreType.DMA((len(ARRIVALS),)),
            pltpu.SemaphoreType.DMA((3,)),
            pltpu.SemaphoreType.DMA((len(own),)),
            pltpu.SemaphoreType.REGULAR((3,)),
        ],
        compiler_params=pltpu.CompilerParams(
            collective_id=0, has_side_effects=True, vmem_limit_bytes=52 * 1024 * 1024
        ),
    )(*[pltpu.with_memory_space_constraint(operand, pltpu.HBM) for operand in operands])


def solution(mesh):
    placed = (
        P(("sp", "tp"), None),
        P("sp", "tp"),
        P("tp", None),
        P("tp", None),
        P("sp", "tp"),
        P("tp", None, None),
        P("tp", None, None),
        P("tp", None, None),
        P("tp", None, None),
        P("tp", None),
        P(),
        P(),
        P(),
        P("sp", "tp"),
        P("sp", "tp"),
        P("tp", "sp"),
    )
    return jax.shard_map(
        per_device, mesh=mesh, in_specs=placed, out_specs=P(("sp", "tp"), None), check_vma=False
    )
```

```python
import functools

import jax
import jax.numpy as jnp
from jax import lax
from jax.experimental import pallas as pl
from jax.experimental.pallas import tpu as pltpu
from jax.sharding import PartitionSpec as P

f32, bf16 = jnp.float32, jnp.bfloat16
HIGH = lax.Precision.HIGHEST
MESH = pl.DeviceIdType.MESH
eps = 1e-06
NZ, NY, NC, NX = 8, 4, 2, 4
ROWS = 256
GROUPS, CHAN, STATE = 8, 16, 64
LANES = 2 * STATE
WIDE = GROUPS * LANES
LOCAL = GROUPS * CHAN
D, HID, SHARD = 2048, 1408, 32
OWN = ROWS // NX
PATH_A = ((512, 256), (640, 384))
PHASES = ((0, 2), (2, 1))
PLANES = (0, -1, 1, -2, 2, -3, 3, 4)
OPENING = (58, 0, 1, 84, 3)
RELAY = (7,)
DIRECT = ()
N_GROUPS, N_ARRIVALS = 21, 47
ORDER = (
    128, 119, 120, 124, 121, 61, 26, 59, 2, 4, 6, 30, 85, 116, 122, 129, 117, 27, 118, 5, 123, 34,
    8, 10, 31, 28, 11, 42, 38, 130, 29, 9, 35, 125, 126, 127, 65, 15, 43, 7, 32, 16, 46, 50, 14, 33,
    36, 39, 13, 37, 12, 44, 131, 60, 62, 21, 54, 133, 138, 45, 153, 19, 51, 143, 18, 40, 64, 88, 63,
    86, 17, 92, 66, 41, 148, 87, 55, 24, 20, 23, 52, 47, 69, 96, 89, 67, 93, 53, 163, 22, 100, 68,
    25, 56, 71, 48, 74, 108, 97, 70, 72, 57, 168, 90, 73, 94, 104, 49, 158, 132, 79, 112, 134, 135,
    91, 139, 109, 98, 140, 75, 95, 144, 77, 76, 145, 101, 105, 78, 99, 149, 113, 150, 136, 110, 141,
    80, 102, 146, 82, 106, 81, 111, 164, 83, 114, 165, 103, 154, 155, 151, 107, 159, 160, 137, 115,
    169, 170, 142, 147, 166, 156, 152, 161, 171, 167, 157, 162, 172,
)
ARRIVALS = (
    0, 1, 2, 3, 4, 5, 6, 7, 8, 9, 10, 11, 12, 13, 14, 15, 16, 17, 18, 19, 1, 20, 21, 22, 23, 2, 8,
    3, 24, 10, 25, 26, 12, 17, 11, 27, 13, 14, 28, 18, 23, 1, 29, 4, 27, 8, 21, 7, 30, 24, 22, 20,
    23, 2, 3, 31, 32, 11, 0, 33, 17, 34, 27, 28, 9, 10, 1, 29, 15, 8, 18, 32, 21, 23, 2, 14, 22, 20,
    31, 27, 7, 35, 0, 3, 5, 28, 32, 36, 26, 29, 9, 37, 10, 15, 18, 1, 38, 16, 27, 39, 23, 40, 41,
    32, 42, 43, 44, 45, 5, 46, 37, 36, 38, 16,
)


def iota(shape, dim):
    return lax.broadcasted_iota(jnp.int32, shape, dim)


def where_one(test):
    return jnp.where(test, 1.0, 0.0).astype(f32)


def nt(a, b, precision=None):
    return lax.dot_general(
        a, b, (((1,), (1,)), ((), ())), precision=precision, preferred_element_type=f32
    )


def nn(a, b, precision=None):
    return lax.dot_general(
        a, b, (((1,), (0,)), ((), ())), precision=precision, preferred_element_type=f32
    )


def swap(a):
    return pltpu.roll(a, STATE, 1)


def sign_lanes(shape):
    return jnp.where(iota(shape, 1) < STATE, -1.0, 1.0).astype(f32)


def turned(a, c, s):
    return a * c + swap(a) * s


def silu(x):
    return x * jax.nn.sigmoid(x)


def kernel(
    resid, mix_h, forget_h, decay_h, turn_h, in_re_h, in_im_h, out_re_h, out_im_h, skip_h, mix_gain_h,
    w_out, ffn_gain_h, gate, up, down_t, out,
    mix, forget_t, decay, turn, in_re, in_im, out_re, out_im, skip, mix_gain, ffn_gain,
    G, RA, WO, MX, X, RM, GA, UA, HB, PT, RS, RB, RQ, RT, UB, YB, ST, C1, C2,
    send_sem, recv_sem, local_sem, entry_sem, hello_sem,
):
    me, x = lax.axis_index("sp"), lax.axis_index("tp")
    c = lax.rem(me, NC)
    y = lax.rem(lax.div(me, NC), NY)
    z = lax.div(me, NC * NY)
    slot = lax.rem(me, NC * NY)

    def at_sp(zz, yy, cc):
        return {"sp": (zz * NY + yy) * NC + cc}

    def zr(d):
        return lax.rem(z + (d + NZ), NZ)

    def yr(d):
        return lax.rem(y + (d + NY), NY)

    def xr(d):
        return lax.rem(x + (d + NX), NX)

    plane_peers = [{"sp": z * NY * NC + lax.rem(slot + d, NY * NC)} for d in range(1, NY * NC)]
    z_peers = [at_sp(zr(d), y, c) for d in range(1, NZ)]
    x_peers = [{"tp": xr(d)} for d in range(1, NX)]
    yp, ym = at_sp(z, yr(1), c), at_sp(z, yr(-1), c)
    zp, zm = at_sp(zr(1), y, c), at_sp(zr(-1), y, c)
    partner = at_sp(z, y, 1 - c)

    groups, arrivals = {}, {}

    def send(group, name, src, dst, to):
        k = groups.setdefault(group, len(groups))
        n = ARRIVALS[arrivals.setdefault(name, len(arrivals))]
        pltpu.make_async_remote_copy(
            src_ref=src, dst_ref=dst, send_sem=send_sem.at[k], recv_sem=recv_sem.at[n],
            device_id=to, device_id_type=MESH,
        ).start()

    def waiter(k, n, bytes_of):
        return pltpu.make_async_remote_copy(
            src_ref=bytes_of, dst_ref=bytes_of, send_sem=send_sem.at[k], recv_sem=recv_sem.at[n],
            device_id=partner, device_id_type=MESH,
        )

    def recv(name, bytes_of):
        waiter(0, ARRIVALS[arrivals[name]], bytes_of).wait_recv()

    def sent(group, bytes_of):
        waiter(groups[group], 0, bytes_of).wait_send()

    tasks, drains = {}, []

    def task(f):
        tasks[f.__name__] = f
        return f

    def gather_tasks(p):
        first, count = PHASES[p]
        cut, cut_plus = PATH_A[p]
        tiles = (HID - cut) // 128
        few, many = cut + tiles // 2 * 128, cut + (tiles - tiles // 2) * 128
        path_a, path_a1, path_a2 = (0, cut), (0, cut_plus), (cut_plus, cut)
        path_b = (cut, HID)

        def halves(odd):
            middle = many if odd else few
            return (cut, middle), (middle, HID)

        def block(dz, dy, lanes):
            return G.at[
                pl.ds(first, count), zr(dz), yr(dy), c, :, pl.ds(lanes[0], lanes[1] - lanes[0])
            ]

        def sized(planes, rows, lanes):
            return G.at[
                pl.ds(first, count), pl.ds(0, planes), pl.ds(0, rows), c, :,
                pl.ds(lanes[0], lanes[1] - lanes[0]),
            ]

        def go(name, ref, to):
            send(f"{p}{name[0]}", f"{p}{name}", ref, ref, to)

        def both(name, ref, plus, minus):
            go(name, ref, plus)
            go(name, ref, minus)

        def got(name, lanes, count_of=1):
            recv(f"{p}{name}", sized(1, count_of, lanes))

        def a0():
            both("A0", block(0, 0, path_a), yp, ym)

        def b0():
            both("B1", block(0, 0, path_b), zp, zm)

        def a1():
            got("A0", path_a, 2)
            go("A1", block(0, -1, path_a1), yp)
            go("A1", block(0, 1, path_a2), ym)

        def s0():
            both("Z01", block(0, 0, path_a), zp, zm)

        def s1():
            both("Z11", block(0, -1, path_a), zp, zm)
            both("Z31", block(0, 1, path_a), zp, zm)

        def s2():
            got("A1", path_a)
            both("Z21", block(0, 2, path_a), zp, zm)

        def q(row, s):
            dy = (0, -1, 2, 1)[row]
            got(f"Z{row}{s}", path_a, 2 if s < 4 else 1)
            if s < 3 or (s == 3 and row in (0, 1)):
                go(f"Z{row}{s + 1}", block(-s, dy, path_a), zp)
            if s < 3 or (s == 3 and row in (2, 3)):
                go(f"Z{row}{s + 1}", block(s, dy, path_a), zm)

        def b(s):
            got(f"B{s}", path_b, 2 if s < 4 else 1)
            plus, minus = (path_b, path_b) if s < 3 else halves(p)
            if s < 4:
                go(f"B{s + 1}", block(-s, 0, plus), zp)
                go(f"B{s + 1}", block(s, 0, minus), zm)

        def y_(k):
            both(f"Y{k}", block(PLANES[k], 0, path_b), yp, ym)

        def f(k):
            got(f"Y{k}", path_b, 2)
            plus, minus = halves(k % 2)
            go(f"F{k}", block(PLANES[k], -1, plus), yp)
            go(f"F{k}", block(PLANES[k], 1, minus), ym)

        def d(k):
            got(f"F{k}", path_b)
            go(f"D{k}", G.at[pl.ds(first, count), zr(PLANES[k]), :, c], partner)

        def e(k):
            recv(f"{p}D{k}", sized(1, NY, (0, HID)))

        def all_sent():
            for kind, planes, rows, lanes in (
                ("A", 1, 3, path_a), ("Z", 7, 4, path_a), ("Y", 8, 2, path_b), ("F", 8, 1, path_b),
                ("B", 7, 1, path_b), ("D", 8, 4, (0, HID)),
            ):
                sent(f"{p}{kind}", sized(planes, rows, lanes))

        drains.append(all_sent)
        for name, f_ in (("a0", a0), ("b0", b0), ("a1", a1), ("s0", s0), ("s1", s1), ("s2", s2)):
            tasks[f"{p}{name}"] = f_
        for s in range(1, 5):
            tasks[f"{p}b{s}"] = functools.partial(b, s)
            for row in range(NY):
                tasks[f"{p}q{row}{s}"] = functools.partial(q, row, s)
        for k in range(NZ):
            tasks[f"{p}y{k}"] = functools.partial(y_, k)
            tasks[f"{p}f{k}"] = functools.partial(f, k)
            tasks[f"{p}d{k}"] = functools.partial(d, k)
            tasks[f"{p}e{k}"] = functools.partial(e, k)

    for p in range(len(PHASES)):
        gather_tasks(p)

    barrier = pltpu.get_barrier_semaphore()
    peers = plane_peers + [zp, zm] + x_peers
    for peer in peers:
        pl.semaphore_signal(barrier, inc=1, device_id=peer, device_id_type=MESH)
    small = [
        (mix_h, mix), (forget_h, forget_t), (decay_h, decay), (turn_h, turn), (in_re_h, in_re),
        (in_im_h, in_im), (out_re_h, out_re), (out_im_h, out_im), (skip_h, skip),
        (mix_gain_h, mix_gain), (ffn_gain_h, ffn_gain),
    ]
    early = [pltpu.make_async_copy(a, b, entry_sem.at[k]) for k, (a, b) in enumerate(small)]
    loads = [
        pltpu.make_async_copy(gate, G.at[0, z, y, c], local_sem.at[0]),
        pltpu.make_async_copy(up, G.at[1, z, y, c], local_sem.at[0]),
        pltpu.make_async_copy(down_t, G.at[2, z, y, c], local_sem.at[0]),
        pltpu.make_async_copy(resid, RA.at[x], local_sem.at[1]),
        pltpu.make_async_copy(w_out, WO, local_sem.at[2]),
    ]
    for load in loads[:3] + early + loads[3:]:
        load.start()

    def hello(n):
        for peer in (zp, zm):
            pl.semaphore_signal(hello_sem.at[n], inc=1, device_id=peer, device_id_type=MESH)

    def met(n):
        pl.semaphore_wait(hello_sem.at[n], 2)
        if n < 2:
            hello(n + 1)

    for n in range(3):
        tasks[f"h{n}"] = functools.partial(met, n)

    with jax.named_scope("entry"):
        pl.semaphore_wait(barrier, len(peers))
        own_weights = G.at[:, z, y, c]
        pltpu.make_async_copy(own_weights, own_weights, local_sem.at[0]).wait()
        hello(0)
    with jax.named_scope("opening"):
        for task_number in OPENING:
            list(tasks.values())[task_number]()
        for load in early:
            load.wait()
    with jax.named_scope("prep"):
        drive = mix[...]
        spread = where_one(lax.rem(iota((CHAN, LOCAL), 1), CHAN) == iota((CHAN, LOCAL), 0))
        twice = where_one(lax.rem(iota((STATE, LANES), 1), STATE) == iota((STATE, LANES), 0))
        rate2 = nn(decay[...], twice, HIGH)
        turn2 = nn(turn[...], twice, HIGH)
        lower = iota((ROWS, ROWS), 0) >= iota((ROWS, ROWS), 1)
        lower_one = where_one(lower)
        forget_rows = forget_t[...]
        run_log = nt(lower_one, forget_rows, HIGH)
        run_log_t = nt(forget_rows, lower_one, HIGH)
        w = 2.0 * rate2
        series = 1.0 + w / 6.0
        for k in (5.0, 4.0, 3.0, 2.0):
            series = 1.0 + (w / k) * series
        in_factor = jnp.sqrt(-(w * series))
        first_half = where_one(iota((STATE, LANES), 1) == iota((STATE, LANES), 0)).astype(bf16)
        second_half = where_one(
            iota((STATE, LANES), 1) == iota((STATE, LANES), 0) + STATE
        ).astype(bf16)
        row_group = lax.div(iota((LOCAL, LANES), 0), CHAN)

        def by_group(rows):
            return jnp.concatenate(
                [jnp.where(row_group == g, rows, 0.0).astype(bf16) for g in range(GROUPS)], axis=1
            )

        in_map = by_group(
            nn(in_re[...].astype(bf16), first_half) + nn(in_im[...].astype(bf16), second_half)
        )
        UB[...] = nn(drive, in_map)
        sign = sign_lanes((1, LANES))
        sign8 = sign_lanes((GROUPS, LANES))
        coarse = (iota((16, LANES), 0) - 8).astype(f32) * 16.0
        fine = iota((16, LANES), 0).astype(f32)
        centred = (iota((ROWS, LANES), 0) - ROWS // 2).astype(f32)

    def phase_tables(g):
        angle = turn2[g : g + 1]
        ca, sa = jnp.cos(angle * coarse), jnp.sin(angle * coarse)
        cb, sb = jnp.cos(angle * fine), jnp.sin(angle * fine)
        cos = [ca[k : k + 1] * cb - sa[k : k + 1] * sb for k in range(16)]
        sin = [sa[k : k + 1] * cb + ca[k : k + 1] * sb for k in range(16)]
        return jnp.concatenate(cos, axis=0), jnp.concatenate(sin, axis=0) * sign

    def power(n, log=0.0):
        size = jnp.exp(rate2 * n + log)
        return size * jnp.cos(turn2 * n), size * jnp.sin(turn2 * n) * sign8

    v = {}
    on_diagonal = iota((GROUPS, LANES), 0) == iota((GROUPS, LANES), 1)

    def as_row(column):
        return jnp.sum(jnp.where(on_diagonal, column, 0.0), axis=0, keepdims=True)

    def as_column(row):
        return jnp.sum(jnp.where(on_diagonal, row, 0.0), axis=1, keepdims=True)

    @task
    def local():
        ends = []
        last = run_log[ROWS - 1 : ROWS]
        for g in range(GROUPS):
            lanes = slice(LANES * g, LANES * (g + 1))
            cos, sin = phase_tables(g)
            grow = jnp.exp(-rate2[g : g + 1] * centred) * in_factor[g : g + 1]
            b_g = UB[:, lanes]
            u = (b_g * cos - swap(b_g) * sin) * grow
            UB[:, lanes] = u
            fall = jnp.exp(rate2[g : g + 1] * centred)
            ST[0, :, lanes] = cos * fall
            ST[1, :, lanes] = sin * fall
            weight = jnp.exp(last[:, g : g + 1] - run_log[:, g : g + 1])
            total = jnp.sum(u * weight, axis=0, keepdims=True)
            at_end = slice(ROWS - 1, ROWS)
            ends.append(turned(total, ST[0, at_end, lanes], ST[1, at_end, lanes]))
        last_col = jnp.sum(
            jnp.where(iota((GROUPS, ROWS), 1) == ROWS - 1, run_log_t, 0.0), axis=1, keepdims=True
        )
        C1[slot, 0:GROUPS] = jnp.concatenate(ends, axis=0)
        C1[slot, GROUPS:] = as_row(last_col)

    @task
    def c1():
        for d in range(1, NY * NC):
            send("C1", "C1", C1.at[slot], C1.at[slot], plane_peers[d - 1])

    @task
    def masked():
        for g in range(GROUPS):
            lanes = slice(LANES * g, LANES * (g + 1))
            gap = run_log[:, g : g + 1] - run_log_t[g : g + 1]
            weights = jnp.where(lower, jnp.exp(jnp.minimum(gap, 0.0)), 0.0).astype(bf16)
            YB[:, lanes] = nn(weights, UB[:, lanes].astype(bf16))

    @task
    def carry():
        c_one, s_one = power(float(ROWS))
        recv("C1", C1.at[1:])
        acc = jnp.zeros((GROUPS, LANES), f32)
        log_acc = jnp.zeros((GROUPS, 1), f32)
        before, log_before = acc, log_acc
        for j in range(NY * NC):
            here = slot == j
            before = jnp.where(here, acc, before)
            log_before = jnp.where(here, log_acc, log_before)
            log_j = as_column(C1[j, GROUPS:])
            acc = jnp.exp(log_j) * turned(acc, c_one, s_one) + C1[j, 0:GROUPS]
            log_acc = log_acc + log_j
        C2[z, 0:GROUPS] = acc
        C2[z, GROUPS:] = as_row(log_acc)
        v["before"], v["log_before"] = before, log_before

    @task
    def c2():
        for d in range(1, NZ):
            send("C2", "C2", C2.at[z], C2.at[z], z_peers[d - 1])

    @task
    def outmap():
        v["out_map"] = by_group(
            nn(out_re[...].astype(bf16), first_half) - nn(out_im[...].astype(bf16), second_half)
        )
        skip_rows = nn(skip[...], spread, HIGH)
        in_group = lax.div(iota((GROUPS, LOCAL), 1), CHAN) == iota((GROUPS, LOCAL), 0)
        v["skip_row"] = jnp.sum(jnp.where(in_group, skip_rows, 0.0), axis=0, keepdims=True)

    @task
    def far():
        c_plane, s_plane = power(float(ROWS * NY * NC))
        c_in, s_in = power(slot.astype(f32) * float(ROWS), v["log_before"])
        c_mid, s_mid = power(float(ROWS // 2 + 1))
        recv("C2", C2.at[1:])
        total = jnp.zeros((GROUPS, LANES), f32)
        for j in range(NZ):
            fade = jnp.exp(as_column(C2[j, GROUPS:]))
            step_on = fade * turned(total, c_plane, s_plane) + C2[j, 0:GROUPS]
            total = jnp.where(j < z, step_on, total)
        v["carry"] = turned(v["before"] + turned(total, c_in, s_in), c_mid, s_mid)

    @task
    def resp():
        for g in range(GROUPS):
            lanes = slice(LANES * g, LANES * (g + 1))
            full = YB[:, lanes] + jnp.exp(run_log[:, g : g + 1]) * v["carry"][g : g + 1]
            YB[:, lanes] = turned(full, ST[0, :, lanes], ST[1, :, lanes])
        response = nt(YB[...].astype(bf16), v["out_map"]) + v["skip_row"] * drive.astype(f32)
        MX[x] = jax.nn.gelu(response).astype(bf16)

    @task
    def m():
        for d in range(1, NX):
            send("M", "M", MX.at[x], MX.at[x], x_peers[d - 1])

    half = OWN // 2

    @task
    def r0():
        loads[3].wait()
        send("R", "R", RA.at[x], RA.at[x], x_peers[0])
        send("R", "R", RA.at[x], RA.at[x], x_peers[2])

    @task
    def r1():
        recv("R", RA.at[2:])
        send("Q", "Q", RA.at[xr(-1), 0:half], RA.at[xr(-1), 0:half], x_peers[0])
        send("Q", "Q", RA.at[xr(1), half:], RA.at[xr(1), half:], x_peers[2])

    @task
    def r2():
        recv("Q", RA.at[0])
        loads[4].wait()

    @task
    def proj():
        recv("M", MX.at[1:])
        mixed = [MX[q].astype(f32) for q in range(NX)]
        total = sum(jnp.sum(m * m, axis=1, keepdims=True) for m in mixed)
        scale = lax.rsqrt(total / float(LOCAL * NX) + eps)
        gains = mix_gain[...]
        normed = jnp.concatenate(
            [
                (mixed[q] * scale * gains[:, LOCAL * q : LOCAL * (q + 1)]).astype(bf16)
                for q in range(NX)
            ],
            axis=1,
        )
        squares = jnp.zeros((ROWS, 1), f32)
        for k in range(4):
            lanes = slice(512 * k, 512 * (k + 1))
            piece = nn(normed, WO[:, lanes]) + RA[:, :, lanes].reshape(ROWS, 512).astype(f32)
            RM[:, lanes] = piece
            squares = squares + jnp.sum(piece * piece, axis=1, keepdims=True)
        scale = lax.rsqrt(squares / float(D) + eps)
        for k in range(4):
            lanes = slice(512 * k, 512 * (k + 1))
            X[:, lanes] = (RM[:, lanes] * scale * ffn_gain[:, lanes]).astype(bf16)

    def column_slice(k):
        return pl.ds(pl.multiple_of(zr(PLANES[k]) * ROWS, ROWS), ROWS)

    def first(k):
        piece = X[:, column_slice(k)]
        for m, store in ((0, GA), (1, UA)):
            product = nn(piece, G[m, zr(PLANES[k])].reshape(ROWS, HID))
            store[...] = product if k == 0 else store[...] + product

    @task
    def hidden():
        HB[...] = (silu(GA[...]) * UA[...]).astype(bf16)

    def second(k):
        part = nt(HB[...], G[2, zr(PLANES[k])].reshape(ROWS, HID))
        PT[:, :, column_slice(k)] = part.astype(bf16).reshape(NX, OWN, ROWS)

    def part_slice(k, side):
        return pl.ds(pl.multiple_of(zr(PLANES[k]) * ROWS + 128 * side, 128), 128)

    def scat(k):
        if k in DIRECT:
            cols = column_slice(k)
            for d in (2, 1, 3):
                send("T", f"S{k}", PT.at[xr(d), :, cols], RT.at[DIRECT.index(k), x], x_peers[d - 1])
            return
        for side, to in ((0, x_peers[0]), (1, x_peers[2])):
            send("S", f"S{k}", PT.at[xr(2), :, part_slice(k, side)], RB.at[k, side], to)
        if k in RELAY:
            near(k, "W")

    def near(k, kind):
        cols = column_slice(k)
        send(kind, f"{kind}{k}", PT.at[xr(1), :, cols], RS.at[0, :, cols], x_peers[0])
        send(kind, f"{kind}{k}", PT.at[xr(-1), :, cols], RS.at[1, :, cols], x_peers[2])

    def pass_(k):
        recv(f"S{k}", RB.at[k])
        if k in RELAY:
            n = RELAY.index(k)
            for side, to in ((0, x_peers[0]), (1, x_peers[2])):
                send("U", f"V{k}", RB.at[k, side], RQ.at[n, side], to)
            return
        for side, dx in ((0, 1), (1, -1)):
            lanes = part_slice(k, side)
            sum_ = PT[xr(dx), :, lanes].astype(f32) + RB[k, side].astype(f32)
            PT[xr(dx), :, lanes] = sum_.astype(bf16)
        near(k, "V")

    def fin(k):
        cols = column_slice(k)
        ffn = PT[x, :, cols].astype(f32)
        if k in DIRECT:
            n = DIRECT.index(k)
            recv(f"S{k}", RT.at[n, 1:])
            for d in range(1, NX):
                ffn = ffn + RT[n, xr(d)].astype(f32)
        else:
            recv(f"W{k}" if k in RELAY else f"V{k}", RS.at[:, :, 0:ROWS])
            ffn = ffn + RS[0, :, cols].astype(f32) + RS[1, :, cols].astype(f32)
        if k in RELAY:
            n = RELAY.index(k)
            recv(f"V{k}", RQ.at[n])
            ffn = ffn + jnp.concatenate([RQ[n, 0], RQ[n, 1]], axis=1).astype(f32)
        kept = RM[pl.ds(pl.multiple_of(x * OWN, OWN), OWN), cols]
        out[:, cols] = (kept + 0.5 * ffn).astype(bf16)

    for k in range(NZ):
        tasks[f"first{k}"] = functools.partial(first, k)
        tasks[f"second{k}"] = functools.partial(second, k)
        tasks[f"scat{k}"] = functools.partial(scat, k)
        tasks[f"pass{k}"] = functools.partial(pass_, k)
        tasks[f"fin{k}"] = functools.partial(fin, k)

    table = list(tasks)
    for task_number in ORDER:
        with jax.named_scope(table[task_number]):
            tasks[table[task_number]]()
    with jax.named_scope("drain"):
        assert len(groups) == N_GROUPS and len(arrivals) == len(ARRIVALS)
        for drain in drains:
            drain()
        sent("C1", C1.at[1:])
        sent("C2", C2.at[1:])
        sent("M", MX.at[1:])
        sent("R", RA.at[2:])
        sent("Q", RA.at[0])
        passed = NZ - len(DIRECT)
        summed = passed - len(RELAY)
        sent("S", RB.at[0:passed])
        sent("V", RS.at[:, :, 0 : summed * ROWS])
        if DIRECT:
            sent("T", RT.at[:, 1:])
        if RELAY:
            sent("W", RS.at[:, :, 0 : len(RELAY) * ROWS])
            sent("U", RQ)


def per_device(
    resid, mix_in, decay_rate, turn_rate, forget, input_real, input_imag, output_real, output_imag,
    skip_gain, mix_gain, w_out, ffn_gain, gating_matrix, w_up, w_down,
):
    operands = (
        resid, mix_in, forget.T, decay_rate, turn_rate,
        input_real.transpose(0, 2, 1).reshape(-1, STATE),
        input_imag.transpose(0, 2, 1).reshape(-1, STATE),
        output_real.reshape(-1, STATE), output_imag.reshape(-1, STATE),
        skip_gain, mix_gain.reshape(1, -1), w_out, ffn_gain.reshape(1, -1),
        gating_matrix, w_up, w_down.T,
    )
    own = [pltpu.VMEM(operands[k].shape, operands[k].dtype) for k in (*range(1, 11), 12)]
    return pl.pallas_call(
        kernel,
        out_shape=jax.ShapeDtypeStruct((OWN, D), bf16),
        in_specs=[pl.BlockSpec(memory_space=pl.ANY)] * len(operands),
        out_specs=pl.BlockSpec(memory_space=pltpu.VMEM),
        scratch_shapes=own + [
            pltpu.VMEM((3, NZ, NY, NC, SHARD, HID), bf16),
            pltpu.VMEM((NX, OWN, D), bf16),
            pltpu.VMEM((LOCAL * NX, D), bf16),
            pltpu.VMEM((NX, ROWS, LOCAL), bf16),
            pltpu.VMEM((ROWS, D), bf16),
            pltpu.VMEM((ROWS, D), f32),
            pltpu.VMEM((ROWS, HID), f32),
            pltpu.VMEM((ROWS, HID), f32),
            pltpu.VMEM((ROWS, HID), bf16),
            pltpu.VMEM((NX, OWN, D), bf16),
            pltpu.VMEM((2, OWN, D), bf16),
            pltpu.VMEM((NZ, 2, OWN, 128), bf16),
            pltpu.VMEM((max(len(RELAY), 1), 2, OWN, 128), bf16),
            pltpu.VMEM((max(len(DIRECT), 1), NX, OWN, ROWS), bf16),
            pltpu.VMEM((ROWS, WIDE), f32),
            pltpu.VMEM((ROWS, WIDE), f32),
            pltpu.VMEM((2, ROWS, WIDE), f32),
            pltpu.VMEM((NY * NC, GROUPS + 1, LANES), f32),
            pltpu.VMEM((NZ, GROUPS + 1, LANES), f32),
            pltpu.SemaphoreType.DMA((N_GROUPS,)),
            pltpu.SemaphoreType.DMA((N_ARRIVALS,)),
            pltpu.SemaphoreType.DMA((3,)),
            pltpu.SemaphoreType.DMA((len(own),)),
            pltpu.SemaphoreType.REGULAR((3,)),
        ],
        compiler_params=pltpu.CompilerParams(
            collective_id=0, has_side_effects=True, vmem_limit_bytes=52 * 1024 * 1024
        ),
    )(*[pltpu.with_memory_space_constraint(operand, pltpu.HBM) for operand in operands])


def solution(mesh):
    placed = (
        P(("sp", "tp"), None),
        P("sp", "tp"),
        P("tp", None),
        P("tp", None),
        P("sp", "tp"),
        P("tp", None, None),
        P("tp", None, None),
        P("tp", None, None),
        P("tp", None, None),
        P("tp", None),
        P(),
        P(),
        P(),
        P("sp", "tp"),
        P("sp", "tp"),
        P("tp", "sp"),
    )
    return jax.shard_map(
        per_device, mesh=mesh, in_specs=placed, out_specs=P(("sp", "tp"), None), check_vma=False
    )
```

```python
import functools

import jax
import jax.numpy as jnp
from jax import lax
from jax.experimental import pallas as pl
from jax.experimental.pallas import tpu as pltpu
from jax.sharding import PartitionSpec as P

f32, bf16 = jnp.float32, jnp.bfloat16
HIGH = lax.Precision.HIGHEST
MESH = pl.DeviceIdType.MESH
eps = 1e-06
NZ, NY, NC, NX = 8, 4, 2, 4
ROWS = 256
GROUPS, CHAN, STATE = 8, 16, 64
LANES = 2 * STATE
WIDE = GROUPS * LANES
LOCAL = GROUPS * CHAN
D, HID, SHARD = 2048, 1408, 32
OWN = ROWS // NX
PATH_A = ((512, 256), (640, 384))
PHASES = ((0, 2), (2, 1))
PLANES = (0, -1, 1, -2, 2, -3, 3, 4)
OPENING = (58, 0, 1, 84, 3)
RELAY = (7,)
DIRECT = ()
N_GROUPS, N_ARRIVALS = 21, 47
ORDER = (
    128, 119, 120, 124, 121, 61, 26, 59, 2, 4, 6, 30, 85, 116, 122, 129, 117, 27, 118, 5, 123, 34,
    8, 10, 31, 28, 11, 42, 38, 130, 29, 9, 35, 125, 126, 127, 65, 15, 43, 7, 32, 16, 46, 50, 14, 33,
    36, 39, 13, 37, 12, 44, 131, 60, 62, 21, 54, 133, 138, 45, 153, 19, 51, 143, 18, 40, 64, 88, 63,
    86, 17, 92, 66, 41, 148, 87, 55, 24, 20, 23, 52, 47, 69, 96, 89, 67, 93, 53, 163, 22, 100, 68,
    25, 56, 71, 48, 74, 108, 97, 70, 72, 57, 168, 90, 73, 94, 104, 49, 158, 132, 79, 112, 134, 135,
    91, 139, 109, 98, 140, 75, 95, 144, 77, 76, 145, 101, 105, 78, 99, 149, 113, 150, 136, 110, 141,
    80, 102, 146, 82, 106, 81, 111, 164, 83, 114, 165, 103, 154, 155, 151, 107, 159, 160, 137, 115,
    169, 170, 142, 147, 166, 156, 152, 161, 171, 167, 157, 162, 172,
)
ARRIVALS = (
    0, 1, 2, 3, 4, 5, 6, 7, 8, 9, 10, 11, 12, 13, 14, 15, 16, 17, 18, 19, 1, 20, 21, 22, 23, 2, 8,
    3, 24, 10, 25, 26, 12, 17, 11, 27, 13, 14, 28, 18, 23, 1, 29, 4, 27, 8, 21, 7, 30, 24, 22, 20,
    23, 2, 3, 31, 32, 11, 0, 33, 17, 34, 27, 28, 9, 10, 1, 29, 15, 8, 18, 32, 21, 23, 2, 14, 22, 20,
    31, 27, 7, 35, 0, 3, 5, 28, 32, 36, 26, 29, 9, 37, 10, 15, 18, 1, 38, 16, 27, 39, 23, 40, 41,
    32, 42, 43, 44, 45, 5, 46, 37, 36, 38, 16,
)


def iota(shape, dim):
    return lax.broadcasted_iota(jnp.int32, shape, dim)


def where_one(test):
    return jnp.where(test, 1.0, 0.0).astype(f32)


def nt(a, b, precision=None):
    return lax.dot_general(
        a, b, (((1,), (1,)), ((), ())), precision=precision, preferred_element_type=f32
    )


def nn(a, b, precision=None):
    return lax.dot_general(
        a, b, (((1,), (0,)), ((), ())), precision=precision, preferred_element_type=f32
    )


def swap(a):
    return pltpu.roll(a, STATE, 1)


def sign_lanes(shape):
    return jnp.where(iota(shape, 1) < STATE, -1.0, 1.0).astype(f32)


def turned(a, c, s):
    return a * c + swap(a) * s


def silu(x):
    return x * jax.nn.sigmoid(x)


def kernel(
    resid, mix_h, forget_h, decay_h, turn_h, in_re_h, in_im_h, out_re_h, out_im_h, skip_h, mix_gain_h,
    w_out, ffn_gain_h, gate, up, down_t, out,
    mix, forget_t, decay, turn, in_re, in_im, out_re, out_im, skip, mix_gain, ffn_gain,
    G, RA, WO, MX, X, RM, GA, UA, HB, PT, RS, RB, RQ, RT, UB, YB, ST, C1, C2,
    send_sem, recv_sem, local_sem, entry_sem, hello_sem,
):
    me, x = lax.axis_index("sp"), lax.axis_index("tp")
    c = lax.rem(me, NC)
    y = lax.rem(lax.div(me, NC), NY)
    z = lax.div(me, NC * NY)
    slot = lax.rem(me, NC * NY)

    def at_sp(zz, yy, cc):
        return {"sp": (zz * NY + yy) * NC + cc}

    def zr(d):
        return lax.rem(z + (d + NZ), NZ)

    def yr(d):
        return lax.rem(y + (d + NY), NY)

    def xr(d):
        return lax.rem(x + (d + NX), NX)

    plane_peers = [{"sp": z * NY * NC + lax.rem(slot + d, NY * NC)} for d in range(1, NY * NC)]
    z_peers = [at_sp(zr(d), y, c) for d in range(1, NZ)]
    x_peers = [{"tp": xr(d)} for d in range(1, NX)]
    yp, ym = at_sp(z, yr(1), c), at_sp(z, yr(-1), c)
    zp, zm = at_sp(zr(1), y, c), at_sp(zr(-1), y, c)
    partner = at_sp(z, y, 1 - c)

    groups, arrivals = {}, {}

    def send(group, name, src, dst, to):
        k = groups.setdefault(group, len(groups))
        n = ARRIVALS[arrivals.setdefault(name, len(arrivals))]
        pltpu.make_async_remote_copy(
            src_ref=src, dst_ref=dst, send_sem=send_sem.at[k], recv_sem=recv_sem.at[n],
            device_id=to, device_id_type=MESH,
        ).start()

    def waiter(k, n, bytes_of):
        return pltpu.make_async_remote_copy(
            src_ref=bytes_of, dst_ref=bytes_of, send_sem=send_sem.at[k], recv_sem=recv_sem.at[n],
            device_id=partner, device_id_type=MESH,
        )

    def recv(name, bytes_of):
        waiter(0, ARRIVALS[arrivals[name]], bytes_of).wait_recv()

    def sent(group, bytes_of):
        waiter(groups[group], 0, bytes_of).wait_send()

    tasks, drains = {}, []

    def task(f):
        tasks[f.__name__] = f
        return f

    def gather_tasks(p):
        first, count = PHASES[p]
        cut, cut_plus = PATH_A[p]
        tiles = (HID - cut) // 128
        few, many = cut + tiles // 2 * 128, cut + (tiles - tiles // 2) * 128
        path_a, path_a1, path_a2 = (0, cut), (0, cut_plus), (cut_plus, cut)
        path_b = (cut, HID)

        def halves(odd):
            middle = many if odd else few
            return (cut, middle), (middle, HID)

        def block(dz, dy, lanes):
            return G.at[
                pl.ds(first, count), zr(dz), yr(dy), c, :, pl.ds(lanes[0], lanes[1] - lanes[0])
            ]

        def sized(planes, rows, lanes):
            return G.at[
                pl.ds(first, count), pl.ds(0, planes), pl.ds(0, rows), c, :,
                pl.ds(lanes[0], lanes[1] - lanes[0]),
            ]

        def go(name, ref, to):
            send(f"{p}{name[0]}", f"{p}{name}", ref, ref, to)

        def both(name, ref, plus, minus):
            go(name, ref, plus)
            go(name, ref, minus)

        def got(name, lanes, count_of=1):
            recv(f"{p}{name}", sized(1, count_of, lanes))

        def a0():
            both("A0", block(0, 0, path_a), yp, ym)

        def b0():
            both("B1", block(0, 0, path_b), zp, zm)

        def a1():
            got("A0", path_a, 2)
            go("A1", block(0, -1, path_a1), yp)
            go("A1", block(0, 1, path_a2), ym)

        def s0():
            both("Z01", block(0, 0, path_a), zp, zm)

        def s1():
            both("Z11", block(0, -1, path_a), zp, zm)
            both("Z31", block(0, 1, path_a), zp, zm)

        def s2():
            got("A1", path_a)
            both("Z21", block(0, 2, path_a), zp, zm)

        def q(row, s):
            dy = (0, -1, 2, 1)[row]
            got(f"Z{row}{s}", path_a, 2 if s < 4 else 1)
            if s < 3 or (s == 3 and row in (0, 1)):
                go(f"Z{row}{s + 1}", block(-s, dy, path_a), zp)
            if s < 3 or (s == 3 and row in (2, 3)):
                go(f"Z{row}{s + 1}", block(s, dy, path_a), zm)

        def b(s):
            got(f"B{s}", path_b, 2 if s < 4 else 1)
            plus, minus = (path_b, path_b) if s < 3 else halves(p)
            if s < 4:
                go(f"B{s + 1}", block(-s, 0, plus), zp)
                go(f"B{s + 1}", block(s, 0, minus), zm)

        def y_(k):
            both(f"Y{k}", block(PLANES[k], 0, path_b), yp, ym)

        def f(k):
            got(f"Y{k}", path_b, 2)
            plus, minus = halves(k % 2)
            go(f"F{k}", block(PLANES[k], -1, plus), yp)
            go(f"F{k}", block(PLANES[k], 1, minus), ym)

        def d(k):
            got(f"F{k}", path_b)
            go(f"D{k}", G.at[pl.ds(first, count), zr(PLANES[k]), :, c], partner)

        def e(k):
            recv(f"{p}D{k}", sized(1, NY, (0, HID)))

        def all_sent():
            for kind, planes, rows, lanes in (
                ("A", 1, 3, path_a), ("Z", 7, 4, path_a), ("Y", 8, 2, path_b), ("F", 8, 1, path_b),
                ("B", 7, 1, path_b), ("D", 8, 4, (0, HID)),
            ):
                sent(f"{p}{kind}", sized(planes, rows, lanes))

        drains.append(all_sent)
        for name, f_ in (("a0", a0), ("b0", b0), ("a1", a1), ("s0", s0), ("s1", s1), ("s2", s2)):
            tasks[f"{p}{name}"] = f_
        for s in range(1, 5):
            tasks[f"{p}b{s}"] = functools.partial(b, s)
            for row in range(NY):
                tasks[f"{p}q{row}{s}"] = functools.partial(q, row, s)
        for k in range(NZ):
            tasks[f"{p}y{k}"] = functools.partial(y_, k)
            tasks[f"{p}f{k}"] = functools.partial(f, k)
            tasks[f"{p}d{k}"] = functools.partial(d, k)
            tasks[f"{p}e{k}"] = functools.partial(e, k)

    for p in range(len(PHASES)):
        gather_tasks(p)

    small = [
        (mix_h, mix), (forget_h, forget_t), (decay_h, decay), (turn_h, turn), (in_re_h, in_re),
        (in_im_h, in_im), (out_re_h, out_re), (out_im_h, out_im), (skip_h, skip),
        (mix_gain_h, mix_gain), (ffn_gain_h, ffn_gain),
    ]
    early = [pltpu.make_async_copy(a, b, entry_sem.at[k]) for k, (a, b) in enumerate(small)]
    loads = [
        pltpu.make_async_copy(gate, G.at[0, z, y, c], local_sem.at[0]),
        pltpu.make_async_copy(up, G.at[1, z, y, c], local_sem.at[0]),
        pltpu.make_async_copy(down_t, G.at[2, z, y, c], local_sem.at[0]),
        pltpu.make_async_copy(resid, RA.at[x], local_sem.at[1]),
        pltpu.make_async_copy(w_out, WO, local_sem.at[2]),
    ]
    for load in loads[:3]:
        load.start()
    barrier = pltpu.get_barrier_semaphore()
    peers = plane_peers + [zp, zm] + x_peers
    for peer in peers:
        pl.semaphore_signal(barrier, inc=1, device_id=peer, device_id_type=MESH)
    for load in early + loads[3:]:
        load.start()

    def hello(n):
        for peer in (zp, zm):
            pl.semaphore_signal(hello_sem.at[n], inc=1, device_id=peer, device_id_type=MESH)

    def met(n):
        pl.semaphore_wait(hello_sem.at[n], 2)
        if n < 2:
            hello(n + 1)

    for n in range(3):
        tasks[f"h{n}"] = functools.partial(met, n)

    with jax.named_scope("entry"):
        pl.semaphore_wait(barrier, len(peers))
        own_weights = G.at[:, z, y, c]
        pltpu.make_async_copy(own_weights, own_weights, local_sem.at[0]).wait()
        hello(0)
    with jax.named_scope("opening"):
        for task_number in OPENING:
            list(tasks.values())[task_number]()
        for load in early:
            load.wait()
    with jax.named_scope("prep"):
        drive = mix[...]
        spread = where_one(lax.rem(iota((CHAN, LOCAL), 1), CHAN) == iota((CHAN, LOCAL), 0))
        twice = where_one(lax.rem(iota((STATE, LANES), 1), STATE) == iota((STATE, LANES), 0))
        rate2 = nn(decay[...], twice, HIGH)
        turn2 = nn(turn[...], twice, HIGH)
        lower = iota((ROWS, ROWS), 0) >= iota((ROWS, ROWS), 1)
        lower_one = where_one(lower)
        forget_rows = forget_t[...]
        run_log = nt(lower_one, forget_rows, HIGH)
        run_log_t = nt(forget_rows, lower_one, HIGH)
        w = 2.0 * rate2
        series = 1.0 + w / 6.0
        for k in (5.0, 4.0, 3.0, 2.0):
            series = 1.0 + (w / k) * series
        in_factor = jnp.sqrt(-(w * series))
        first_half = where_one(iota((STATE, LANES), 1) == iota((STATE, LANES), 0)).astype(bf16)
        second_half = where_one(
            iota((STATE, LANES), 1) == iota((STATE, LANES), 0) + STATE
        ).astype(bf16)
        row_group = lax.div(iota((LOCAL, LANES), 0), CHAN)

        def by_group(rows):
            return jnp.concatenate(
                [jnp.where(row_group == g, rows, 0.0).astype(bf16) for g in range(GROUPS)], axis=1
            )

        in_map = by_group(
            nn(in_re[...].astype(bf16), first_half) + nn(in_im[...].astype(bf16), second_half)
        )
        UB[...] = nn(drive, in_map)
        sign = sign_lanes((1, LANES))
        sign8 = sign_lanes((GROUPS, LANES))
        coarse = (iota((16, LANES), 0) - 8).astype(f32) * 16.0
        fine = iota((16, LANES), 0).astype(f32)
        centred = (iota((ROWS, LANES), 0) - ROWS // 2).astype(f32)

    def phase_tables(g):
        angle = turn2[g : g + 1]
        ca, sa = jnp.cos(angle * coarse), jnp.sin(angle * coarse)
        cb, sb = jnp.cos(angle * fine), jnp.sin(angle * fine)
        cos = [ca[k : k + 1] * cb - sa[k : k + 1] * sb for k in range(16)]
        sin = [sa[k : k + 1] * cb + ca[k : k + 1] * sb for k in range(16)]
        return jnp.concatenate(cos, axis=0), jnp.concatenate(sin, axis=0) * sign

    def power(n, log=0.0):
        size = jnp.exp(rate2 * n + log)
        return size * jnp.cos(turn2 * n), size * jnp.sin(turn2 * n) * sign8

    v = {}
    on_diagonal = iota((GROUPS, LANES), 0) == iota((GROUPS, LANES), 1)

    def as_row(column):
        return jnp.sum(jnp.where(on_diagonal, column, 0.0), axis=0, keepdims=True)

    def as_column(row):
        return jnp.sum(jnp.where(on_diagonal, row, 0.0), axis=1, keepdims=True)

    @task
    def local():
        ends = []
        last = run_log[ROWS - 1 : ROWS]
        for g in range(GROUPS):
            lanes = slice(LANES * g, LANES * (g + 1))
            cos, sin = phase_tables(g)
            grow = jnp.exp(-rate2[g : g + 1] * centred) * in_factor[g : g + 1]
            b_g = UB[:, lanes]
            u = (b_g * cos - swap(b_g) * sin) * grow
            UB[:, lanes] = u
            fall = jnp.exp(rate2[g : g + 1] * centred)
            ST[0, :, lanes] = cos * fall
            ST[1, :, lanes] = sin * fall
            weight = jnp.exp(last[:, g : g + 1] - run_log[:, g : g + 1])
            total = jnp.sum(u * weight, axis=0, keepdims=True)
            at_end = slice(ROWS - 1, ROWS)
            ends.append(turned(total, ST[0, at_end, lanes], ST[1, at_end, lanes]))
        last_col = jnp.sum(
            jnp.where(iota((GROUPS, ROWS), 1) == ROWS - 1, run_log_t, 0.0), axis=1, keepdims=True
        )
        C1[slot, 0:GROUPS] = jnp.concatenate(ends, axis=0)
        C1[slot, GROUPS:] = as_row(last_col)

    @task
    def c1():
        for d in range(1, NY * NC):
            send("C1", "C1", C1.at[slot], C1.at[slot], plane_peers[d - 1])

    @task
    def masked():
        for g in range(GROUPS):
            lanes = slice(LANES * g, LANES * (g + 1))
            gap = run_log[:, g : g + 1] - run_log_t[g : g + 1]
            weights = jnp.where(lower, jnp.exp(jnp.minimum(gap, 0.0)), 0.0).astype(bf16)
            YB[:, lanes] = nn(weights, UB[:, lanes].astype(bf16))

    @task
    def carry():
        c_one, s_one = power(float(ROWS))
        recv("C1", C1.at[1:])
        acc = jnp.zeros((GROUPS, LANES), f32)
        log_acc = jnp.zeros((GROUPS, 1), f32)
        before, log_before = acc, log_acc
        for j in range(NY * NC):
            here = slot == j
            before = jnp.where(here, acc, before)
            log_before = jnp.where(here, log_acc, log_before)
            log_j = as_column(C1[j, GROUPS:])
            acc = jnp.exp(log_j) * turned(acc, c_one, s_one) + C1[j, 0:GROUPS]
            log_acc = log_acc + log_j
        C2[z, 0:GROUPS] = acc
        C2[z, GROUPS:] = as_row(log_acc)
        v["before"], v["log_before"] = before, log_before

    @task
    def c2():
        for d in range(1, NZ):
            send("C2", "C2", C2.at[z], C2.at[z], z_peers[d - 1])

    @task
    def outmap():
        v["out_map"] = by_group(
            nn(out_re[...].astype(bf16), first_half) - nn(out_im[...].astype(bf16), second_half)
        )
        skip_rows = nn(skip[...], spread, HIGH)
        in_group = lax.div(iota((GROUPS, LOCAL), 1), CHAN) == iota((GROUPS, LOCAL), 0)
        v["skip_row"] = jnp.sum(jnp.where(in_group, skip_rows, 0.0), axis=0, keepdims=True)

    @task
    def far():
        c_plane, s_plane = power(float(ROWS * NY * NC))
        c_in, s_in = power(slot.astype(f32) * float(ROWS), v["log_before"])
        c_mid, s_mid = power(float(ROWS // 2 + 1))
        recv("C2", C2.at[1:])
        total = jnp.zeros((GROUPS, LANES), f32)
        for j in range(NZ):
            fade = jnp.exp(as_column(C2[j, GROUPS:]))
            step_on = fade * turned(total, c_plane, s_plane) + C2[j, 0:GROUPS]
            total = jnp.where(j < z, step_on, total)
        v["carry"] = turned(v["before"] + turned(total, c_in, s_in), c_mid, s_mid)

    @task
    def resp():
        for g in range(GROUPS):
            lanes = slice(LANES * g, LANES * (g + 1))
            full = YB[:, lanes] + jnp.exp(run_log[:, g : g + 1]) * v["carry"][g : g + 1]
            YB[:, lanes] = turned(full, ST[0, :, lanes], ST[1, :, lanes])
        response = nt(YB[...].astype(bf16), v["out_map"]) + v["skip_row"] * drive.astype(f32)
        MX[x] = jax.nn.gelu(response).astype(bf16)

    @task
    def m():
        for d in range(1, NX):
            send("M", "M", MX.at[x], MX.at[x], x_peers[d - 1])

    half = OWN // 2

    @task
    def r0():
        loads[3].wait()
        send("R", "R", RA.at[x], RA.at[x], x_peers[0])
        send("R", "R", RA.at[x], RA.at[x], x_peers[2])

    @task
    def r1():
        recv("R", RA.at[2:])
        send("Q", "Q", RA.at[xr(-1), 0:half], RA.at[xr(-1), 0:half], x_peers[0])
        send("Q", "Q", RA.at[xr(1), half:], RA.at[xr(1), half:], x_peers[2])

    @task
    def r2():
        recv("Q", RA.at[0])
        loads[4].wait()

    @task
    def proj():
        recv("M", MX.at[1:])
        mixed = [MX[q].astype(f32) for q in range(NX)]
        total = sum(jnp.sum(m * m, axis=1, keepdims=True) for m in mixed)
        scale = lax.rsqrt(total / float(LOCAL * NX) + eps)
        gains = mix_gain[...]
        normed = jnp.concatenate(
            [
                (mixed[q] * scale * gains[:, LOCAL * q : LOCAL * (q + 1)]).astype(bf16)
                for q in range(NX)
            ],
            axis=1,
        )
        squares = jnp.zeros((ROWS, 1), f32)
        for k in range(4):
            lanes = slice(512 * k, 512 * (k + 1))
            piece = nn(normed, WO[:, lanes]) + RA[:, :, lanes].reshape(ROWS, 512).astype(f32)
            RM[:, lanes] = piece
            squares = squares + jnp.sum(piece * piece, axis=1, keepdims=True)
        scale = lax.rsqrt(squares / float(D) + eps)
        for k in range(4):
            lanes = slice(512 * k, 512 * (k + 1))
            X[:, lanes] = (RM[:, lanes] * scale * ffn_gain[:, lanes]).astype(bf16)

    def column_slice(k):
        return pl.ds(pl.multiple_of(zr(PLANES[k]) * ROWS, ROWS), ROWS)

    def first(k):
        piece = X[:, column_slice(k)]
        for m, store in ((0, GA), (1, UA)):
            product = nn(piece, G[m, zr(PLANES[k])].reshape(ROWS, HID))
            store[...] = product if k == 0 else store[...] + product

    @task
    def hidden():
        HB[...] = (silu(GA[...]) * UA[...]).astype(bf16)

    def second(k):
        part = nt(HB[...], G[2, zr(PLANES[k])].reshape(ROWS, HID))
        PT[:, :, column_slice(k)] = part.astype(bf16).reshape(NX, OWN, ROWS)

    def part_slice(k, side):
        return pl.ds(pl.multiple_of(zr(PLANES[k]) * ROWS + 128 * side, 128), 128)

    def scat(k):
        if k in DIRECT:
            cols = column_slice(k)
            for d in (2, 1, 3):
                send("T", f"S{k}", PT.at[xr(d), :, cols], RT.at[DIRECT.index(k), x], x_peers[d - 1])
            return
        for side, to in ((0, x_peers[0]), (1, x_peers[2])):
            send("S", f"S{k}", PT.at[xr(2), :, part_slice(k, side)], RB.at[k, side], to)
        if k in RELAY:
            near(k, "W")

    def near(k, kind):
        cols = column_slice(k)
        send(kind, f"{kind}{k}", PT.at[xr(1), :, cols], RS.at[0, :, cols], x_peers[0])
        send(kind, f"{kind}{k}", PT.at[xr(-1), :, cols], RS.at[1, :, cols], x_peers[2])

    def pass_(k):
        recv(f"S{k}", RB.at[k])
        if k in RELAY:
            n = RELAY.index(k)
            for side, to in ((0, x_peers[0]), (1, x_peers[2])):
                send("U", f"V{k}", RB.at[k, side], RQ.at[n, side], to)
            return
        for side, dx in ((0, 1), (1, -1)):
            lanes = part_slice(k, side)
            sum_ = PT[xr(dx), :, lanes].astype(f32) + RB[k, side].astype(f32)
            PT[xr(dx), :, lanes] = sum_.astype(bf16)
        near(k, "V")

    def fin(k):
        cols = column_slice(k)
        ffn = PT[x, :, cols].astype(f32)
        if k in DIRECT:
            n = DIRECT.index(k)
            recv(f"S{k}", RT.at[n, 1:])
            for d in range(1, NX):
                ffn = ffn + RT[n, xr(d)].astype(f32)
        else:
            recv(f"W{k}" if k in RELAY else f"V{k}", RS.at[:, :, 0:ROWS])
            ffn = ffn + RS[0, :, cols].astype(f32) + RS[1, :, cols].astype(f32)
        if k in RELAY:
            n = RELAY.index(k)
            recv(f"V{k}", RQ.at[n])
            ffn = ffn + jnp.concatenate([RQ[n, 0], RQ[n, 1]], axis=1).astype(f32)
        kept = RM[pl.ds(pl.multiple_of(x * OWN, OWN), OWN), cols]
        out[:, cols] = (kept + 0.5 * ffn).astype(bf16)

    for k in range(NZ):
        tasks[f"first{k}"] = functools.partial(first, k)
        tasks[f"second{k}"] = functools.partial(second, k)
        tasks[f"scat{k}"] = functools.partial(scat, k)
        tasks[f"pass{k}"] = functools.partial(pass_, k)
        tasks[f"fin{k}"] = functools.partial(fin, k)

    table = list(tasks)
    for task_number in ORDER:
        with jax.named_scope(table[task_number]):
            tasks[table[task_number]]()
    with jax.named_scope("drain"):
        assert len(groups) == N_GROUPS and len(arrivals) == len(ARRIVALS)
        for drain in drains:
            drain()
        sent("C1", C1.at[1:])
        sent("C2", C2.at[1:])
        sent("M", MX.at[1:])
        sent("R", RA.at[2:])
        sent("Q", RA.at[0])
        passed = NZ - len(DIRECT)
        summed = passed - len(RELAY)
        sent("S", RB.at[0:passed])
        sent("V", RS.at[:, :, 0 : summed * ROWS])
        if DIRECT:
            sent("T", RT.at[:, 1:])
        if RELAY:
            sent("W", RS.at[:, :, 0 : len(RELAY) * ROWS])
            sent("U", RQ)


def per_device(
    resid, mix_in, decay_rate, turn_rate, forget, input_real, input_imag, output_real, output_imag,
    skip_gain, mix_gain, w_out, ffn_gain, gating_matrix, w_up, w_down,
):
    operands = (
        resid, mix_in, forget.T, decay_rate, turn_rate,
        input_real.transpose(0, 2, 1).reshape(-1, STATE),
        input_imag.transpose(0, 2, 1).reshape(-1, STATE),
        output_real.reshape(-1, STATE), output_imag.reshape(-1, STATE),
        skip_gain, mix_gain.reshape(1, -1), w_out, ffn_gain.reshape(1, -1),
        gating_matrix, w_up, w_down.T,
    )
    own = [pltpu.VMEM(operands[k].shape, operands[k].dtype) for k in (*range(1, 11), 12)]
    return pl.pallas_call(
        kernel,
        out_shape=jax.ShapeDtypeStruct((OWN, D), bf16),
        in_specs=[pl.BlockSpec(memory_space=pl.ANY)] * len(operands),
        out_specs=pl.BlockSpec(memory_space=pltpu.VMEM),
        scratch_shapes=own + [
            pltpu.VMEM((3, NZ, NY, NC, SHARD, HID), bf16),
            pltpu.VMEM((NX, OWN, D), bf16),
            pltpu.VMEM((LOCAL * NX, D), bf16),
            pltpu.VMEM((NX, ROWS, LOCAL), bf16),
            pltpu.VMEM((ROWS, D), bf16),
            pltpu.VMEM((ROWS, D), f32),
            pltpu.VMEM((ROWS, HID), f32),
            pltpu.VMEM((ROWS, HID), f32),
            pltpu.VMEM((ROWS, HID), bf16),
            pltpu.VMEM((NX, OWN, D), bf16),
            pltpu.VMEM((2, OWN, D), bf16),
            pltpu.VMEM((NZ, 2, OWN, 128), bf16),
            pltpu.VMEM((max(len(RELAY), 1), 2, OWN, 128), bf16),
            pltpu.VMEM((max(len(DIRECT), 1), NX, OWN, ROWS), bf16),
            pltpu.VMEM((ROWS, WIDE), f32),
            pltpu.VMEM((ROWS, WIDE), f32),
            pltpu.VMEM((2, ROWS, WIDE), f32),
            pltpu.VMEM((NY * NC, GROUPS + 1, LANES), f32),
            pltpu.VMEM((NZ, GROUPS + 1, LANES), f32),
            pltpu.SemaphoreType.DMA((N_GROUPS,)),
            pltpu.SemaphoreType.DMA((N_ARRIVALS,)),
            pltpu.SemaphoreType.DMA((3,)),
            pltpu.SemaphoreType.DMA((len(own),)),
            pltpu.SemaphoreType.REGULAR((3,)),
        ],
        compiler_params=pltpu.CompilerParams(
            collective_id=0, has_side_effects=True, vmem_limit_bytes=52 * 1024 * 1024
        ),
    )(*[pltpu.with_memory_space_constraint(operand, pltpu.HBM) for operand in operands])


def solution(mesh):
    placed = (
        P(("sp", "tp"), None),
        P("sp", "tp"),
        P("tp", None),
        P("tp", None),
        P("sp", "tp"),
        P("tp", None, None),
        P("tp", None, None),
        P("tp", None, None),
        P("tp", None, None),
        P("tp", None),
        P(),
        P(),
        P(),
        P("sp", "tp"),
        P("sp", "tp"),
        P("tp", "sp"),
    )
    return jax.shard_map(
        per_device, mesh=mesh, in_specs=placed, out_specs=P(("sp", "tp"), None), check_vma=False
    )
```
